256 devices in a mesh: row: 32 (over z, x), col: 8 (over y, core).
Axes of the slice: x: 4, y: 4, z: 8, core: 2. Of those that a mesh axis runs over, the one named last changes fastest.
Arguments:
- tokens: bfloat16 [8192, 2048], P('row'), may hold values from -6 to 6
- norm_gain: float32 [2048], replicated, may hold values from 0.5 to 1.5
- first_gate: bfloat16 [2048, 1024], P(None, 'col'), may hold values from -0.125 to 0.125
- second_gate: bfloat16 [2048, 1024], P(None, 'col'), may hold values from -0.125 to 0.125
- value_weight: bfloat16 [2048, 1024], P(None, 'col'), may hold values from -0.125 to 0.125
- short_weight: bfloat16 [3, 3, 1024], P(None, None, 'col'), may hold values from -3.5 to 3.5
- short_bias: float32 [3, 1024], P(None, 'col'), may hold values from -2 to 2
- embed_weight: float32 [33, 64], replicated, may hold values from -1 to 1
- embed_bias: float32 [64], replicated, may hold values from -3 to 3
- inner_weight: float32 [64, 64], replicated, may hold values from -0.75 to 0.75
- inner_bias: float32 [64], replicated, may hold values from -3 to 3
- filter_freq: float32 [64], replicated, may hold values from 0.5 to 1.5
- filter_weight: float32 [2, 2, 64, 1024], P(None, None, None, ('col', 'row')), may hold values from -0.0234375 to 0.0234375
- filter_skip: float32 [2, 1024], P(None, ('col', 'row')), may hold values from -3 to 3
- output_gain: float32 [1024], P('col'), may hold values from 0.5 to 1.5
- output_weight: bfloat16 [1024, 2048], replicated, may hold values from -0.1875 to 0.1875
Outputs:
- mixed_output: bfloat16 [8192, 2048], P(('row', 'col'))
The draws below stay inside these ranges and needn't reach their ends.
All inputs are finite; a program needn't handle non-finite values.
Results may differ from the reference program's by a relative error of at most 0.01.
Values may be sent and summed in bfloat16 or wider, within the bound.
A program may use at most 64 MiB of HBM per device.

```python
import math
import jax
import jax.numpy as jnp
from jax import lax

MODEL_WIDTH = 2048
CHANNELS = 1024
GROUPS = 8
SHORT = 3
FREQ_BANDS = 16
FEATURES = 33
FILTER_HIDDEN = 64
SEQ_LEN = 8192


def shard_levels(key, dims, cuts, smallest, top_value):
    loudness = 1.0
    for dim, blocks in cuts:
        draws = jax.random.uniform(jax.random.fold_in(jax.random.fold_in(key, 6), dim), (blocks,), jnp.float32, smallest / len(cuts), top_value / len(cuts))
        loudness = loudness * jnp.repeat(jnp.exp(draws), dims[dim] // blocks).reshape((-1,) + (1,) * (len(dims) - 1 - dim))
    return loudness


def scatter_about(stream_key, shape, deviation, limit, cuts=(), held_as=jnp.bfloat16):
    array = deviation * jax.random.normal(stream_key, shape, jnp.float32)
    if cuts:
        array = array * shard_levels(stream_key, shape, cuts, -0.22, 0.18)
    return jnp.clip(array, -limit, limit).astype(held_as)


def setup_inputs(seed: int = 0) -> dict:
    key_of = jax.random.split(jax.random.key(seed), 17)
    return {
        "tokens": scatter_about(key_of[0], (SEQ_LEN, MODEL_WIDTH), 1.0, 6.0, ((0, 32),)),
        "norm_gain": jnp.clip(1.0 + 0.1 * jax.random.normal(key_of[1], (MODEL_WIDTH,), jnp.float32), 0.5, 1.5),
        "first_gate": scatter_about(key_of[2], (MODEL_WIDTH, CHANNELS), MODEL_WIDTH ** -0.5, 0.125, ((1, 8),)),
        "second_gate": scatter_about(key_of[3], (MODEL_WIDTH, CHANNELS), MODEL_WIDTH ** -0.5, 0.125, ((1, 8),)),
        "value_weight": scatter_about(key_of[4], (MODEL_WIDTH, CHANNELS), MODEL_WIDTH ** -0.5, 0.125, ((1, 8),)),
        "short_weight": scatter_about(key_of[5], (3, SHORT, CHANNELS), SHORT ** -0.5, 3.5, ((2, 8),)),
        "short_bias": scatter_about(key_of[6], (3, CHANNELS), 0.3, 2.0, ((1, 8),), jnp.float32),
        "embed_weight": scatter_about(key_of[7], (FEATURES, FILTER_HIDDEN), FEATURES ** -0.5, 1.0, (), jnp.float32),
        "embed_bias": scatter_about(key_of[8], (FILTER_HIDDEN,), 0.5, 3.0, (), jnp.float32),
        "inner_weight": scatter_about(key_of[9], (FILTER_HIDDEN, FILTER_HIDDEN), FILTER_HIDDEN ** -0.5, 0.75, (), jnp.float32),
        "inner_bias": scatter_about(key_of[10], (FILTER_HIDDEN,), 0.5, 3.0, (), jnp.float32),
        "filter_freq": jnp.clip(1.0 + 0.1 * jax.random.normal(key_of[11], (FILTER_HIDDEN,), jnp.float32), 0.5, 1.5),
        "filter_weight": scatter_about(key_of[12], (2, 2, FILTER_HIDDEN, CHANNELS), (FILTER_HIDDEN * SEQ_LEN // 8) ** -0.5, 0.0234375, ((3, 256),), jnp.float32),
        "filter_skip": scatter_about(key_of[13], (2, CHANNELS), 0.5, 3.0, ((1, 256),), jnp.float32),
        "output_gain": jnp.clip(1.0 + 0.1 * jax.random.normal(key_of[14], (CHANNELS,), jnp.float32), 0.5, 1.5),
        "output_weight": scatter_about(key_of[15], (CHANNELS, MODEL_WIDTH), CHANNELS ** -0.5, 0.1875),
    }


HIGHEST = lax.Precision.HIGHEST
NORM_EPS = 1e-06
DECAY_TARGET = 0.01
FAST_SPAN = 0.3
SLOW_SPAN = 1.5

def position_features(length):
    position_ramp = jnp.linspace(0.0, 1.0, length, dtype=jnp.float32)[:, None]
    angles = 2.0 * math.pi * jnp.arange(length, dtype=jnp.float32)[:, None] / length
    band_freqs = jnp.linspace(0.0001, FREQ_BANDS - 1, FREQ_BANDS, dtype=jnp.float32)[None, :]
    features = jnp.concatenate([position_ramp, jnp.cos(band_freqs * angles), -jnp.sin(band_freqs * angles)], axis=1)
    return (position_ramp, features)

def filter_hidden(length, embed_weight, embed_bias, inner_weight, inner_bias, filter_freq):
    position_ramp, features = position_features(length)
    hidden = jnp.sin(filter_freq * (jnp.dot(features, embed_weight, precision=HIGHEST) + embed_bias))
    hidden = jnp.sin(filter_freq * (jnp.dot(hidden, inner_weight, precision=HIGHEST) + inner_bias))
    return (position_ramp, hidden)

def decay_rates():
    fastest = math.log(DECAY_TARGET) / FAST_SPAN
    slowest = math.log(DECAY_TARGET) / SLOW_SPAN
    return jnp.abs(jnp.linspace(slowest, fastest, CHANNELS, dtype=jnp.float32))

def short_filter(padded, weights, bias_row, length):
    result = bias_row.astype(jnp.float32)
    for tap_index in range(weights.shape[0]):
        result = result + padded[tap_index:tap_index + length].astype(jnp.float32) * weights[tap_index].astype(jnp.float32)
    return result

def two_sided(signal, forward, backward, skip_gain):
    length = signal.shape[0]
    circular_taps = jnp.concatenate([forward, jnp.zeros_like(forward[:1]), backward[:0:-1]], axis=0)
    spectrum = jnp.fft.rfft(signal, n=2 * length, axis=0) * jnp.fft.rfft(circular_taps, axis=0)
    return jnp.fft.irfft(spectrum, n=2 * length, axis=0)[:length] + signal * skip_gain

def reference(tokens, norm_gain, first_gate, second_gate, value_weight, short_weight, short_bias, embed_weight, embed_bias, inner_weight, inner_bias, filter_freq, filter_weight, filter_skip, output_gain, output_weight):
    widened = tokens.astype(jnp.float32)
    normed = (widened * lax.rsqrt(lax.optimization_barrier(jnp.mean(widened * widened, axis=1, keepdims=True)) + NORM_EPS) * norm_gain).astype(jnp.bfloat16)
    gate_first = jnp.dot(normed, first_gate, preferred_element_type=jnp.float32).astype(jnp.bfloat16)
    gate_second = jnp.dot(normed, second_gate, preferred_element_type=jnp.float32).astype(jnp.bfloat16)
    gate_value = jnp.dot(normed, value_weight, preferred_element_type=jnp.float32).astype(jnp.bfloat16)
    length = tokens.shape[0]
    position_ramp, hidden = filter_hidden(length, embed_weight, embed_bias, inner_weight, inner_bias, filter_freq)
    group_width = CHANNELS // GROUPS
    half_width = SHORT // 2

    def blocks(matrix):
        split = matrix.reshape(matrix.shape[:-1] + (GROUPS, group_width))
        return jnp.moveaxis(split, -2, 0)

    def one_block(pieces):
        first_block, second_block, value_block, weight_block, bias_block, filter_block, skip_block, decay_block, gain_block = pieces
        window = jnp.exp(-position_ramp * decay_block[None, :])
        smoothed = []
        for branch, source in enumerate((first_block, second_block, value_block)):
            padded = jnp.pad(source.astype(jnp.float32), ((half_width, SHORT - 1 - half_width), (0, 0)))
            smoothed.append(short_filter(padded, weight_block[branch], bias_block[branch], length))
        signal = smoothed[2]
        for order_index in range(2):
            forward = jnp.dot(hidden, filter_block[order_index, 0], precision=HIGHEST) * window
            backward = jnp.dot(hidden, filter_block[order_index, 1], precision=HIGHEST) * window
            signal = smoothed[order_index] * two_sided(signal, forward, backward, skip_block[order_index])
        scaled = signal * lax.rsqrt(lax.optimization_barrier(jnp.mean(signal * signal, axis=1, keepdims=True)) + NORM_EPS)
        return (scaled * gain_block).astype(jnp.bfloat16)
    normed_blocks = lax.map(one_block, (blocks(gate_first), blocks(gate_second), blocks(gate_value), blocks(short_weight), blocks(short_bias), blocks(filter_weight), blocks(filter_skip), blocks(decay_rates()), blocks(output_gain)))
    mixed = jnp.moveaxis(normed_blocks, 0, 1).reshape(length, CHANNELS)
    return jnp.dot(mixed, output_weight, preferred_element_type=jnp.float32).astype(jnp.bfloat16)
```

```python
import math

import jax
import jax.numpy as jnp
import ml_dtypes
import numpy as np
from jax import lax
from jax.experimental import pallas as pl
from jax.experimental.pallas import tpu as pltpu
from jax.sharding import PartitionSpec as P

CHANNELS = 1024
GROUPS = 8
FREQ_BANDS = 16
NORM_EPS = 1e-06
DECAY_TARGET = 0.01
FAST_SPAN = 0.3
SLOW_SPAN = 1.5

LENGTH = 8192
WIDTH = 2048
COLS = 128
LIVE = 64
HALF = 72
TOTAL = 16384
ROWS = 32
OWN = 4
FEATS = 48
CHUNK = 2048

BF = jnp.bfloat16
F32 = jnp.float32
MESH = pl.DeviceIdType.MESH


def split_np(matrix):
    high = matrix.astype(np.float32).astype(ml_dtypes.bfloat16)
    low = (matrix - high.astype(np.float64)).astype(np.float32).astype(ml_dtypes.bfloat16)
    return high, low


def make_constants():
    k1 = np.arange(HALF)
    a = np.arange(LIVE)
    b = np.arange(COLS)
    cos_in = np.cos(2 * np.pi * np.outer(k1, a) / COLS)
    sin_in = np.sin(2 * np.pi * np.outer(k1, a) / COLS)
    first = np.concatenate([cos_in, -sin_in], 0)
    turn = 2 * np.pi * np.outer(k1, b) / TOTAL
    twiddle = np.concatenate([np.cos(turn), np.sin(turn)], 1).astype(np.float32)
    cos_out = np.cos(2 * np.pi * (np.outer(b, b) % COLS) / COLS)
    sin_out = np.sin(2 * np.pi * (np.outer(b, b) % COLS) / COLS)
    second = np.block([[cos_out, -sin_out], [sin_out, cos_out]])
    back = np.block([[cos_out, sin_out], [-sin_out, cos_out]])
    weight = np.where((k1 == 0) | (k1 == COLS // 2), 1.0, 2.0) * (k1 <= COLS // 2)
    last = np.concatenate([cos_in.T * weight, -sin_in.T * weight], 1) / TOTAL
    first_h, first_l = split_np(first)
    last_h, last_l = split_np(last)
    n = np.arange(LENGTH)
    ramp = np.linspace(0.0, 1.0, LENGTH)[None, :]
    bands = np.linspace(0.0001, FREQ_BANDS - 1, FREQ_BANDS, dtype=np.float32).astype(np.float64)
    angle = bands[:, None] * (2 * np.pi * n / LENGTH)[None, :]
    feats = np.zeros((FEATS, LENGTH))
    feats[0:1] = ramp
    feats[1 : 1 + FREQ_BANDS] = np.cos(angle)
    feats[1 + FREQ_BANDS : 1 + 2 * FREQ_BANDS] = -np.sin(angle)
    feats[1 + 2 * FREQ_BANDS] = 1.0
    return dict(
        first=np.concatenate([first_h, first_l, first_h], 1),
        twiddle=twiddle,
        second=np.stack(split_np(second)),
        back=np.stack(split_np(back)),
        last=np.concatenate([last_h, last_l, last_h], 1),
        feats=np.concatenate(split_np(feats), 0),
    )


def sine_coefficients():
    v = 0.25 * np.cos(np.pi * (np.arange(400) + 0.5) / 800)
    basis = np.stack([v ** (2 * j + 1) for j in range(5)], 1)
    scale = 1.0 / np.sin(2 * np.pi * v)
    found = np.linalg.lstsq(basis * scale[:, None], np.ones_like(v), rcond=None)[0]
    return [float(c) for c in found]


SINE = sine_coefficients()


def sine_of_turns(turns):
    v = 0.25 - jnp.abs(turns - jnp.round(turns))
    square = v * v
    result = SINE[4]
    for c in SINE[3::-1]:
        result = result * square + c
    return result * v


def split(value):
    high = value.astype(BF)
    return high, (value - high.astype(F32)).astype(BF)


def dot(left, right):
    return jnp.dot(left, right, preferred_element_type=F32)


def tall(value):
    high, low = split(value)
    return jnp.concatenate([high, high, low], axis=0)


def wide(value):
    high, low = split(value)
    return jnp.concatenate([high, low, high], axis=1)


def dot_table(value, table, lo, hi):
    high, low = split(value)
    return (
        dot(high, table[0, :, lo:hi]) + dot(low, table[0, :, lo:hi]) + dot(high, table[1, :, lo:hi])
    )


def into_spectrum(signal, first, twiddle):
    part = dot(first[...], tall(signal))
    cos, sin = twiddle[:, :COLS], twiddle[:, COLS:]
    pieces = []
    for i in range(OWN):
        real = part[:HALF, i * COLS : (i + 1) * COLS]
        imag = part[HALF:, i * COLS : (i + 1) * COLS]
        pieces.append(jnp.concatenate([real * cos + imag * sin, imag * cos - real * sin], axis=1))
    return jnp.concatenate(pieces, axis=0)


def from_spectrum(spectrum, back, last, twiddle):
    part = dot_table(spectrum, back, 0, 2 * COLS)
    cos, sin = twiddle[:, :COLS], twiddle[:, COLS:]
    reals, imags = [], []
    for i in range(OWN):
        real = part[i * HALF : (i + 1) * HALF, :COLS]
        imag = part[i * HALF : (i + 1) * HALF, COLS:]
        reals.append(real * cos - imag * sin)
        imags.append(real * sin + imag * cos)
    turned = jnp.concatenate(
        [jnp.concatenate(reals, axis=1), jnp.concatenate(imags, axis=1)], axis=0
    )
    return dot(last[...], tall(turned))


def kernel(
    tokens_hbm, norm_gain_hbm, gate0_hbm, gate1_hbm, gate2_hbm, short_w_hbm, short_b_hbm,
    embed_w_hbm, embed_b_hbm, inner_w_hbm, inner_b_hbm, freq_hbm, filter_w_hbm, skip_hbm,
    out_gain_hbm, out_w_hbm, first_hbm, twiddle_hbm, second_hbm, back_hbm, last_hbm, feats_hbm,
    out_ref,
    tokens, norm_gain, gates, short_w, short_b, embed_w, embed_b, inner_w, inner_b, freq,
    filter_w, skip, out_gain, out_w, first, twiddle, second, back, last, feats,
    normed, flat, packed, send1, recv1, params, mixed_taps, spectra, smooth,
    send2, recv2, send3, recv3, load_sem, send_sems, recv_sems,
):
    me = lax.axis_index("row")
    col = lax.axis_index("col")
    n_col = 8

    barrier = pltpu.get_barrier_semaphore()

    def greet_row(k, carry):
        pl.semaphore_signal(
            barrier, inc=1, device_id=(lax.rem(me + k, ROWS), col), device_id_type=MESH
        )
        return carry

    def greet_col(k, carry):
        pl.semaphore_signal(
            barrier, inc=1, device_id=(me, lax.rem(col + k, n_col)), device_id_type=MESH
        )
        return carry

    lax.fori_loop(1, ROWS, greet_row, 0)
    lax.fori_loop(1, n_col, greet_col, 0)

    loads = [
        pltpu.make_async_copy(src, dst, load_sem.at[j])
        for j, (src, dst) in enumerate(
            [
                (tokens_hbm, tokens),
                (norm_gain_hbm, norm_gain),
                (gate0_hbm, gates.at[:, 0:128]),
                (gate1_hbm, gates.at[:, 128:256]),
                (gate2_hbm, gates.at[:, 256:384]),
                (embed_w_hbm, embed_w),
                (embed_b_hbm, embed_b),
                (inner_w_hbm, inner_w),
                (inner_b_hbm, inner_b),
                (freq_hbm, freq),
                (filter_w_hbm, filter_w),
                (feats_hbm, feats),
                (first_hbm, first),
                (twiddle_hbm, twiddle),
                (second_hbm, second),
                (short_w_hbm, short_w),
                (short_b_hbm, short_b),
                (skip_hbm, skip),
                (back_hbm, back),
                (last_hbm, last),
                (out_gain_hbm, out_gain),
                (out_w_hbm, out_w),
            ]
        )
    ]
    for load in loads:
        load.start()

    for load in loads[0:2]:
        load.wait()

    def normalise(j, carry):
        rows = pl.ds(pl.multiple_of(j * 64, 64), 64)
        wide_tokens = tokens[rows, :].astype(F32)
        mean = jnp.mean(wide_tokens * wide_tokens, axis=1, keepdims=True)
        normed[rows, :] = (wide_tokens * lax.rsqrt(mean + NORM_EPS) * norm_gain[...]).astype(BF)
        return carry

    lax.fori_loop(0, 4, normalise, 0)
    for load in loads[2:5]:
        load.wait()
    projected = dot(normed[...], gates[...])
    projected = projected.astype(BF).astype(F32).T
    for b in range(3):
        for half in range(2):
            flat[pl.ds(half * 128, 128), :] = projected[
                b * 128 : (b + 1) * 128, half * 128 : (half + 1) * 128
            ]
        for half in range(2):
            for i in range(OWN):
                packed[pl.ds(4 * half + i, ROWS, stride=8), :] = flat[
                    pl.ds(128 * half + i, ROWS, stride=4), :
                ]
        send1[:, b] = packed[...].reshape(ROWS, 8, COLS).astype(BF)

    pl.semaphore_wait(barrier, ROWS - 1 + n_col - 1)

    def row_copy(source, target, number, k):
        there = lax.rem(me + k, ROWS)
        return pltpu.make_async_remote_copy(
            src_ref=source.at[there],
            dst_ref=target.at[me],
            send_sem=send_sems.at[number],
            recv_sem=recv_sems.at[number],
            device_id=(there, col),
            device_id_type=MESH,
        )

    def send_out(k, carry):
        row_copy(send1, recv1, 0, k).start()
        return carry

    lax.fori_loop(1, ROWS, send_out, 0)
    recv1[me] = send1[me]

    for load in loads[5:15]:
        load.wait()
    params[...] = jnp.zeros_like(params)
    scale = freq[...] * (1.0 / (2.0 * math.pi))
    params[0:33, 0:64] = embed_w[...] * scale
    params[33:34, 0:64] = embed_b[...] * scale - 0.25
    params[48:49, 0:64] = inner_b[...] * scale - 0.25
    params[64:128, 0:64] = inner_w[...] * scale
    params[0:64, 64:80] = jnp.concatenate(
        [filter_w[o, e] for o in range(2) for e in range(2)], axis=1
    )
    turned = params[...].T
    embed_t = wide(turned[0:64, 0:FEATS])
    inner_bias = turned[0:64, 48:49]
    inner_t = wide(turned[0:64, 64:128])
    filter_t = wide(turned[64:80, 0:64])

    row8 = lax.broadcasted_iota(jnp.int32, (8, 1), 0)
    channel = (col * ROWS + me) * OWN + lax.rem(row8, OWN)
    fastest = math.log(DECAY_TARGET) / FAST_SPAN
    slowest = math.log(DECAY_TARGET) / SLOW_SPAN
    place = channel.astype(F32) * (1.0 / (CHANNELS - 1))
    decay = jnp.abs(slowest * (1.0 - place) + fastest * place)

    def taps_of(j, carry):
        start = pl.multiple_of(j * CHUNK, CHUNK)
        lanes = pl.ds(start, CHUNK)
        high, low = feats[0:FEATS, lanes], feats[FEATS:, lanes]
        hidden = sine_of_turns(dot(embed_t, jnp.concatenate([high, high, low], axis=0)))
        hidden = sine_of_turns(dot(inner_t, tall(hidden)) + inner_bias)
        taps = dot(filter_t, tall(hidden))
        lag = start + lax.broadcasted_iota(jnp.int32, (8, CHUNK), 1)
        row = lax.broadcasted_iota(jnp.int32, (8, CHUNK), 0)
        window = jnp.exp(-(lag.astype(F32) * (1.0 / (LENGTH - 1))) * decay)
        window = jnp.where((lag == 0) & (row >= OWN), 0.0, window)
        for o in range(2):
            both = taps[8 * o : 8 * o + 8] * window
            other = pltpu.roll(both, OWN, axis=0)
            both = jnp.where(row < OWN, both + other, other - both)
            for q in range(CHUNK // COLS):
                at = pl.multiple_of(start // COLS * 8, 8) + o * LIVE * 8 + q * 8
                mixed_taps[pl.ds(pl.multiple_of(at, 8), 8), :] = both[:, q * COLS : (q + 1) * COLS]
        return carry

    lax.fori_loop(0, LENGTH // CHUNK, taps_of, 0)
    for o in range(2):
        for part in range(2):
            signal = jnp.concatenate(
                [
                    mixed_taps[pl.ds(o * LIVE * 8 + part * OWN + i, LIVE, stride=8), :]
                    for i in range(OWN)
                ],
                axis=1,
            )
            spectra[o, :, part * COLS : (part + 1) * COLS] = dot_table(
                into_spectrum(signal, first, twiddle), second, part * COLS, (part + 1) * COLS
            )

    for load in loads[15:21]:
        load.wait()
    lane8 = lax.broadcasted_iota(jnp.int32, (8, COLS), 1)
    mine = lane8 == OWN * me + lax.rem(lax.broadcasted_iota(jnp.int32, (8, COLS), 0), OWN)

    def own_column(line):
        return jnp.sum(
            jnp.where(mine, jnp.broadcast_to(line, (8, COLS)), 0.0), axis=1, keepdims=True
        )

    all_short = short_w[...].astype(F32)
    columns = [
        [own_column(all_short[b, j : j + 1]) for j in range(3)] + [own_column(short_b[b : b + 1, :])]
        for b in range(3)
    ]

    def wait_row(target, number):
        pltpu.make_async_copy(
            target.at[pl.ds(0, ROWS - 1)], target.at[pl.ds(0, ROWS - 1)], recv_sems.at[number]
        ).wait()

    wait_row(recv1, 0)
    row = lax.broadcasted_iota(jnp.int32, (256, COLS), 0)
    lane = lax.broadcasted_iota(jnp.int32, (256, COLS), 1)
    smoothed = []
    for b in range(3):
        here = recv1[:, b].astype(F32).reshape(256, COLS)
        before = pltpu.roll(here, 1, axis=1)
        before = jnp.where(lane == 0, pltpu.roll(before, OWN, axis=0), before)
        before = jnp.where((lane == 0) & (row < OWN), 0.0, before)
        after = pltpu.roll(here, COLS - 1, axis=1)
        after = jnp.where(lane == COLS - 1, pltpu.roll(after, 256 - OWN, axis=0), after)
        after = jnp.where((lane == COLS - 1) & (row >= 256 - OWN), 0.0, after)
        tap = [jnp.broadcast_to(c, (8, COLS))[None] for c in columns[b]]
        shape = (ROWS, 8, COLS)
        value = tap[3] + before.reshape(shape) * tap[0]
        value = value + here.reshape(shape) * tap[1]
        value = value + after.reshape(shape) * tap[2]
        smooth[b] = value.reshape(256, COLS)
        smoothed.append(
            jnp.concatenate(
                [smooth[b, pl.ds(i, LIVE, stride=OWN), :] for i in range(OWN)], axis=1
            )
        )

    signal = smoothed[2]
    for o in range(2):
        spectrum = dot_table(into_spectrum(signal, first, twiddle), second, 0, 2 * COLS)
        real, imag = spectrum[:, :COLS], spectrum[:, COLS:]
        t_real, t_imag = spectra[o, :, :COLS], spectra[o, :, COLS:]
        product = jnp.concatenate(
            [real * t_real - imag * t_imag, real * t_imag + imag * t_real], axis=1
        )
        direct = jnp.concatenate(
            [
                signal[:, i * COLS : (i + 1) * COLS]
                * jnp.broadcast_to(skip[o : o + 1, i : i + 1], (LIVE, COLS))
                for i in range(OWN)
            ],
            axis=1,
        )
        signal = smoothed[o] * (from_spectrum(product, back, last, twiddle) + direct)

    for i in range(OWN):
        flat[pl.ds(i * LIVE, LIVE), :] = signal[:, i * COLS : (i + 1) * COLS]
    for i in range(OWN):
        for half in range(2):
            packed[pl.ds(2 * i + half, ROWS, stride=8), :] = flat[
                pl.ds(i * LIVE + half, ROWS, stride=2), :
            ]
    send2[...] = packed[...].reshape(ROWS, 8, COLS).astype(BF)

    def send_back(k, carry):
        row_copy(send2, recv2, 1, k).start()
        return carry

    lax.fori_loop(1, ROWS, send_back, 0)
    recv2[me] = send2[me]
    wait_row(recv2, 1)

    values = recv2[...].astype(F32)
    squares = jnp.sum(values * values, axis=0)
    squares = squares + pltpu.roll(squares, 4, axis=0)
    squares = squares + pltpu.roll(squares, 2, axis=0)
    factor = lax.rsqrt(squares * (GROUPS / CHANNELS) + NORM_EPS)
    flat[...] = (values * factor[None]).reshape(256, COLS)
    for half in range(2):
        turned = flat[pl.ds(half, COLS, stride=2), :].T * out_gain[...]
        send3[4 * half : 4 * half + 4] = turned.reshape(4, 32, COLS).astype(BF)

    def send_over(k, carry):
        there = lax.rem(col + k, n_col)
        pltpu.make_async_remote_copy(
            src_ref=send3.at[there],
            dst_ref=recv3.at[col],
            send_sem=send_sems.at[2],
            recv_sem=recv_sems.at[2],
            device_id=(me, there),
            device_id_type=MESH,
        ).start()
        return carry

    lax.fori_loop(1, n_col, send_over, 0)
    recv3[col] = send3[col]
    loads[21].wait()
    pltpu.make_async_copy(
        recv3.at[pl.ds(0, n_col - 1)], recv3.at[pl.ds(0, n_col - 1)], recv_sems.at[2]
    ).wait()
    mixed = jnp.concatenate([recv3[c] for c in range(n_col)], axis=1)
    for q in range(4):
        out_ref[:, q * 512 : (q + 1) * 512] = dot(mixed, out_w[:, q * 512 : (q + 1) * 512]).astype(
            BF
        )

    for number, source in ((0, send1), (1, send2)):
        pltpu.make_async_copy(
            source.at[pl.ds(0, ROWS - 1)], source.at[pl.ds(0, ROWS - 1)], send_sems.at[number]
        ).wait()
    pltpu.make_async_copy(
        send3.at[pl.ds(0, n_col - 1)], send3.at[pl.ds(0, n_col - 1)], send_sems.at[2]
    ).wait()


def local(
    tokens, norm_gain, first_gate, second_gate, value_weight, short_weight, short_bias,
    embed_weight, embed_bias, inner_weight, inner_bias, filter_freq, filter_weight, filter_skip,
    output_gain, output_weight,
):
    constants = make_constants()
    operands = [
        tokens, norm_gain[None], first_gate, second_gate, value_weight, short_weight, short_bias,
        embed_weight, embed_bias[None], inner_weight, inner_bias[None], filter_freq[None],
        filter_weight, filter_skip, output_gain[None], output_weight,
    ] + [
        jnp.asarray(constants[name])
        for name in ("first", "twiddle", "second", "back", "last", "feats")
    ]
    vmem = pltpu.VMEM
    scratch = (
        [vmem(x.shape, x.dtype) for x in operands[0:2]]
        + [vmem((WIDTH, 384), BF)]
        + [vmem(x.shape, x.dtype) for x in operands[5:]]
    )
    scratch += [
        vmem((256, WIDTH), BF),
        vmem((256, COLS), F32),
        vmem((256, COLS), F32),
        vmem((ROWS, 3, 8, COLS), BF),
        vmem((ROWS, 3, 8, COLS), BF),
        vmem((128, 128), F32),
        vmem((2 * LIVE * 8, COLS), F32),
        vmem((2, OWN * HALF, 2 * COLS), F32),
        vmem((3, 256, COLS), F32),
        vmem((ROWS, 8, COLS), BF),
        vmem((ROWS, 8, COLS), BF),
        vmem((8, 32, COLS), BF),
        vmem((8, 32, COLS), BF),
        pltpu.SemaphoreType.DMA((22,)),
        pltpu.SemaphoreType.DMA((3,)),
        pltpu.SemaphoreType.DMA((3,)),
    ]
    return pl.pallas_call(
        kernel,
        out_shape=jax.ShapeDtypeStruct((32, WIDTH), BF),
        in_specs=[pl.BlockSpec(memory_space=pl.ANY)] * len(operands),
        out_specs=pl.BlockSpec(memory_space=pltpu.VMEM),
        scratch_shapes=scratch,
        compiler_params=pltpu.CompilerParams(
            collective_id=0, has_side_effects=True, vmem_limit_bytes=48 * 1024 * 1024
        ),
    )(*operands)


def solution(mesh):
    in_specs = (
        P("row", None),
        P(),
        P(None, "col"),
        P(None, "col"),
        P(None, "col"),
        P(None, None, "col"),
        P(None, "col"),
        P(),
        P(),
        P(),
        P(),
        P(),
        P(None, None, None, ("col", "row")),
        P(None, ("col", "row")),
        P("col"),
        P(),
    )
    out_specs = P(("row", "col"), None)
    return jax.shard_map(local, mesh=mesh, in_specs=in_specs, out_specs=out_specs, check_vma=False)
```

```python
import math

import jax
import jax.numpy as jnp
import ml_dtypes
import numpy as np
from jax import lax
from jax.experimental import pallas as pl
from jax.experimental.pallas import tpu as pltpu
from jax.sharding import PartitionSpec as P

CHANNELS = 1024
GROUPS = 8
FREQ_BANDS = 16
NORM_EPS = 1e-06
DECAY_TARGET = 0.01
FAST_SPAN = 0.3
SLOW_SPAN = 1.5

LENGTH = 8192
WIDTH = 2048
COLS = 128
LIVE = 64
HALF = 72
TOTAL = 16384
ROWS = 32
OWN = 4
FEATS = 48
CHUNK = 2048

BF = jnp.bfloat16
F32 = jnp.float32
MESH = pl.DeviceIdType.MESH


def split_np(matrix):
    high = matrix.astype(np.float32).astype(ml_dtypes.bfloat16)
    low = (matrix - high.astype(np.float64)).astype(np.float32).astype(ml_dtypes.bfloat16)
    return high, low


def make_constants():
    k1 = np.arange(HALF)
    a = np.arange(LIVE)
    b = np.arange(COLS)
    cos_in = np.cos(2 * np.pi * np.outer(k1, a) / COLS)
    sin_in = np.sin(2 * np.pi * np.outer(k1, a) / COLS)
    first = np.concatenate([cos_in, -sin_in], 0)
    turn = 2 * np.pi * np.outer(k1, b) / TOTAL
    twiddle = np.concatenate([np.cos(turn), np.sin(turn)], 1).astype(np.float32)
    cos_out = np.cos(2 * np.pi * (np.outer(b, b) % COLS) / COLS)
    sin_out = np.sin(2 * np.pi * (np.outer(b, b) % COLS) / COLS)
    second = np.block([[cos_out, -sin_out], [sin_out, cos_out]])
    back = np.block([[cos_out, sin_out], [-sin_out, cos_out]])
    weight = np.where((k1 == 0) | (k1 == COLS // 2), 1.0, 2.0) * (k1 <= COLS // 2)
    last = np.concatenate([cos_in.T * weight, -sin_in.T * weight], 1) / TOTAL
    first_h, first_l = split_np(first)
    last_h, last_l = split_np(last)
    n = np.arange(LENGTH)
    ramp = np.linspace(0.0, 1.0, LENGTH)[None, :]
    bands = np.linspace(0.0001, FREQ_BANDS - 1, FREQ_BANDS, dtype=np.float32).astype(np.float64)
    angle = bands[:, None] * (2 * np.pi * n / LENGTH)[None, :]
    feats = np.zeros((FEATS, LENGTH))
    feats[0:1] = ramp
    feats[1 : 1 + FREQ_BANDS] = np.cos(angle)
    feats[1 + FREQ_BANDS : 1 + 2 * FREQ_BANDS] = -np.sin(angle)
    feats[1 + 2 * FREQ_BANDS] = 1.0
    return dict(
        first=np.concatenate([first_h, first_l, first_h], 1),
        twiddle=twiddle,
        second=np.stack(split_np(second)),
        back=np.stack(split_np(back)),
        last=np.concatenate([last_h, last_l, last_h], 1),
        feats=np.concatenate(split_np(feats), 0),
    )


def sine_coefficients():
    v = 0.25 * np.cos(np.pi * (np.arange(400) + 0.5) / 800)
    basis = np.stack([v ** (2 * j + 1) for j in range(5)], 1)
    scale = 1.0 / np.sin(2 * np.pi * v)
    found = np.linalg.lstsq(basis * scale[:, None], np.ones_like(v), rcond=None)[0]
    return [float(c) for c in found]


SINE = sine_coefficients()


def sine_of_turns(turns):
    v = 0.25 - jnp.abs(turns - jnp.round(turns))
    square = v * v
    result = SINE[4]
    for c in SINE[3::-1]:
        result = result * square + c
    return result * v


def split(value):
    high = value.astype(BF)
    return high, (value - high.astype(F32)).astype(BF)


def dot(left, right):
    return jnp.dot(left, right, preferred_element_type=F32)


def tall(value):
    high, low = split(value)
    return jnp.concatenate([high, high, low], axis=0)


def wide(value):
    high, low = split(value)
    return jnp.concatenate([high, low, high], axis=1)


def dot_table(value, table, lo, hi):
    high, low = split(value)
    return (
        dot(high, table[0, :, lo:hi]) + dot(low, table[0, :, lo:hi]) + dot(high, table[1, :, lo:hi])
    )


def into_spectrum(signal, first, twiddle):
    part = dot(first[...], tall(signal))
    cos, sin = twiddle[:, :COLS], twiddle[:, COLS:]
    pieces = []
    for i in range(OWN):
        real = part[:HALF, i * COLS : (i + 1) * COLS]
        imag = part[HALF:, i * COLS : (i + 1) * COLS]
        pieces.append(jnp.concatenate([real * cos + imag * sin, imag * cos - real * sin], axis=1))
    return jnp.concatenate(pieces, axis=0)


def from_spectrum(spectrum, back, last, twiddle):
    part = dot_table(spectrum, back, 0, 2 * COLS)
    cos, sin = twiddle[:, :COLS], twiddle[:, COLS:]
    reals, imags = [], []
    for i in range(OWN):
        real = part[i * HALF : (i + 1) * HALF, :COLS]
        imag = part[i * HALF : (i + 1) * HALF, COLS:]
        reals.append(real * cos - imag * sin)
        imags.append(real * sin + imag * cos)
    turned = jnp.concatenate(
        [jnp.concatenate(reals, axis=1), jnp.concatenate(imags, axis=1)], axis=0
    )
    return dot(last[...], tall(turned))


def kernel(
    tokens_hbm, norm_gain_hbm, gate0_hbm, gate1_hbm, gate2_hbm, short_w_hbm, short_b_hbm,
    embed_w_hbm, embed_b_hbm, inner_w_hbm, inner_b_hbm, freq_hbm, filter_w_hbm, skip_hbm,
    out_gain_hbm, out_w_hbm, first_hbm, twiddle_hbm, second_hbm, back_hbm, last_hbm, feats_hbm,
    out_ref,
    tokens, norm_gain, gates, short_w, short_b, embed_w, embed_b, inner_w, inner_b, freq,
    filter_w, skip, out_gain, out_w, first, twiddle, second, back, last, feats,
    normed, flat, packed, send1, recv1, params, mixed_taps, spectra, smooth,
    send2, recv2, send3, recv3, load_sem, send_sems, recv_sems,
):
    me = lax.axis_index("row")
    col = lax.axis_index("col")
    n_col = 8

    barrier = pltpu.get_barrier_semaphore()

    def greet_row(k, carry):
        pl.semaphore_signal(
            barrier, inc=1, device_id=(lax.rem(me + k, ROWS), col), device_id_type=MESH
        )
        return carry

    def greet_col(k, carry):
        pl.semaphore_signal(
            barrier, inc=1, device_id=(me, lax.rem(col + k, n_col)), device_id_type=MESH
        )
        return carry

    lax.fori_loop(1, ROWS, greet_row, 0)
    lax.fori_loop(1, n_col, greet_col, 0)

    loads = [
        pltpu.make_async_copy(src, dst, load_sem.at[j])
        for j, (src, dst) in enumerate(
            [
                (tokens_hbm, tokens),
                (norm_gain_hbm, norm_gain),
                (gate0_hbm, gates.at[:, 0:128]),
                (gate1_hbm, gates.at[:, 128:256]),
                (gate2_hbm, gates.at[:, 256:384]),
                (embed_w_hbm, embed_w),
                (embed_b_hbm, embed_b),
                (inner_w_hbm, inner_w),
                (inner_b_hbm, inner_b),
                (freq_hbm, freq),
                (filter_w_hbm, filter_w),
                (feats_hbm, feats),
                (first_hbm, first),
                (twiddle_hbm, twiddle),
                (second_hbm, second),
                (short_w_hbm, short_w),
                (short_b_hbm, short_b),
                (skip_hbm, skip),
                (back_hbm, back),
                (last_hbm, last),
                (out_gain_hbm, out_gain),
                (out_w_hbm, out_w),
            ]
        )
    ]
    for load in loads:
        load.start()

    for load in loads[0:2]:
        load.wait()

    def normalise(j, carry):
        rows = pl.ds(pl.multiple_of(j * 64, 64), 64)
        wide_tokens = tokens[rows, :].astype(F32)
        mean = jnp.mean(wide_tokens * wide_tokens, axis=1, keepdims=True)
        normed[rows, :] = (wide_tokens * lax.rsqrt(mean + NORM_EPS) * norm_gain[...]).astype(BF)
        return carry

    lax.fori_loop(0, 4, normalise, 0)
    for load in loads[2:5]:
        load.wait()
    projected = dot(normed[...], gates[...])
    projected = projected.astype(BF).astype(F32).T
    for b in range(3):
        for half in range(2):
            flat[pl.ds(half * 128, 128), :] = projected[
                b * 128 : (b + 1) * 128, half * 128 : (half + 1) * 128
            ]
        for half in range(2):
            for i in range(OWN):
                packed[pl.ds(4 * half + i, ROWS, stride=8), :] = flat[
                    pl.ds(128 * half + i, ROWS, stride=4), :
                ]
        send1[:, b] = packed[...].reshape(ROWS, 8, COLS).astype(BF)

    pl.semaphore_wait(barrier, ROWS - 1 + n_col - 1)

    def row_copy(source, target, number, k):
        there = lax.rem(me + k, ROWS)
        return pltpu.make_async_remote_copy(
            src_ref=source.at[there],
            dst_ref=target.at[me],
            send_sem=send_sems.at[number],
            recv_sem=recv_sems.at[number],
            device_id=(there, col),
            device_id_type=MESH,
        )

    def send_out(k, carry):
        row_copy(send1, recv1, 0, k).start()
        return carry

    lax.fori_loop(1, ROWS, send_out, 0)
    recv1[me] = send1[me]

    for load in loads[5:15]:
        load.wait()
    params[...] = jnp.zeros_like(params)
    scale = freq[...] * (1.0 / (2.0 * math.pi))
    params[0:33, 0:64] = embed_w[...] * scale
    params[33:34, 0:64] = embed_b[...] * scale - 0.25
    params[48:49, 0:64] = inner_b[...] * scale - 0.25
    params[64:128, 0:64] = inner_w[...] * scale
    turned = params[...].T
    embed_t = wide(turned[0:64, 0:FEATS])
    inner_bias = turned[0:64, 48:49]
    inner_t = wide(turned[0:64, 64:128])
    filter_t = wide(
        jnp.concatenate([filter_w[o, e] for o in range(2) for e in range(2)], axis=0)
    )

    row8 = lax.broadcasted_iota(jnp.int32, (8, 1), 0)
    channel = (col * ROWS + me) * OWN + lax.rem(row8, OWN)
    fastest = math.log(DECAY_TARGET) / FAST_SPAN
    slowest = math.log(DECAY_TARGET) / SLOW_SPAN
    place = channel.astype(F32) * (1.0 / (CHANNELS - 1))
    decay = jnp.abs(slowest * (1.0 - place) + fastest * place)

    def taps_of(j, carry):
        start = pl.multiple_of(j * CHUNK, CHUNK)
        lanes = pl.ds(start, CHUNK)
        high, low = feats[0:FEATS, lanes], feats[FEATS:, lanes]
        hidden = sine_of_turns(dot(embed_t, jnp.concatenate([high, high, low], axis=0)))
        hidden = sine_of_turns(dot(inner_t, tall(hidden)) + inner_bias)
        taps = dot(filter_t, tall(hidden))
        lag = start + lax.broadcasted_iota(jnp.int32, (8, CHUNK), 1)
        row = lax.broadcasted_iota(jnp.int32, (8, CHUNK), 0)
        window = jnp.exp(-(lag.astype(F32) * (1.0 / (LENGTH - 1))) * decay)
        window = jnp.where((lag == 0) & (row >= OWN), 0.0, window)
        for o in range(2):
            both = taps[8 * o : 8 * o + 8] * window
            other = pltpu.roll(both, OWN, axis=0)
            both = jnp.where(row < OWN, both + other, other - both)
            for q in range(CHUNK // COLS):
                at = pl.multiple_of(start // COLS * 8, 8) + o * LIVE * 8 + q * 8
                mixed_taps[pl.ds(pl.multiple_of(at, 8), 8), :] = both[:, q * COLS : (q + 1) * COLS]
        return carry

    lax.fori_loop(0, LENGTH // CHUNK, taps_of, 0)
    for o in range(2):
        for part in range(2):
            signal = jnp.concatenate(
                [
                    mixed_taps[pl.ds(o * LIVE * 8 + part * OWN + i, LIVE, stride=8), :]
                    for i in range(OWN)
                ],
                axis=1,
            )
            spectra[o, :, part * COLS : (part + 1) * COLS] = dot_table(
                into_spectrum(signal, first, twiddle), second, part * COLS, (part + 1) * COLS
            )

    for load in loads[15:21]:
        load.wait()
    lane8 = lax.broadcasted_iota(jnp.int32, (8, COLS), 1)
    mine = lane8 == OWN * me + lax.rem(lax.broadcasted_iota(jnp.int32, (8, COLS), 0), OWN)

    def own_column(line):
        return jnp.sum(
            jnp.where(mine, jnp.broadcast_to(line, (8, COLS)), 0.0), axis=1, keepdims=True
        )

    all_short = short_w[...].astype(F32)
    columns = [
        [own_column(all_short[b, j : j + 1]) for j in range(3)] + [own_column(short_b[b : b + 1, :])]
        for b in range(3)
    ]

    def wait_row(target, number):
        pltpu.make_async_copy(
            target.at[pl.ds(0, ROWS - 1)], target.at[pl.ds(0, ROWS - 1)], recv_sems.at[number]
        ).wait()

    wait_row(recv1, 0)
    row = lax.broadcasted_iota(jnp.int32, (256, COLS), 0)
    lane = lax.broadcasted_iota(jnp.int32, (256, COLS), 1)
    smoothed = []
    for b in range(3):
        here = recv1[:, b].astype(F32).reshape(256, COLS)
        before = pltpu.roll(here, 1, axis=1)
        before = jnp.where(lane == 0, pltpu.roll(before, OWN, axis=0), before)
        before = jnp.where((lane == 0) & (row < OWN), 0.0, before)
        after = pltpu.roll(here, COLS - 1, axis=1)
        after = jnp.where(lane == COLS - 1, pltpu.roll(after, 256 - OWN, axis=0), after)
        after = jnp.where((lane == COLS - 1) & (row >= 256 - OWN), 0.0, after)
        tap = [jnp.broadcast_to(c, (8, COLS))[None] for c in columns[b]]
        shape = (ROWS, 8, COLS)
        value = tap[3] + before.reshape(shape) * tap[0]
        value = value + here.reshape(shape) * tap[1]
        value = value + after.reshape(shape) * tap[2]
        smooth[b] = value.reshape(256, COLS)
        smoothed.append(
            jnp.concatenate(
                [smooth[b, pl.ds(i, LIVE, stride=OWN), :] for i in range(OWN)], axis=1
            )
        )

    signal = smoothed[2]
    for o in range(2):
        spectrum = dot_table(into_spectrum(signal, first, twiddle), second, 0, 2 * COLS)
        real, imag = spectrum[:, :COLS], spectrum[:, COLS:]
        t_real, t_imag = spectra[o, :, :COLS], spectra[o, :, COLS:]
        product = jnp.concatenate(
            [real * t_real - imag * t_imag, real * t_imag + imag * t_real], axis=1
        )
        direct = jnp.concatenate(
            [
                signal[:, i * COLS : (i + 1) * COLS]
                * jnp.broadcast_to(skip[o : o + 1, i : i + 1], (LIVE, COLS))
                for i in range(OWN)
            ],
            axis=1,
        )
        signal = smoothed[o] * (from_spectrum(product, back, last, twiddle) + direct)

    for i in range(OWN):
        flat[pl.ds(i * LIVE, LIVE), :] = signal[:, i * COLS : (i + 1) * COLS]
    for i in range(OWN):
        for half in range(2):
            packed[pl.ds(2 * i + half, ROWS, stride=8), :] = flat[
                pl.ds(i * LIVE + half, ROWS, stride=2), :
            ]
    send2[...] = packed[...].reshape(ROWS, 8, COLS).astype(BF)

    def send_back(k, carry):
        row_copy(send2, recv2, 1, k).start()
        return carry

    lax.fori_loop(1, ROWS, send_back, 0)
    recv2[me] = send2[me]
    wait_row(recv2, 1)

    values = recv2[...].astype(F32)
    squares = jnp.sum(values * values, axis=0)
    squares = squares + pltpu.roll(squares, 4, axis=0)
    squares = squares + pltpu.roll(squares, 2, axis=0)
    factor = lax.rsqrt(squares * (GROUPS / CHANNELS) + NORM_EPS)
    flat[...] = (values * factor[None]).reshape(256, COLS)
    for half in range(2):
        turned = flat[pl.ds(half, COLS, stride=2), :].T * out_gain[...]
        send3[4 * half : 4 * half + 4] = turned.reshape(4, 32, COLS).astype(BF)

    def send_over(k, carry):
        there = lax.rem(col + k, n_col)
        pltpu.make_async_remote_copy(
            src_ref=send3.at[there],
            dst_ref=recv3.at[col],
            send_sem=send_sems.at[2],
            recv_sem=recv_sems.at[2],
            device_id=(me, there),
            device_id_type=MESH,
        ).start()
        return carry

    lax.fori_loop(1, n_col, send_over, 0)
    recv3[col] = send3[col]
    loads[21].wait()
    pltpu.make_async_copy(
        recv3.at[pl.ds(0, n_col - 1)], recv3.at[pl.ds(0, n_col - 1)], recv_sems.at[2]
    ).wait()
    mixed = jnp.concatenate([recv3[c] for c in range(n_col)], axis=1)
    for q in range(4):
        out_ref[:, q * 512 : (q + 1) * 512] = dot(mixed, out_w[:, q * 512 : (q + 1) * 512]).astype(
            BF
        )

    for number, source in ((0, send1), (1, send2)):
        pltpu.make_async_copy(
            source.at[pl.ds(0, ROWS - 1)], source.at[pl.ds(0, ROWS - 1)], send_sems.at[number]
        ).wait()
    pltpu.make_async_copy(
        send3.at[pl.ds(0, n_col - 1)], send3.at[pl.ds(0, n_col - 1)], send_sems.at[2]
    ).wait()


def local(
    tokens, norm_gain, first_gate, second_gate, value_weight, short_weight, short_bias,
    embed_weight, embed_bias, inner_weight, inner_bias, filter_freq, filter_weight, filter_skip,
    output_gain, output_weight,
):
    constants = make_constants()
    operands = [
        tokens, norm_gain[None], first_gate, second_gate, value_weight, short_weight, short_bias,
        embed_weight, embed_bias[None], inner_weight, inner_bias[None], filter_freq[None],
        jnp.swapaxes(filter_weight, 2, 3), filter_skip, output_gain[None], output_weight,
    ] + [
        jnp.asarray(constants[name])
        for name in ("first", "twiddle", "second", "back", "last", "feats")
    ]
    vmem = pltpu.VMEM
    scratch = (
        [vmem(x.shape, x.dtype) for x in operands[0:2]]
        + [vmem((WIDTH, 384), BF)]
        + [vmem(x.shape, x.dtype) for x in operands[5:]]
    )
    scratch += [
        vmem((256, WIDTH), BF),
        vmem((256, COLS), F32),
        vmem((256, COLS), F32),
        vmem((ROWS, 3, 8, COLS), BF),
        vmem((ROWS, 3, 8, COLS), BF),
        vmem((128, 128), F32),
        vmem((2 * LIVE * 8, COLS), F32),
        vmem((2, OWN * HALF, 2 * COLS), F32),
        vmem((3, 256, COLS), F32),
        vmem((ROWS, 8, COLS), BF),
        vmem((ROWS, 8, COLS), BF),
        vmem((8, 32, COLS), BF),
        vmem((8, 32, COLS), BF),
        pltpu.SemaphoreType.DMA((22,)),
        pltpu.SemaphoreType.DMA((3,)),
        pltpu.SemaphoreType.DMA((3,)),
    ]
    return pl.pallas_call(
        kernel,
        out_shape=jax.ShapeDtypeStruct((32, WIDTH), BF),
        in_specs=[pl.BlockSpec(memory_space=pltpu.HBM)] * len(operands),
        out_specs=pl.BlockSpec(memory_space=pltpu.VMEM),
        scratch_shapes=scratch,
        compiler_params=pltpu.CompilerParams(
            collective_id=0, has_side_effects=True, vmem_limit_bytes=67_043_328
        ),
    )(*operands)


def solution(mesh):
    in_specs = (
        P("row", None),
        P(),
        P(None, "col"),
        P(None, "col"),
        P(None, "col"),
        P(None, None, "col"),
        P(None, "col"),
        P(),
        P(),
        P(),
        P(),
        P(),
        P(None, None, None, ("col", "row")),
        P(None, ("col", "row")),
        P("col"),
        P(),
    )
    out_specs = P(("row", "col"), None)
    return jax.shard_map(local, mesh=mesh, in_specs=in_specs, out_specs=out_specs, check_vma=False)
```

```python
import math

import jax
import jax.numpy as jnp
import ml_dtypes
import numpy as np
from jax import lax
from jax.experimental import pallas as pl
from jax.experimental.pallas import tpu as pltpu
from jax.sharding import PartitionSpec as P

CHANNELS = 1024
GROUPS = 8
FREQ_BANDS = 16
NORM_EPS = 1e-06
DECAY_TARGET = 0.01
FAST_SPAN = 0.3
SLOW_SPAN = 1.5

LENGTH = 8192
WIDTH = 2048
COLS = 128
LIVE = 64
HALF = 72
TOTAL = 16384
ROWS = 32
OWN = 4
FEATS = 48
CHUNK = 2048


def farthest_first(steps):
    return [offset for _, offset in sorted(steps, reverse=True) if any(offset)]


FAR_ROWS = farthest_first(
    [(min(dz, 8 - dz) + min(dx, 4 - dx), (dz, dx)) for dz in range(8) for dx in range(4)]
)
FAR_COLS = farthest_first(
    [(2 * min(dy, 4 - dy) + dc, (dy, dc)) for dy in range(4) for dc in range(2)]
)

BF = jnp.bfloat16
F32 = jnp.float32
MESH = pl.DeviceIdType.MESH


def split_np(matrix):
    high = matrix.astype(np.float32).astype(ml_dtypes.bfloat16)
    low = (matrix - high.astype(np.float64)).astype(np.float32).astype(ml_dtypes.bfloat16)
    return high, low


def make_constants():
    k1 = np.arange(HALF)
    a = np.arange(LIVE)
    b = np.arange(COLS)
    cos_in = np.cos(2 * np.pi * np.outer(k1, a) / COLS)
    sin_in = np.sin(2 * np.pi * np.outer(k1, a) / COLS)
    first = np.concatenate([cos_in, -sin_in], 0)
    turn = 2 * np.pi * np.outer(k1, b) / TOTAL
    twiddle = np.concatenate([np.cos(turn), np.sin(turn)], 1).astype(np.float32)
    cos_out = np.cos(2 * np.pi * (np.outer(b, b) % COLS) / COLS)
    sin_out = np.sin(2 * np.pi * (np.outer(b, b) % COLS) / COLS)
    second = np.block([[cos_out, -sin_out], [sin_out, cos_out]])
    back = np.block([[cos_out, sin_out], [-sin_out, cos_out]])
    weight = np.where((k1 == 0) | (k1 == COLS // 2), 1.0, 2.0) * (k1 <= COLS // 2)
    last = np.concatenate([cos_in.T * weight, -sin_in.T * weight], 1) / TOTAL
    first_h, first_l = split_np(first)
    last_h, last_l = split_np(last)
    n = np.arange(LENGTH)
    ramp = np.linspace(0.0, 1.0, LENGTH)[None, :]
    bands = np.linspace(0.0001, FREQ_BANDS - 1, FREQ_BANDS, dtype=np.float32).astype(np.float64)
    angle = bands[:, None] * (2 * np.pi * n / LENGTH)[None, :]
    feats = np.zeros((FEATS, LENGTH))
    feats[0:1] = ramp
    feats[1 : 1 + FREQ_BANDS] = np.cos(angle)
    feats[1 + FREQ_BANDS : 1 + 2 * FREQ_BANDS] = -np.sin(angle)
    feats[1 + 2 * FREQ_BANDS] = 1.0
    return dict(
        first=np.concatenate([first_h, first_l, first_h], 1),
        twiddle=twiddle,
        second=np.stack(split_np(second)),
        back=np.stack(split_np(back)),
        last=np.concatenate([last_h, last_l, last_h], 1),
        feats=np.concatenate(split_np(feats), 0),
    )


def sine_coefficients():
    v = 0.25 * np.cos(np.pi * (np.arange(400) + 0.5) / 800)
    basis = np.stack([v ** (2 * j + 1) for j in range(5)], 1)
    scale = 1.0 / np.sin(2 * np.pi * v)
    found = np.linalg.lstsq(basis * scale[:, None], np.ones_like(v), rcond=None)[0]
    return [float(c) for c in found]


SINE = sine_coefficients()


def sine_of_turns(turns):
    v = 0.25 - jnp.abs(turns - jnp.round(turns))
    square = v * v
    result = SINE[4]
    for c in SINE[3::-1]:
        result = result * square + c
    return result * v


def split(value):
    high = value.astype(BF)
    return high, (value - high.astype(F32)).astype(BF)


def dot(left, right):
    return jnp.dot(left, right, preferred_element_type=F32)


def tall(value):
    high, low = split(value)
    return jnp.concatenate([high, high, low], axis=0)


def wide(value):
    high, low = split(value)
    return jnp.concatenate([high, low, high], axis=1)


def dot_table(value, table, lo, hi):
    high, low = split(value)
    return (
        dot(high, table[0, :, lo:hi]) + dot(low, table[0, :, lo:hi]) + dot(high, table[1, :, lo:hi])
    )


def into_spectrum(signal, first, twiddle):
    part = dot(first[...], tall(signal))
    cos, sin = twiddle[:, :COLS], twiddle[:, COLS:]
    pieces = []
    for i in range(OWN):
        real = part[:HALF, i * COLS : (i + 1) * COLS]
        imag = part[HALF:, i * COLS : (i + 1) * COLS]
        pieces.append(jnp.concatenate([real * cos + imag * sin, imag * cos - real * sin], axis=1))
    return jnp.concatenate(pieces, axis=0)


def from_spectrum(spectrum, back, last, twiddle):
    part = dot_table(spectrum, back, 0, 2 * COLS)
    cos, sin = twiddle[:, :COLS], twiddle[:, COLS:]
    reals, imags = [], []
    for i in range(OWN):
        real = part[i * HALF : (i + 1) * HALF, :COLS]
        imag = part[i * HALF : (i + 1) * HALF, COLS:]
        reals.append(real * cos - imag * sin)
        imags.append(real * sin + imag * cos)
    turned = jnp.concatenate(
        [jnp.concatenate(reals, axis=1), jnp.concatenate(imags, axis=1)], axis=0
    )
    return dot(last[...], tall(turned))


def kernel(
    tokens_hbm, norm_gain_hbm, gate0_hbm, gate1_hbm, gate2_hbm, short_w_hbm, short_b_hbm,
    embed_w_hbm, embed_b_hbm, inner_w_hbm, inner_b_hbm, freq_hbm, filter_w_hbm, skip_hbm,
    out_gain_hbm, out_w_hbm, first_hbm, twiddle_hbm, second_hbm, back_hbm, last_hbm, feats_hbm,
    out_ref,
    tokens, norm_gain, gates, short_w, short_b, embed_w, embed_b, inner_w, inner_b, freq,
    filter_w, skip, out_gain, out_w, first, twiddle, second, back, last, feats,
    normed, flat, packed, send1, recv1, params, mixed_taps, spectra, smooth,
    send2, recv2, send3, recv3, load_sem, send_sems, recv_sems,
):
    me = lax.axis_index("row")
    col = lax.axis_index("col")
    n_col = 8

    barrier = pltpu.get_barrier_semaphore()

    z, x = lax.div(me, 4), lax.rem(me, 4)
    row_peers = [lax.rem(z + dz, 8) * 4 + lax.rem(x + dx, 4) for dz, dx in FAR_ROWS]
    y, core = lax.div(col, 2), lax.rem(col, 2)
    col_peers = [lax.rem(y + dy, 4) * 2 + lax.rem(core + dc, 2) for dy, dc in FAR_COLS]
    for there in row_peers:
        pl.semaphore_signal(barrier, inc=1, device_id=(there, col), device_id_type=MESH)
    for there in col_peers:
        pl.semaphore_signal(barrier, inc=1, device_id=(me, there), device_id_type=MESH)

    loads = [
        pltpu.make_async_copy(src, dst, load_sem.at[j])
        for j, (src, dst) in enumerate(
            [
                (tokens_hbm, tokens),
                (norm_gain_hbm, norm_gain),
                (gate0_hbm, gates.at[:, 0:128]),
                (gate1_hbm, gates.at[:, 128:256]),
                (gate2_hbm, gates.at[:, 256:384]),
                (embed_w_hbm, embed_w),
                (embed_b_hbm, embed_b),
                (inner_w_hbm, inner_w),
                (inner_b_hbm, inner_b),
                (freq_hbm, freq),
                (filter_w_hbm, filter_w),
                (feats_hbm, feats),
                (first_hbm, first),
                (twiddle_hbm, twiddle),
                (second_hbm, second),
                (short_w_hbm, short_w),
                (short_b_hbm, short_b),
                (skip_hbm, skip),
                (back_hbm, back),
                (last_hbm, last),
                (out_gain_hbm, out_gain),
                (out_w_hbm, out_w),
            ]
        )
    ]
    for load in loads:
        load.start()

    for load in loads[0:2]:
        load.wait()

    def normalise(j, carry):
        rows = pl.ds(pl.multiple_of(j * 64, 64), 64)
        wide_tokens = tokens[rows, :].astype(F32)
        mean = jnp.mean(wide_tokens * wide_tokens, axis=1, keepdims=True)
        normed[rows, :] = (wide_tokens * lax.rsqrt(mean + NORM_EPS) * norm_gain[...]).astype(BF)
        return carry

    lax.fori_loop(0, 4, normalise, 0)
    for load in loads[2:5]:
        load.wait()
    projected = dot(normed[...], gates[...])
    projected = projected.astype(BF).astype(F32).T
    for b in range(3):
        for half in range(2):
            flat[pl.ds(half * 128, 128), :] = projected[
                b * 128 : (b + 1) * 128, half * 128 : (half + 1) * 128
            ]
        for half in range(2):
            for i in range(OWN):
                packed[pl.ds(4 * half + i, ROWS, stride=8), :] = flat[
                    pl.ds(128 * half + i, ROWS, stride=4), :
                ]
        send1[b] = packed[...].reshape(ROWS, 8, COLS).astype(BF)

    pl.semaphore_wait(barrier, ROWS - 1 + n_col - 1)

    def send_rows(source, target, number):
        for there in row_peers:
            pltpu.make_async_remote_copy(
                src_ref=source.at[there],
                dst_ref=target.at[me],
                send_sem=send_sems.at[number],
                recv_sem=recv_sems.at[number],
                device_id=(there, col),
                device_id_type=MESH,
            ).start()
        target[me] = source[me]

    for b in (2, 0, 1):
        send_rows(send1.at[b], recv1.at[b], b)

    for load in loads[5:15]:
        load.wait()
    params[...] = jnp.zeros_like(params)
    scale = freq[...] * (1.0 / (2.0 * math.pi))
    params[0:33, 0:64] = embed_w[...] * scale
    params[33:34, 0:64] = embed_b[...] * scale - 0.25
    params[48:49, 0:64] = inner_b[...] * scale - 0.25
    params[64:128, 0:64] = inner_w[...] * scale
    turned = params[...].T
    embed_t = wide(turned[0:64, 0:FEATS])
    inner_bias = turned[0:64, 48:49]
    inner_t = wide(turned[0:64, 64:128])
    filter_t = wide(
        jnp.concatenate([filter_w[o, e] for o in range(2) for e in range(2)], axis=0)
    )

    row8 = lax.broadcasted_iota(jnp.int32, (8, 1), 0)
    channel = (col * ROWS + me) * OWN + lax.rem(row8, OWN)
    fastest = math.log(DECAY_TARGET) / FAST_SPAN
    slowest = math.log(DECAY_TARGET) / SLOW_SPAN
    place = channel.astype(F32) * (1.0 / (CHANNELS - 1))
    decay = jnp.abs(slowest * (1.0 - place) + fastest * place)

    def taps_of(j, carry):
        start = pl.multiple_of(j * CHUNK, CHUNK)
        lanes = pl.ds(start, CHUNK)
        high, low = feats[0:FEATS, lanes], feats[FEATS:, lanes]
        hidden = sine_of_turns(dot(embed_t, jnp.concatenate([high, high, low], axis=0)))
        hidden = sine_of_turns(dot(inner_t, tall(hidden)) + inner_bias)
        taps = dot(filter_t, tall(hidden))
        lag = start + lax.broadcasted_iota(jnp.int32, (8, CHUNK), 1)
        row = lax.broadcasted_iota(jnp.int32, (8, CHUNK), 0)
        window = jnp.exp(-(lag.astype(F32) * (1.0 / (LENGTH - 1))) * decay)
        window = jnp.where((lag == 0) & (row >= OWN), 0.0, window)
        for o in range(2):
            both = taps[8 * o : 8 * o + 8] * window
            other = pltpu.roll(both, OWN, axis=0)
            both = jnp.where(row < OWN, both + other, other - both)
            for q in range(CHUNK // COLS):
                at = pl.multiple_of(start // COLS * 8, 8) + o * LIVE * 8 + q * 8
                mixed_taps[pl.ds(pl.multiple_of(at, 8), 8), :] = both[:, q * COLS : (q + 1) * COLS]
        return carry

    lax.fori_loop(0, LENGTH // CHUNK, taps_of, 0)
    for o in range(2):
        for part in range(2):
            signal = jnp.concatenate(
                [
                    mixed_taps[pl.ds(o * LIVE * 8 + part * OWN + i, LIVE, stride=8), :]
                    for i in range(OWN)
                ],
                axis=1,
            )
            spectra[o, :, part * COLS : (part + 1) * COLS] = dot_table(
                into_spectrum(signal, first, twiddle), second, part * COLS, (part + 1) * COLS
            )

    for load in loads[15:21]:
        load.wait()
    lane8 = lax.broadcasted_iota(jnp.int32, (8, COLS), 1)
    mine = lane8 == OWN * me + lax.rem(lax.broadcasted_iota(jnp.int32, (8, COLS), 0), OWN)

    def own_column(line):
        return jnp.sum(
            jnp.where(mine, jnp.broadcast_to(line, (8, COLS)), 0.0), axis=1, keepdims=True
        )

    all_short = short_w[...].astype(F32)
    columns = [
        [own_column(all_short[b, j : j + 1]) for j in range(3)] + [own_column(short_b[b : b + 1, :])]
        for b in range(3)
    ]

    def wait_row(target, number):
        pltpu.make_async_copy(
            target.at[pl.ds(0, ROWS - 1)], target.at[pl.ds(0, ROWS - 1)], recv_sems.at[number]
        ).wait()

    row = lax.broadcasted_iota(jnp.int32, (256, COLS), 0)
    lane = lax.broadcasted_iota(jnp.int32, (256, COLS), 1)

    def smoothed(b):
        wait_row(recv1.at[b], b)
        here = recv1[b].astype(F32).reshape(256, COLS)
        before = pltpu.roll(here, 1, axis=1)
        before = jnp.where(lane == 0, pltpu.roll(before, OWN, axis=0), before)
        before = jnp.where((lane == 0) & (row < OWN), 0.0, before)
        after = pltpu.roll(here, COLS - 1, axis=1)
        after = jnp.where(lane == COLS - 1, pltpu.roll(after, 256 - OWN, axis=0), after)
        after = jnp.where((lane == COLS - 1) & (row >= 256 - OWN), 0.0, after)
        tap = [jnp.broadcast_to(c, (8, COLS))[None] for c in columns[b]]
        shape = (ROWS, 8, COLS)
        value = tap[3] + before.reshape(shape) * tap[0]
        value = value + here.reshape(shape) * tap[1]
        value = value + after.reshape(shape) * tap[2]
        smooth[b] = value.reshape(256, COLS)
        return jnp.concatenate(
            [smooth[b, pl.ds(i, LIVE, stride=OWN), :] for i in range(OWN)], axis=1
        )

    signal = smoothed(2)
    for o in range(2):
        spectrum = dot_table(into_spectrum(signal, first, twiddle), second, 0, 2 * COLS)
        real, imag = spectrum[:, :COLS], spectrum[:, COLS:]
        t_real, t_imag = spectra[o, :, :COLS], spectra[o, :, COLS:]
        product = jnp.concatenate(
            [real * t_real - imag * t_imag, real * t_imag + imag * t_real], axis=1
        )
        direct = jnp.concatenate(
            [
                signal[:, i * COLS : (i + 1) * COLS]
                * jnp.broadcast_to(skip[o : o + 1, i : i + 1], (LIVE, COLS))
                for i in range(OWN)
            ],
            axis=1,
        )
        signal = from_spectrum(product, back, last, twiddle) + direct
        signal = signal * smoothed(o)

    for i in range(OWN):
        flat[pl.ds(i * LIVE, LIVE), :] = signal[:, i * COLS : (i + 1) * COLS]
    for i in range(OWN):
        for half in range(2):
            packed[pl.ds(2 * i + half, ROWS, stride=8), :] = flat[
                pl.ds(i * LIVE + half, ROWS, stride=2), :
            ]
    send2[...] = packed[...].reshape(ROWS, 8, COLS).astype(BF)

    send_rows(send2, recv2, 3)
    wait_row(recv2, 3)

    values = recv2[...].astype(F32)
    squares = jnp.sum(values * values, axis=0)
    squares = squares + pltpu.roll(squares, 4, axis=0)
    squares = squares + pltpu.roll(squares, 2, axis=0)
    factor = lax.rsqrt(squares * (GROUPS / CHANNELS) + NORM_EPS)
    flat[...] = (values * factor[None]).reshape(256, COLS)
    for half in range(2):
        turned = flat[pl.ds(half, COLS, stride=2), :].T * out_gain[...]
        send3[4 * half : 4 * half + 4] = turned.reshape(4, 32, COLS).astype(BF)

    for there in col_peers:
        pltpu.make_async_remote_copy(
            src_ref=send3.at[there],
            dst_ref=recv3.at[col],
            send_sem=send_sems.at[4],
            recv_sem=recv_sems.at[4],
            device_id=(me, there),
            device_id_type=MESH,
        ).start()
    recv3[col] = send3[col]
    loads[21].wait()
    pltpu.make_async_copy(
        recv3.at[pl.ds(0, n_col - 1)], recv3.at[pl.ds(0, n_col - 1)], recv_sems.at[4]
    ).wait()
    mixed = jnp.concatenate([recv3[c] for c in range(n_col)], axis=1)
    for q in range(4):
        out_ref[:, q * 512 : (q + 1) * 512] = dot(mixed, out_w[:, q * 512 : (q + 1) * 512]).astype(
            BF
        )

    for number in range(4):
        source = send1.at[number] if number < 3 else send2
        pltpu.make_async_copy(
            source.at[pl.ds(0, ROWS - 1)], source.at[pl.ds(0, ROWS - 1)], send_sems.at[number]
        ).wait()
    pltpu.make_async_copy(
        send3.at[pl.ds(0, n_col - 1)], send3.at[pl.ds(0, n_col - 1)], send_sems.at[4]
    ).wait()


def local(
    tokens, norm_gain, first_gate, second_gate, value_weight, short_weight, short_bias,
    embed_weight, embed_bias, inner_weight, inner_bias, filter_freq, filter_weight, filter_skip,
    output_gain, output_weight,
):
    constants = make_constants()
    operands = [
        tokens, norm_gain[None], first_gate, second_gate, value_weight, short_weight, short_bias,
        embed_weight, embed_bias[None], inner_weight, inner_bias[None], filter_freq[None],
        jnp.swapaxes(filter_weight, 2, 3), filter_skip, output_gain[None], output_weight,
    ] + [
        jnp.asarray(constants[name])
        for name in ("first", "twiddle", "second", "back", "last", "feats")
    ]
    vmem = pltpu.VMEM
    scratch = (
        [vmem(x.shape, x.dtype) for x in operands[0:2]]
        + [vmem((WIDTH, 384), BF)]
        + [vmem(x.shape, x.dtype) for x in operands[5:]]
    )
    scratch += [
        vmem((256, WIDTH), BF),
        vmem((256, COLS), F32),
        vmem((256, COLS), F32),
        vmem((3, ROWS, 8, COLS), BF),
        vmem((3, ROWS, 8, COLS), BF),
        vmem((128, 128), F32),
        vmem((2 * LIVE * 8, COLS), F32),
        vmem((2, OWN * HALF, 2 * COLS), F32),
        vmem((3, 256, COLS), F32),
        vmem((ROWS, 8, COLS), BF),
        vmem((ROWS, 8, COLS), BF),
        vmem((8, 32, COLS), BF),
        vmem((8, 32, COLS), BF),
        pltpu.SemaphoreType.DMA((22,)),
        pltpu.SemaphoreType.DMA((5,)),
        pltpu.SemaphoreType.DMA((5,)),
    ]
    return pl.pallas_call(
        kernel,
        out_shape=pltpu.VMEM((32, WIDTH), BF),
        in_specs=[pl.BlockSpec(memory_space=pltpu.HBM)] * len(operands),
        out_specs=pl.BlockSpec(memory_space=pltpu.VMEM),
        scratch_shapes=scratch,
        compiler_params=pltpu.CompilerParams(
            collective_id=0, has_side_effects=True, vmem_limit_bytes=66_912_256
        ),
    )(*operands)


def solution(mesh):
    in_specs = (
        P("row", None),
        P(),
        P(None, "col"),
        P(None, "col"),
        P(None, "col"),
        P(None, None, "col"),
        P(None, "col"),
        P(),
        P(),
        P(),
        P(),
        P(),
        P(None, None, None, ("col", "row")),
        P(None, ("col", "row")),
        P("col"),
        P(),
    )
    out_specs = P(("row", "col"), None)
    return jax.shard_map(local, mesh=mesh, in_specs=in_specs, out_specs=out_specs, check_vma=False)
```

```python
import math

import jax
import jax.numpy as jnp
import ml_dtypes
import numpy as np
from jax import lax
from jax.experimental import pallas as pl
from jax.experimental.pallas import tpu as pltpu
from jax.sharding import PartitionSpec as P

CHANNELS = 1024
GROUPS = 8
FREQ_BANDS = 16
NORM_EPS = 1e-06
DECAY_TARGET = 0.01
FAST_SPAN = 0.3
SLOW_SPAN = 1.5

LENGTH = 8192
WIDTH = 2048
COLS = 128
LIVE = 64
HALF = 72
TOTAL = 16384
ROWS = 32
OWN = 4
FEATS = 48
CHUNK = 2048


def farthest_first(steps):
    return [offset for _, offset in sorted(steps, reverse=True) if any(offset)]


FAR_ROWS = farthest_first(
    [(min(dz, 8 - dz) + min(dx, 4 - dx), (dz, dx)) for dz in range(8) for dx in range(4)]
)
FAR_COLS = farthest_first(
    [(2 * min(dy, 4 - dy) + dc, (dy, dc)) for dy in range(4) for dc in range(2)]
)

BF = jnp.bfloat16
F32 = jnp.float32
MESH = pl.DeviceIdType.MESH


def split_np(matrix):
    high = matrix.astype(np.float32).astype(ml_dtypes.bfloat16)
    low = (matrix - high.astype(np.float64)).astype(np.float32).astype(ml_dtypes.bfloat16)
    return high, low


def make_constants():
    k1 = np.arange(HALF)
    a = np.arange(LIVE)
    b = np.arange(COLS)
    cos_in = np.cos(2 * np.pi * np.outer(k1, a) / COLS)
    sin_in = np.sin(2 * np.pi * np.outer(k1, a) / COLS)
    first = np.concatenate([cos_in, -sin_in], 0)
    turn = 2 * np.pi * np.outer(k1, b) / TOTAL
    twiddle = np.concatenate([np.cos(turn), np.sin(turn)], 1).astype(np.float32)
    cos_out = np.cos(2 * np.pi * (np.outer(b, b) % COLS) / COLS)
    sin_out = np.sin(2 * np.pi * (np.outer(b, b) % COLS) / COLS)
    second = np.block([[cos_out, -sin_out], [sin_out, cos_out]])
    back = np.block([[cos_out, sin_out], [-sin_out, cos_out]])
    weight = np.where((k1 == 0) | (k1 == COLS // 2), 1.0, 2.0) * (k1 <= COLS // 2)
    last = np.concatenate([cos_in.T * weight, -sin_in.T * weight], 1) / TOTAL
    first_h, first_l = split_np(first)
    last_h, last_l = split_np(last)
    n = np.arange(LENGTH)
    ramp = np.linspace(0.0, 1.0, LENGTH)[None, :]
    bands = np.linspace(0.0001, FREQ_BANDS - 1, FREQ_BANDS, dtype=np.float32).astype(np.float64)
    angle = bands[:, None] * (2 * np.pi * n / LENGTH)[None, :]
    feats = np.zeros((FEATS, LENGTH))
    feats[0:1] = ramp
    feats[1 : 1 + FREQ_BANDS] = np.cos(angle)
    feats[1 + FREQ_BANDS : 1 + 2 * FREQ_BANDS] = -np.sin(angle)
    feats[1 + 2 * FREQ_BANDS] = 1.0
    return dict(
        first=np.concatenate([first_h, first_l, first_h], 1),
        twiddle=twiddle,
        second=np.stack(split_np(second)),
        back=np.stack(split_np(back)),
        last=np.concatenate([last_h, last_l, last_h], 1),
        feats=np.concatenate(split_np(feats), 0),
    )


def sine_coefficients():
    v = 0.25 * np.cos(np.pi * (np.arange(400) + 0.5) / 800)
    basis = np.stack([v ** (2 * j + 1) for j in range(5)], 1)
    scale = 1.0 / np.sin(2 * np.pi * v)
    found = np.linalg.lstsq(basis * scale[:, None], np.ones_like(v), rcond=None)[0]
    return [float(c) for c in found]


SINE = sine_coefficients()


def sine_of_turns(turns):
    v = 0.25 - jnp.abs(turns - jnp.round(turns))
    square = v * v
    result = SINE[4]
    for c in SINE[3::-1]:
        result = result * square + c
    return result * v


def split(value):
    high = value.astype(BF)
    return high, (value - high.astype(F32)).astype(BF)


def dot(left, right):
    return jnp.dot(left, right, preferred_element_type=F32)


def tall(value):
    high, low = split(value)
    return jnp.concatenate([high, high, low], axis=0)


def wide(value):
    high, low = split(value)
    return jnp.concatenate([high, low, high], axis=1)


def dot_table(value, table, lo, hi):
    high, low = split(value)
    return dot(high, table[0, :, lo:hi])


def into_spectrum(signal, first, twiddle):
    part = dot(first[...], tall(signal))
    cos, sin = twiddle[:, :COLS], twiddle[:, COLS:]
    pieces = []
    for i in range(OWN):
        real = part[:HALF, i * COLS : (i + 1) * COLS]
        imag = part[HALF:, i * COLS : (i + 1) * COLS]
        pieces.append(jnp.concatenate([real * cos + imag * sin, imag * cos - real * sin], axis=1))
    return jnp.concatenate(pieces, axis=0)


def from_spectrum(spectrum, back, last, twiddle):
    part = dot_table(spectrum, back, 0, 2 * COLS)
    cos, sin = twiddle[:, :COLS], twiddle[:, COLS:]
    reals, imags = [], []
    for i in range(OWN):
        real = part[i * HALF : (i + 1) * HALF, :COLS]
        imag = part[i * HALF : (i + 1) * HALF, COLS:]
        reals.append(real * cos - imag * sin)
        imags.append(real * sin + imag * cos)
    turned = jnp.concatenate(
        [jnp.concatenate(reals, axis=1), jnp.concatenate(imags, axis=1)], axis=0
    )
    return dot(last[...], tall(turned))


def kernel(
    tokens_hbm, norm_gain_hbm, gate0_hbm, gate1_hbm, gate2_hbm, short_w_hbm, short_b_hbm,
    embed_w_hbm, embed_b_hbm, inner_w_hbm, inner_b_hbm, freq_hbm, filter_w_hbm, skip_hbm,
    out_gain_hbm, out_w_hbm, first_hbm, twiddle_hbm, second_hbm, back_hbm, last_hbm, feats_hbm,
    out_ref,
    tokens, norm_gain, gates, short_w, short_b, embed_w, embed_b, inner_w, inner_b, freq,
    filter_w, skip, out_gain, out_w, first, twiddle, second, back, last, feats,
    normed, flat, packed, send1, recv1, params, mixed_taps, spectra, smooth,
    send2, recv2, send3, recv3, gate_own, edge_out, edge_in, total, load_sem, send_sems, recv_sems,
):
    me = lax.axis_index("row")
    col = lax.axis_index("col")
    n_col = 8

    barrier = pltpu.get_barrier_semaphore()

    z, x = lax.div(me, 4), lax.rem(me, 4)
    row_peers = [lax.rem(z + dz, 8) * 4 + lax.rem(x + dx, 4) for dz, dx in FAR_ROWS]
    y, core = lax.div(col, 2), lax.rem(col, 2)
    col_peers = [lax.rem(y + dy, 4) * 2 + lax.rem(core + dc, 2) for dy, dc in FAR_COLS]
    for there in row_peers:
        pl.semaphore_signal(barrier, inc=1, device_id=(there, col), device_id_type=MESH)
    for there in col_peers:
        pl.semaphore_signal(barrier, inc=1, device_id=(me, there), device_id_type=MESH)

    loads = [
        pltpu.make_async_copy(src, dst, load_sem.at[j])
        for j, (src, dst) in enumerate(
            [
                (tokens_hbm, tokens),
                (norm_gain_hbm, norm_gain),
                (gate0_hbm, gates.at[:, 0:128]),
                (gate1_hbm, gates.at[:, 128:256]),
                (gate2_hbm, gates.at[:, 256:384]),
                (embed_w_hbm, embed_w),
                (embed_b_hbm, embed_b),
                (inner_w_hbm, inner_w),
                (inner_b_hbm, inner_b),
                (freq_hbm, freq),
                (filter_w_hbm, filter_w),
                (feats_hbm, feats),
                (first_hbm, first),
                (twiddle_hbm, twiddle),
                (second_hbm, second),
                (short_w_hbm, short_w),
                (short_b_hbm, short_b),
                (skip_hbm, skip),
                (back_hbm, back),
                (last_hbm, last),
                (out_gain_hbm, out_gain),
                (out_w_hbm, out_w),
            ]
        )
    ]
    for load in loads:
        load.start()

    for load in loads[0:2]:
        load.wait()

    def normalise(j, carry):
        rows = pl.ds(pl.multiple_of(j * 64, 64), 64)
        wide_tokens = tokens[rows, :].astype(F32)
        mean = jnp.mean(wide_tokens * wide_tokens, axis=1, keepdims=True)
        normed[rows, :] = (wide_tokens * lax.rsqrt(mean + NORM_EPS) * norm_gain[...]).astype(BF)
        return carry

    lax.fori_loop(0, 4, normalise, 0)
    for load in loads[2:5]:
        load.wait()
    projected = dot(normed[...], gates[...])
    projected = projected.astype(BF).astype(F32)
    gate_own[...] = projected[:, 128:256]
    edge_out[0] = projected[248:256, 128:256].astype(BF)
    edge_out[1] = projected[0:8, 128:256].astype(BF)
    for b in range(2):
        turned = projected[:, b * 256 : b * 256 + 128].T
        for half in range(2):
            flat[pl.ds(half * 128, 128), :] = turned[:, half * 128 : (half + 1) * 128]
        for half in range(2):
            for i in range(OWN):
                packed[pl.ds(4 * half + i, ROWS, stride=8), :] = flat[
                    pl.ds(128 * half + i, ROWS, stride=4), :
                ]
        send1[b] = packed[...].reshape(ROWS, 8, COLS).astype(BF)

    pl.semaphore_wait(barrier, ROWS - 1 + n_col - 1)

    def send_rows(source, target, number):
        for there in row_peers:
            pltpu.make_async_remote_copy(
                src_ref=source.at[there],
                dst_ref=target.at[me],
                send_sem=send_sems.at[number],
                recv_sem=recv_sems.at[number],
                device_id=(there, col),
                device_id_type=MESH,
            ).start()
        target[me] = source[me]

    send_rows(send1.at[1], recv1.at[1], 2)
    send_rows(send1.at[0], recv1.at[0], 0)
    for side, there in ((0, lax.rem(me + 1, ROWS)), (1, lax.rem(me + ROWS - 1, ROWS))):
        pltpu.make_async_remote_copy(
            src_ref=edge_out.at[side],
            dst_ref=edge_in.at[side],
            send_sem=send_sems.at[1],
            recv_sem=recv_sems.at[1],
            device_id=(there, col),
            device_id_type=MESH,
        ).start()

    for load in loads[5:15]:
        load.wait()
    params[...] = jnp.zeros_like(params)
    scale = freq[...] * (1.0 / (2.0 * math.pi))
    params[0:33, 0:64] = embed_w[...] * scale
    params[33:34, 0:64] = embed_b[...] * scale - 0.25
    params[48:49, 0:64] = inner_b[...] * scale - 0.25
    params[64:128, 0:64] = inner_w[...] * scale
    turned = params[...].T
    embed_t = wide(turned[0:64, 0:FEATS])
    inner_bias = turned[0:64, 48:49]
    inner_t = wide(turned[0:64, 64:128])
    filter_t = wide(
        jnp.concatenate([filter_w[o, e] for o in range(2) for e in range(2)], axis=0)
    )

    row8 = lax.broadcasted_iota(jnp.int32, (8, 1), 0)
    channel = (col * ROWS + me) * OWN + lax.rem(row8, OWN)
    fastest = math.log(DECAY_TARGET) / FAST_SPAN
    slowest = math.log(DECAY_TARGET) / SLOW_SPAN
    place = channel.astype(F32) * (1.0 / (CHANNELS - 1))
    decay = jnp.abs(slowest * (1.0 - place) + fastest * place)

    def taps_of(j, carry):
        start = pl.multiple_of(j * CHUNK, CHUNK)
        lanes = pl.ds(start, CHUNK)
        high, low = feats[0:FEATS, lanes], feats[FEATS:, lanes]
        hidden = sine_of_turns(dot(embed_t, jnp.concatenate([high, high, low], axis=0)))
        hidden = sine_of_turns(dot(inner_t, tall(hidden)) + inner_bias)
        taps = dot(filter_t, tall(hidden))
        lag = start + lax.broadcasted_iota(jnp.int32, (8, CHUNK), 1)
        row = lax.broadcasted_iota(jnp.int32, (8, CHUNK), 0)
        window = jnp.exp(-(lag.astype(F32) * (1.0 / (LENGTH - 1))) * decay)
        window = jnp.where((lag == 0) & (row >= OWN), 0.0, window)
        for o in range(2):
            both = taps[8 * o : 8 * o + 8] * window
            other = pltpu.roll(both, OWN, axis=0)
            both = jnp.where(row < OWN, both + other, other - both)
            for q in range(CHUNK // COLS):
                at = pl.multiple_of(start // COLS * 8, 8) + o * LIVE * 8 + q * 8
                mixed_taps[pl.ds(pl.multiple_of(at, 8), 8), :] = both[:, q * COLS : (q + 1) * COLS]
        return carry

    lax.fori_loop(0, LENGTH // CHUNK, taps_of, 0)
    for o in range(2):
        for part in range(2):
            signal = jnp.concatenate(
                [
                    mixed_taps[pl.ds(o * LIVE * 8 + part * OWN + i, LIVE, stride=8), :]
                    for i in range(OWN)
                ],
                axis=1,
            )
            spectra[o, :, part * COLS : (part + 1) * COLS] = dot_table(
                into_spectrum(signal, first, twiddle), second, part * COLS, (part + 1) * COLS
            )

    for load in loads[15:21]:
        load.wait()
    lane8 = lax.broadcasted_iota(jnp.int32, (8, COLS), 1)
    mine = lane8 == OWN * me + lax.rem(lax.broadcasted_iota(jnp.int32, (8, COLS), 0), OWN)

    def own_column(line):
        return jnp.sum(
            jnp.where(mine, jnp.broadcast_to(line, (8, COLS)), 0.0), axis=1, keepdims=True
        )

    all_short = short_w[...].astype(F32)
    columns = [
        [own_column(all_short[b, j : j + 1]) for j in range(3)] + [own_column(short_b[b : b + 1, :])]
        for b in (0, 2)
    ]

    def wait_row(target, number):
        pltpu.make_async_copy(
            target.at[pl.ds(0, ROWS - 1)], target.at[pl.ds(0, ROWS - 1)], recv_sems.at[number]
        ).wait()

    row = lax.broadcasted_iota(jnp.int32, (256, COLS), 0)
    lane = lax.broadcasted_iota(jnp.int32, (256, COLS), 1)

    def smoothed(b):
        wait_row(recv1.at[b], 2 * b)
        here = recv1[b].astype(F32).reshape(256, COLS)
        before = pltpu.roll(here, 1, axis=1)
        before = jnp.where(lane == 0, pltpu.roll(before, OWN, axis=0), before)
        before = jnp.where((lane == 0) & (row < OWN), 0.0, before)
        after = pltpu.roll(here, COLS - 1, axis=1)
        after = jnp.where(lane == COLS - 1, pltpu.roll(after, 256 - OWN, axis=0), after)
        after = jnp.where((lane == COLS - 1) & (row >= 256 - OWN), 0.0, after)
        tap = [jnp.broadcast_to(c, (8, COLS))[None] for c in columns[b]]
        shape = (ROWS, 8, COLS)
        value = tap[3] + before.reshape(shape) * tap[0]
        value = value + here.reshape(shape) * tap[1]
        value = value + after.reshape(shape) * tap[2]
        smooth[b] = value.reshape(256, COLS)
        return jnp.concatenate(
            [smooth[b, pl.ds(i, LIVE, stride=OWN), :] for i in range(OWN)], axis=1
        )

    signal = smoothed(1)
    for o in range(2):
        spectrum = dot_table(into_spectrum(signal, first, twiddle), second, 0, 2 * COLS)
        real, imag = spectrum[:, :COLS], spectrum[:, COLS:]
        t_real, t_imag = spectra[o, :, :COLS], spectra[o, :, COLS:]
        product = jnp.concatenate(
            [real * t_real - imag * t_imag, real * t_imag + imag * t_real], axis=1
        )
        direct = jnp.concatenate(
            [
                signal[:, i * COLS : (i + 1) * COLS]
                * jnp.broadcast_to(skip[o : o + 1, i : i + 1], (LIVE, COLS))
                for i in range(OWN)
            ],
            axis=1,
        )
        signal = from_spectrum(product, back, last, twiddle) + direct
        if o == 0:
            signal = signal * smoothed(0)

    for i in range(OWN):
        flat[pl.ds(i * LIVE, LIVE), :] = signal[:, i * COLS : (i + 1) * COLS]
    for i in range(OWN):
        for half in range(2):
            packed[pl.ds(2 * i + half, ROWS, stride=8), :] = flat[
                pl.ds(i * LIVE + half, ROWS, stride=2), :
            ]
    send2[...] = packed[...].reshape(ROWS, 8, COLS).astype(BF)

    send_rows(send2, recv2, 3)
    pltpu.make_async_copy(edge_in, edge_in, recv_sems.at[1]).wait()
    position = lax.broadcasted_iota(jnp.int32, (256, COLS), 0)
    here = gate_own[...]
    first_edge = edge_in[0].astype(F32)[7:8] * jnp.where(me == 0, 0.0, 1.0)
    last_edge = edge_in[1].astype(F32)[0:1] * jnp.where(me == ROWS - 1, 0.0, 1.0)
    before = jnp.where(position == 0, first_edge, pltpu.roll(here, 1, axis=0))
    after = jnp.where(position == 255, last_edge, pltpu.roll(here, 255, axis=0))
    value = short_b[1:2, :] + before * all_short[1, 0:1]
    value = value + here * all_short[1, 1:2]
    gate_own[...] = value + after * all_short[1, 2:3]

    wait_row(recv2, 3)

    flat[...] = recv2[...].astype(F32).reshape(256, COLS)
    for half in range(2):
        gated = flat[pl.ds(half, COLS, stride=2), :].T * gate_own[half * 128 : half * 128 + 128]
        mean = jnp.mean(gated * gated, axis=1, keepdims=True)
        gated = gated * lax.rsqrt(mean + NORM_EPS) * out_gain[...]
        send3[4 * half : 4 * half + 4] = gated.reshape(4, 32, COLS).astype(BF)

    for (dy, _), there in zip(FAR_COLS, col_peers):
        pltpu.make_async_remote_copy(
            src_ref=send3.at[there],
            dst_ref=recv3.at[col],
            send_sem=send_sems.at[4],
            recv_sem=recv_sems.at[4 + dy],
            device_id=(me, there),
            device_id_type=MESH,
        ).start()
    recv3[col] = send3[col]
    loads[21].wait()
    for dy in (0, 1, 3, 2):
        count = 2 if dy else 1
        pltpu.make_async_copy(
            recv3.at[pl.ds(0, count)], recv3.at[pl.ds(0, count)], recv_sems.at[4 + dy]
        ).wait()
        source = lax.rem(y + 4 - dy, 4)
        mixed = jnp.concatenate([recv3[2 * source], recv3[2 * source + 1]], axis=1)
        part = dot(mixed, out_w[pl.ds(pl.multiple_of(source * 256, 256), 256), :])
        if dy == 0:
            total[...] = part
        elif dy != 2:
            total[...] += part
        else:
            out_ref[...] = (total[...] + part).astype(BF)

    for number, source in ((2, send1.at[1]), (0, send1.at[0]), (3, send2)):
        pltpu.make_async_copy(
            source.at[pl.ds(0, ROWS - 1)], source.at[pl.ds(0, ROWS - 1)], send_sems.at[number]
        ).wait()
    pltpu.make_async_copy(edge_out, edge_out, send_sems.at[1]).wait()
    pltpu.make_async_copy(
        send3.at[pl.ds(0, n_col - 1)], send3.at[pl.ds(0, n_col - 1)], send_sems.at[4]
    ).wait()


def local(
    tokens, norm_gain, first_gate, second_gate, value_weight, short_weight, short_bias,
    embed_weight, embed_bias, inner_weight, inner_bias, filter_freq, filter_weight, filter_skip,
    output_gain, output_weight,
):
    constants = make_constants()
    operands = [
        tokens, norm_gain[None], first_gate, second_gate, value_weight, short_weight, short_bias,
        embed_weight, embed_bias[None], inner_weight, inner_bias[None], filter_freq[None],
        jnp.swapaxes(filter_weight, 2, 3), filter_skip, output_gain[None], output_weight,
    ] + [
        jnp.asarray(constants[name])
        for name in ("first", "twiddle", "second", "back", "last", "feats")
    ]
    vmem = pltpu.VMEM
    scratch = (
        [vmem(x.shape, x.dtype) for x in operands[0:2]]
        + [vmem((WIDTH, 384), BF)]
        + [vmem(x.shape, x.dtype) for x in operands[5:]]
    )
    scratch += [
        vmem((256, WIDTH), BF),
        vmem((256, COLS), F32),
        vmem((256, COLS), F32),
        vmem((2, ROWS, 8, COLS), BF),
        vmem((2, ROWS, 8, COLS), BF),
        vmem((128, 128), F32),
        vmem((2 * LIVE * 8, COLS), F32),
        vmem((2, OWN * HALF, 2 * COLS), F32),
        vmem((2, 256, COLS), F32),
        vmem((ROWS, 8, COLS), BF),
        vmem((ROWS, 8, COLS), BF),
        vmem((8, 32, COLS), BF),
        vmem((8, 32, COLS), BF),
        vmem((256, COLS), F32),
        vmem((2, 8, COLS), BF),
        vmem((2, 8, COLS), BF),
        vmem((32, WIDTH), F32),
        pltpu.SemaphoreType.DMA((22,)),
        pltpu.SemaphoreType.DMA((8,)),
        pltpu.SemaphoreType.DMA((8,)),
    ]
    return pl.pallas_call(
        kernel,
        out_shape=pltpu.VMEM((32, WIDTH), BF),
        in_specs=[pl.BlockSpec(memory_space=pltpu.HBM)] * len(operands),
        out_specs=pl.BlockSpec(memory_space=pltpu.VMEM),
        scratch_shapes=scratch,
        compiler_params=pltpu.CompilerParams(
            collective_id=0, has_side_effects=True, vmem_limit_bytes=66_912_256
        ),
    )(*operands)


def solution(mesh):
    in_specs = (
        P("row", None),
        P(),
        P(None, "col"),
        P(None, "col"),
        P(None, "col"),
        P(None, None, "col"),
        P(None, "col"),
        P(),
        P(),
        P(),
        P(),
        P(),
        P(None, None, None, ("col", "row")),
        P(None, ("col", "row")),
        P("col"),
        P(),
    )
    out_specs = P(("row", "col"), None)
    return jax.shard_map(local, mesh=mesh, in_specs=in_specs, out_specs=out_specs, check_vma=False)
```

```python
import math

import jax
import jax.numpy as jnp
import ml_dtypes
import numpy as np
from jax import lax
from jax.experimental import pallas as pl
from jax.experimental.pallas import tpu as pltpu
from jax.sharding import PartitionSpec as P

CHANNELS = 1024
GROUPS = 8
FREQ_BANDS = 16
NORM_EPS = 1e-06
DECAY_TARGET = 0.01
FAST_SPAN = 0.3
SLOW_SPAN = 1.5

LENGTH = 8192
WIDTH = 2048
COLS = 128
LIVE = 64
HALF = 72
TOTAL = 16384
ROWS = 32
OWN = 4
FEATS = 48
CHUNK = 2048


def farthest_first(steps):
    return [offset for _, offset in sorted(steps, reverse=True) if any(offset)]


FAR_ROWS = farthest_first(
    [(min(dz, 8 - dz) + min(dx, 4 - dx), (dz, dx)) for dz in range(8) for dx in range(4)]
)
FAR_COLS = farthest_first(
    [(2 * min(dy, 4 - dy) + dc, (dy, dc)) for dy in range(4) for dc in range(2)]
)

BF = jnp.bfloat16
F32 = jnp.float32
MESH = pl.DeviceIdType.MESH


def split_np(matrix):
    high = matrix.astype(np.float32).astype(ml_dtypes.bfloat16)
    low = (matrix - high.astype(np.float64)).astype(np.float32).astype(ml_dtypes.bfloat16)
    return high, low


def make_constants():
    k1 = np.arange(HALF)
    a = np.arange(LIVE)
    b = np.arange(COLS)
    cos_in = np.cos(2 * np.pi * np.outer(k1, a) / COLS)
    sin_in = np.sin(2 * np.pi * np.outer(k1, a) / COLS)
    first = np.concatenate([cos_in, -sin_in], 0)
    turn = 2 * np.pi * np.outer(k1, b) / TOTAL
    twiddle = np.concatenate([np.cos(turn), np.sin(turn)], 1).astype(np.float32)
    cos_out = np.cos(2 * np.pi * (np.outer(b, b) % COLS) / COLS)
    sin_out = np.sin(2 * np.pi * (np.outer(b, b) % COLS) / COLS)
    second = np.block([[cos_out, -sin_out], [sin_out, cos_out]])
    back = np.block([[cos_out, sin_out], [-sin_out, cos_out]])
    weight = np.where((k1 == 0) | (k1 == COLS // 2), 1.0, 2.0) * (k1 <= COLS // 2)
    last = np.concatenate([cos_in.T * weight, -sin_in.T * weight], 1) / TOTAL
    first_h, first_l = split_np(first)
    last_h, last_l = split_np(last)
    n = np.arange(LENGTH)
    ramp = np.linspace(0.0, 1.0, LENGTH)[None, :]
    bands = np.linspace(0.0001, FREQ_BANDS - 1, FREQ_BANDS, dtype=np.float32).astype(np.float64)
    angle = bands[:, None] * (2 * np.pi * n / LENGTH)[None, :]
    feats = np.zeros((FEATS, LENGTH))
    feats[0:1] = ramp
    feats[1 : 1 + FREQ_BANDS] = np.cos(angle)
    feats[1 + FREQ_BANDS : 1 + 2 * FREQ_BANDS] = -np.sin(angle)
    feats[1 + 2 * FREQ_BANDS] = 1.0
    return dict(
        first=np.concatenate([first_h, first_l, first_h], 1),
        twiddle=twiddle,
        second=np.stack(split_np(second)),
        back=np.stack(split_np(back)),
        last=np.concatenate([last_h, last_l, last_h], 1),
        feats=np.concatenate(split_np(feats), 0),
    )


def sine_coefficients():
    v = 0.25 * np.cos(np.pi * (np.arange(400) + 0.5) / 800)
    basis = np.stack([v ** (2 * j + 1) for j in range(5)], 1)
    scale = 1.0 / np.sin(2 * np.pi * v)
    found = np.linalg.lstsq(basis * scale[:, None], np.ones_like(v), rcond=None)[0]
    return [float(c) for c in found]


SINE = sine_coefficients()


def sine_of_turns(turns):
    v = 0.25 - jnp.abs(turns - jnp.round(turns))
    square = v * v
    result = SINE[4]
    for c in SINE[3::-1]:
        result = result * square + c
    return result * v


def split(value):
    high = value.astype(BF)
    return high, (value - high.astype(F32)).astype(BF)


def dot(left, right):
    return jnp.dot(left, right, preferred_element_type=F32)


def tall(value):
    high, low = split(value)
    return jnp.concatenate([high, high, low], axis=0)


def wide(value):
    high, low = split(value)
    return jnp.concatenate([high, low, high], axis=1)


def dot_table(value, table, lo, hi):
    high, low = split(value)
    return dot(high, table[0, :, lo:hi])


def into_spectrum(signal, first, twiddle):
    part = dot(first[:,:64], signal.astype(BF))
    cos, sin = twiddle[:, :COLS], twiddle[:, COLS:]
    pieces = []
    for i in range(signal.shape[1] // COLS):
        real = part[:HALF, i * COLS : (i + 1) * COLS]
        imag = part[HALF:, i * COLS : (i + 1) * COLS]
        pieces.append(jnp.concatenate([real * cos + imag * sin, imag * cos - real * sin], axis=1))
    return jnp.concatenate(pieces, axis=0)


def from_spectrum(spectrum, back, last, twiddle):
    part = dot_table(spectrum, back, 0, 2 * COLS)
    cos, sin = twiddle[:, :COLS], twiddle[:, COLS:]
    reals, imags = [], []
    for i in range(spectrum.shape[0] // HALF):
        real = part[i * HALF : (i + 1) * HALF, :COLS]
        imag = part[i * HALF : (i + 1) * HALF, COLS:]
        reals.append(real * cos - imag * sin)
        imags.append(real * sin + imag * cos)
    turned = jnp.concatenate(
        [jnp.concatenate(reals, axis=1), jnp.concatenate(imags, axis=1)], axis=0
    )
    return dot(last[:,:144], turned.astype(BF))


def kernel(
    tokens_hbm, norm_gain_hbm, gate0_hbm, gate1_hbm, gate2_hbm, short_w_hbm, short_b_hbm,
    embed_w_hbm, embed_b_hbm, inner_w_hbm, inner_b_hbm, freq_hbm, filter_w_hbm, skip_hbm,
    out_gain_hbm, out_w_hbm, first_hbm, twiddle_hbm, second_hbm, back_hbm, last_hbm, feats_hbm,
    out_ref,
    tokens, norm_gain, gates, short_w, short_b, embed_w, embed_b, inner_w, inner_b, freq,
    filter_w, skip, out_gain, out_w, first, twiddle, second, back, last, feats,
    normed, flat, packed, send1, recv1, params, mixed_taps, spectra, smooth,
    send2, recv2, send3, recv3, gate_own, gate_in, edge_out, edge_in, total, load_sem, send_sems, recv_sems,
):
    me = lax.axis_index("row")
    col = lax.axis_index("col")
    n_col = 8

    loads = [
        pltpu.make_async_copy(src, dst, load_sem.at[j])
        for j, (src, dst) in enumerate(
            [
                (tokens_hbm, tokens),
                (norm_gain_hbm, norm_gain),
                (gate0_hbm, gates.at[:, 0:128]),
                (gate1_hbm, gates.at[:, 128:256]),
                (gate2_hbm, gates.at[:, 256:384]),
                (embed_w_hbm, embed_w),
                (embed_b_hbm, embed_b),
                (inner_w_hbm, inner_w),
                (inner_b_hbm, inner_b),
                (freq_hbm, freq),
                (filter_w_hbm, filter_w),
                (feats_hbm, feats),
                (first_hbm, first),
                (twiddle_hbm, twiddle),
                (second_hbm, second),
                (short_w_hbm, short_w),
                (short_b_hbm, short_b),
                (skip_hbm, skip),
                (back_hbm, back),
                (last_hbm, last),
                (out_gain_hbm, out_gain),
                (out_w_hbm, out_w),
            ]
        )
    ]
    for load in loads:
        load.start()

    barrier = pltpu.get_barrier_semaphore()

    z, x = lax.div(me, 4), lax.rem(me, 4)
    row_peers = [lax.rem(z + dz, 8) * 4 + lax.rem(x + dx, 4) for dz, dx in FAR_ROWS]
    y, core = lax.div(col, 2), lax.rem(col, 2)
    partner = y * 2 + 1 - core
    col_peers = [lax.rem(y + dy, 4) * 2 + lax.rem(core + dc, 2) for dy, dc in FAR_COLS]
    for there in row_peers:
        pl.semaphore_signal(barrier, inc=1, device_id=(there, col), device_id_type=MESH)
    for there in col_peers:
        pl.semaphore_signal(barrier, inc=1, device_id=(me, there), device_id_type=MESH)

    for load in loads[0:2]:
        load.wait()

    def normalise(j, carry):
        rows = pl.ds(pl.multiple_of(j * 64, 64), 64)
        wide_tokens = tokens[rows, :].astype(F32)
        mean = jnp.mean(wide_tokens * wide_tokens, axis=1, keepdims=True)
        normed[rows, :] = (wide_tokens * lax.rsqrt(mean + NORM_EPS) * norm_gain[...]).astype(BF)
        return carry

    lax.fori_loop(0, 4, normalise, 0)
    for load in loads[2:5]:
        load.wait()
    projected = dot(normed[...], gates[...])
    projected = projected.astype(BF).astype(F32)
    gate_own[0:256, :] = projected[:, 128:256]
    edge_out[0] = projected[248:256, 128:256].astype(BF)
    edge_out[1] = projected[0:8, 128:256].astype(BF)
    for b in range(2):
        turned = projected[:, b * 256 : b * 256 + 128].T
        for half in range(2):
            flat[pl.ds(half * 128, 128), :] = turned[:, half * 128 : (half + 1) * 128]
        for half in range(2):
            for i in range(OWN):
                packed[pl.ds(4 * half + i, ROWS, stride=8), :] = flat[
                    pl.ds(128 * half + i, ROWS, stride=4), :
                ]
        send1[b] = packed[...].reshape(ROWS, 8, COLS).astype(BF)

    pl.semaphore_wait(barrier, ROWS - 1 + n_col - 1)

    def send_rows(source, target, number):
        for there in row_peers:
            pltpu.make_async_remote_copy(
                src_ref=source.at[there],
                dst_ref=target.at[me],
                send_sem=send_sems.at[number],
                recv_sem=recv_sems.at[number],
                device_id=(there, col),
                device_id_type=MESH,
            ).start()
        target[me] = source[me]

    send_rows(send1.at[1], recv1.at[1], 2)
    send_rows(send1.at[0], recv1.at[0], 0)
    for side, there in ((0, lax.rem(me + 1, ROWS)), (1, lax.rem(me + ROWS - 1, ROWS))):
        pltpu.make_async_remote_copy(
            src_ref=edge_out.at[side],
            dst_ref=edge_in.at[side],
            send_sem=send_sems.at[1],
            recv_sem=recv_sems.at[1],
            device_id=(there, col),
            device_id_type=MESH,
        ).start()

    for load in loads[5:15]:
        load.wait()
    params[...] = jnp.zeros_like(params)
    scale = freq[...] * (1.0 / (2.0 * math.pi))
    params[0:33, 0:64] = embed_w[...] * scale
    params[33:34, 0:64] = embed_b[...] * scale - 0.25
    params[48:49, 0:64] = inner_b[...] * scale - 0.25
    params[64:128, 0:64] = inner_w[...] * scale
    turned = params[...].T
    embed_t = wide(turned[0:64, 0:FEATS])
    inner_bias = turned[0:64, 48:49]
    inner_t = wide(turned[0:64, 64:128])
    filter_t = wide(
        jnp.concatenate([filter_w[o, e] for o in range(2) for e in range(2)], axis=0)
    )

    row8 = lax.broadcasted_iota(jnp.int32, (8, 1), 0)
    channel = (col * ROWS + me) * OWN + lax.rem(row8, OWN)
    fastest = math.log(DECAY_TARGET) / FAST_SPAN
    slowest = math.log(DECAY_TARGET) / SLOW_SPAN
    place = channel.astype(F32) * (1.0 / (CHANNELS - 1))
    decay = jnp.abs(slowest * (1.0 - place) + fastest * place)

    def taps_of(j, carry):
        start = pl.multiple_of(j * CHUNK, CHUNK)
        lanes = pl.ds(start, CHUNK)
        high, low = feats[0:FEATS, lanes], feats[FEATS:, lanes]
        hidden = sine_of_turns(dot(embed_t, jnp.concatenate([high, high, low], axis=0)))
        hidden = sine_of_turns(dot(inner_t, tall(hidden)) + inner_bias)
        taps = dot(filter_t, tall(hidden))
        lag = start + lax.broadcasted_iota(jnp.int32, (8, CHUNK), 1)
        row = lax.broadcasted_iota(jnp.int32, (8, CHUNK), 0)
        window = jnp.exp(-(lag.astype(F32) * (1.0 / (LENGTH - 1))) * decay)
        window = jnp.where((lag == 0) & (row >= OWN), 0.0, window)
        for o in range(2):
            both = taps[8 * o : 8 * o + 8] * window
            other = pltpu.roll(both, OWN, axis=0)
            both = jnp.where(row < OWN, both + other, other - both)
            for q in range(CHUNK // COLS):
                at = pl.multiple_of(start // COLS * 8, 8) + o * LIVE * 8 + q * 8
                mixed_taps[pl.ds(pl.multiple_of(at, 8), 8), :] = both[:, q * COLS : (q + 1) * COLS]
        return carry

    lax.fori_loop(0, LENGTH // CHUNK, taps_of, 0)
    for o in range(2):
        for part in range(2):
            signal = jnp.concatenate(
                [
                    mixed_taps[pl.ds(o * LIVE * 8 + part * OWN + i, LIVE, stride=8), :]
                    for i in range(OWN)
                ],
                axis=1,
            )
            spectra[o, :, part * COLS : (part + 1) * COLS] = dot_table(
                into_spectrum(signal, first, twiddle), second, part * COLS, (part + 1) * COLS
            )

    for load in loads[15:21]:
        load.wait()
    lane8 = lax.broadcasted_iota(jnp.int32, (8, COLS), 1)
    mine = lane8 == OWN * me + lax.rem(lax.broadcasted_iota(jnp.int32, (8, COLS), 0), OWN)

    def own_column(line):
        return jnp.sum(
            jnp.where(mine, jnp.broadcast_to(line, (8, COLS)), 0.0), axis=1, keepdims=True
        )

    all_short = short_w[...].astype(F32)
    columns = [
        [own_column(all_short[b, j : j + 1]) for j in range(3)] + [own_column(short_b[b : b + 1, :])]
        for b in (0, 2)
    ]

    def wait_row(target, number):
        pltpu.make_async_copy(
            target.at[pl.ds(0, ROWS - 1)], target.at[pl.ds(0, ROWS - 1)], recv_sems.at[number]
        ).wait()

    pltpu.make_async_copy(edge_in, edge_in, recv_sems.at[1]).wait()
    position = lax.broadcasted_iota(jnp.int32, (256, COLS), 0)
    here = gate_own[0:256, :]
    first_edge = edge_in[0].astype(F32)[7:8] * jnp.where(me == 0, 0.0, 1.0)
    last_edge = edge_in[1].astype(F32)[0:1] * jnp.where(me == ROWS - 1, 0.0, 1.0)
    before = jnp.where(position == 0, first_edge, pltpu.roll(here, 1, axis=0))
    after = jnp.where(position == 255, last_edge, pltpu.roll(here, 255, axis=0))
    value = short_b[1:2, :] + before * all_short[1, 0:1]
    value = value + here * all_short[1, 1:2]
    gate_own[0:256, :] = value + after * all_short[1, 2:3]
    gate_own[256:264, :] = jnp.broadcast_to(out_gain[...], (8, COLS))
    pltpu.make_async_remote_copy(
        src_ref=gate_own,
        dst_ref=gate_in,
        send_sem=send_sems.at[5],
        recv_sem=recv_sems.at[8],
        device_id=(me, partner),
        device_id_type=MESH,
    ).start()

    row = lax.broadcasted_iota(jnp.int32, (256, COLS), 0)
    lane = lax.broadcasted_iota(jnp.int32, (256, COLS), 1)

    def smoothed(b):
        wait_row(recv1.at[b], 2 * b)
        here = recv1[b].astype(F32).reshape(256, COLS)
        before = pltpu.roll(here, 1, axis=1)
        before = jnp.where(lane == 0, pltpu.roll(before, OWN, axis=0), before)
        before = jnp.where((lane == 0) & (row < OWN), 0.0, before)
        after = pltpu.roll(here, COLS - 1, axis=1)
        after = jnp.where(lane == COLS - 1, pltpu.roll(after, 256 - OWN, axis=0), after)
        after = jnp.where((lane == COLS - 1) & (row >= 256 - OWN), 0.0, after)
        tap = [jnp.broadcast_to(c, (8, COLS))[None] for c in columns[b]]
        shape = (ROWS, 8, COLS)
        value = tap[3] + before.reshape(shape) * tap[0]
        value = value + here.reshape(shape) * tap[1]
        value = value + after.reshape(shape) * tap[2]
        smooth[b] = value.reshape(256, COLS)
        return jnp.concatenate(
            [smooth[b, pl.ds(i, LIVE, stride=OWN), :] for i in range(OWN)], axis=1
        )

    pairs = 2
    value = smoothed(1)
    signals = [value[:, p * COLS : (p + pairs) * COLS] for p in range(0, OWN, pairs)]
    for o in range(2):
        spectrum = [
            dot_table(into_spectrum(signal, first, twiddle), second, 0, 2 * COLS)
            for signal in signals
        ]
        products = []
        for p, found in enumerate(spectrum):
            real, imag = found[:, :COLS], found[:, COLS:]
            rows = slice(p * pairs * HALF, (p + 1) * pairs * HALF)
            t_real, t_imag = spectra[o, rows, :COLS], spectra[o, rows, COLS:]
            products.append(
                jnp.concatenate(
                    [real * t_real - imag * t_imag, real * t_imag + imag * t_real], axis=1
                )
            )
        convolved = [from_spectrum(product, back, last, twiddle) for product in products]
        signals = [
            found
            + jnp.concatenate(
                [
                    signal[:, i * COLS : (i + 1) * COLS]
                    * jnp.broadcast_to(
                        skip[o : o + 1, p * pairs + i : p * pairs + i + 1], (LIVE, COLS)
                    )
                    for i in range(pairs)
                ],
                axis=1,
            )
            for p, (found, signal) in enumerate(zip(convolved, signals))
        ]
        if o == 0:
            gate = smoothed(0)
            signals = [
                signal * gate[:, p * pairs * COLS : (p + 1) * pairs * COLS]
                for p, signal in enumerate(signals)
            ]
    signal = jnp.concatenate(signals, axis=1)

    for i in range(OWN):
        flat[pl.ds(i * LIVE, LIVE), :] = signal[:, i * COLS : (i + 1) * COLS]
    for i in range(OWN):
        for half in range(2):
            packed[pl.ds(2 * i + half, ROWS, stride=8), :] = flat[
                pl.ds(i * LIVE + half, ROWS, stride=2), :
            ]
    send2[...] = packed[...].reshape(ROWS, 8, COLS).astype(BF)

    for there in row_peers + [me]:
        pltpu.make_async_remote_copy(
            src_ref=send2.at[there],
            dst_ref=recv2.at[me],
            send_sem=send_sems.at[3],
            recv_sem=recv_sems.at[3],
            device_id=(there, partner),
            device_id_type=MESH,
        ).start()
    pltpu.make_async_copy(recv2, recv2, recv_sems.at[3]).wait()
    pltpu.make_async_copy(gate_in, gate_in, recv_sems.at[8]).wait()

    flat[...] = recv2[...].astype(F32).reshape(256, COLS)
    for half in range(2):
        gated = flat[pl.ds(half, COLS, stride=2), :].T * gate_in[half * 128 : half * 128 + 128]
        mean = jnp.mean(gated * gated, axis=1, keepdims=True)
        gated = gated * lax.rsqrt(mean + NORM_EPS) * gate_in[256:257]
        send3[4 * half : 4 * half + 4] = gated.reshape(4, 32, COLS).astype(BF)

    for (dy, _), there in zip(FAR_COLS, col_peers):
        pltpu.make_async_remote_copy(
            src_ref=send3.at[there],
            dst_ref=recv3.at[partner],
            send_sem=send_sems.at[4],
            recv_sem=recv_sems.at[4 + dy],
            device_id=(me, there),
            device_id_type=MESH,
        ).start()
    recv3[partner] = send3[col]
    loads[21].wait()
    for dy in (0, 1, 3, 2):
        count = 2 if dy else 1
        pltpu.make_async_copy(
            recv3.at[pl.ds(0, count)], recv3.at[pl.ds(0, count)], recv_sems.at[4 + dy]
        ).wait()
        source = lax.rem(y + 4 - dy, 4)
        mixed = jnp.concatenate([recv3[2 * source], recv3[2 * source + 1]], axis=1)
        part = dot(mixed, out_w[pl.ds(pl.multiple_of(source * 256, 256), 256), :])
        if dy == 0:
            total[...] = part
        elif dy != 2:
            total[...] += part
        else:
            out_ref[...] = (total[...] + part).astype(BF)

    for number, source in ((2, send1.at[1]), (0, send1.at[0])):
        pltpu.make_async_copy(
            source.at[pl.ds(0, ROWS - 1)], source.at[pl.ds(0, ROWS - 1)], send_sems.at[number]
        ).wait()
    pltpu.make_async_copy(edge_out, edge_out, send_sems.at[1]).wait()
    pltpu.make_async_copy(send2, send2, send_sems.at[3]).wait()
    pltpu.make_async_copy(gate_own, gate_own, send_sems.at[5]).wait()
    pltpu.make_async_copy(
        send3.at[pl.ds(0, n_col - 1)], send3.at[pl.ds(0, n_col - 1)], send_sems.at[4]
    ).wait()


def local(
    tokens, norm_gain, first_gate, second_gate, value_weight, short_weight, short_bias,
    embed_weight, embed_bias, inner_weight, inner_bias, filter_freq, filter_weight, filter_skip,
    output_gain, output_weight,
):
    constants = make_constants()
    operands = [
        tokens, norm_gain[None], first_gate, second_gate, value_weight, short_weight, short_bias,
        embed_weight, embed_bias[None], inner_weight, inner_bias[None], filter_freq[None],
        jnp.swapaxes(filter_weight, 2, 3), filter_skip, output_gain[None], output_weight,
    ] + [
        jnp.asarray(constants[name])
        for name in ("first", "twiddle", "second", "back", "last", "feats")
    ]
    vmem = pltpu.VMEM
    scratch = (
        [vmem(x.shape, x.dtype) for x in operands[0:2]]
        + [vmem((WIDTH, 384), BF)]
        + [vmem(x.shape, x.dtype) for x in operands[5:]]
    )
    scratch += [
        vmem((256, WIDTH), BF),
        vmem((256, COLS), F32),
        vmem((256, COLS), F32),
        vmem((2, ROWS, 8, COLS), BF),
        vmem((2, ROWS, 8, COLS), BF),
        vmem((128, 128), F32),
        vmem((2 * LIVE * 8, COLS), F32),
        vmem((2, OWN * HALF, 2 * COLS), F32),
        vmem((2, 256, COLS), F32),
        vmem((ROWS, 8, COLS), BF),
        vmem((ROWS, 8, COLS), BF),
        vmem((8, 32, COLS), BF),
        vmem((8, 32, COLS), BF),
        vmem((264, COLS), F32),
        vmem((264, COLS), F32),
        vmem((2, 8, COLS), BF),
        vmem((2, 8, COLS), BF),
        vmem((32, WIDTH), F32),
        pltpu.SemaphoreType.DMA((22,)),
        pltpu.SemaphoreType.DMA((6,)),
        pltpu.SemaphoreType.DMA((9,)),
    ]
    return pl.pallas_call(
        kernel,
        out_shape=pltpu.VMEM((32, WIDTH), BF),
        in_specs=[pl.BlockSpec(memory_space=pltpu.HBM)] * len(operands),
        out_specs=pl.BlockSpec(memory_space=pltpu.VMEM),
        scratch_shapes=scratch,
        compiler_params=pltpu.CompilerParams(
            collective_id=0, has_side_effects=True, vmem_limit_bytes=66_912_256
        ),
    )(*operands)


def solution(mesh):
    in_specs = (
        P("row", None),
        P(),
        P(None, "col"),
        P(None, "col"),
        P(None, "col"),
        P(None, None, "col"),
        P(None, "col"),
        P(),
        P(),
        P(),
        P(),
        P(),
        P(None, None, None, ("col", "row")),
        P(None, ("col", "row")),
        P("col"),
        P(),
    )
    out_specs = P(("row", "col"), None)
    return jax.shard_map(local, mesh=mesh, in_specs=in_specs, out_specs=out_specs, check_vma=False)
```

```python
import math

import jax
import jax.numpy as jnp
import ml_dtypes
import numpy as np
from jax import lax
from jax.experimental import pallas as pl
from jax.experimental.pallas import tpu as pltpu
from jax.sharding import PartitionSpec as P

CHANNELS = 1024
GROUPS = 8
FREQ_BANDS = 16
NORM_EPS = 1e-06
DECAY_TARGET = 0.01
FAST_SPAN = 0.3
SLOW_SPAN = 1.5

LENGTH = 8192
WIDTH = 2048
COLS = 128
LIVE = 64
EAGER = 1
HALF = 72
TOTAL = 16384
ROWS = 32
OWN = 4
FEATS = 48
CHUNK = 2048


def farthest_first(steps):
    return [offset for _, offset in sorted(steps, reverse=True) if any(offset)]


FAR_ROWS = farthest_first(
    [(min(dz, 8 - dz) + min(dx, 4 - dx), (dz, dx)) for dz in range(8) for dx in range(4)]
)
FAR_COLS = farthest_first(
    [(2 * min(dy, 4 - dy) + dc, (dy, dc)) for dy in range(4) for dc in range(2)]
)

BF = jnp.bfloat16
F32 = jnp.float32
MESH = pl.DeviceIdType.MESH


def split_np(matrix):
    high = matrix.astype(np.float32).astype(ml_dtypes.bfloat16)
    low = (matrix - high.astype(np.float64)).astype(np.float32).astype(ml_dtypes.bfloat16)
    return high, low


def make_constants():
    k1 = np.arange(HALF)
    a = np.arange(LIVE)
    b = np.arange(COLS)
    cos_in = np.cos(2 * np.pi * np.outer(k1, a) / COLS)
    sin_in = np.sin(2 * np.pi * np.outer(k1, a) / COLS)
    first = np.concatenate([cos_in, -sin_in], 0)
    turn = 2 * np.pi * np.outer(k1, b) / TOTAL
    twiddle = np.concatenate([np.cos(turn), np.sin(turn)], 1).astype(np.float32)
    cos_out = np.cos(2 * np.pi * (np.outer(b, b) % COLS) / COLS)
    sin_out = np.sin(2 * np.pi * (np.outer(b, b) % COLS) / COLS)
    second = np.block([[cos_out, -sin_out], [sin_out, cos_out]])
    back = np.block([[cos_out, sin_out], [-sin_out, cos_out]])
    weight = np.where((k1 == 0) | (k1 == COLS // 2), 1.0, 2.0) * (k1 <= COLS // 2)
    last = np.concatenate([cos_in.T * weight, -sin_in.T * weight], 1) / TOTAL
    tables = np.zeros((720, 2 * COLS))
    tables[0:256] = second
    tables[256:512] = back
    tables[512 : 512 + 2 * HALF, :LIVE] = first
    tables[656:720, : 2 * HALF] = last
    n = np.arange(LENGTH)
    ramp = np.linspace(0.0, 1.0, LENGTH)[None, :]
    bands = np.linspace(0.0001, FREQ_BANDS - 1, FREQ_BANDS, dtype=np.float32).astype(np.float64)
    angle = bands[:, None] * (2 * np.pi * n / LENGTH)[None, :]
    feats = np.zeros((FEATS, LENGTH))
    feats[0:1] = ramp
    feats[1 : 1 + FREQ_BANDS] = np.cos(angle)
    feats[1 + FREQ_BANDS : 1 + 2 * FREQ_BANDS] = -np.sin(angle)
    feats[1 + 2 * FREQ_BANDS] = 1.0
    return dict(
        twiddle=twiddle,
        tables=split_np(tables)[0],
        feats=np.concatenate(split_np(feats), 0),
    )


def sine_coefficients():
    v = 0.25 * np.cos(np.pi * (np.arange(400) + 0.5) / 800)
    basis = np.stack([v ** (2 * j + 1) for j in range(5)], 1)
    scale = 1.0 / np.sin(2 * np.pi * v)
    found = np.linalg.lstsq(basis * scale[:, None], np.ones_like(v), rcond=None)[0]
    return [float(c) for c in found]


SINE = sine_coefficients()


def sine_of_turns(turns):
    v = 0.25 - jnp.abs(turns - jnp.round(turns))
    square = v * v
    result = SINE[4]
    for c in SINE[3::-1]:
        result = result * square + c
    return result * v


def split(value):
    high = value.astype(BF)
    return high, (value - high.astype(F32)).astype(BF)


def dot(left, right):
    return jnp.dot(left, right, preferred_element_type=F32)


def tall(value):
    high, low = split(value)
    return jnp.concatenate([high, high, low], axis=0)


def wide(value):
    high, low = split(value)
    return jnp.concatenate([high, low, high], axis=1)


def into_spectrum(signal, tables, twiddle):
    part = dot(tables[512:656, :LIVE], signal.astype(BF))
    cos, sin = twiddle[:, :COLS], twiddle[:, COLS:]
    pieces = []
    for i in range(signal.shape[1] // COLS):
        real = part[:HALF, i * COLS : (i + 1) * COLS]
        imag = part[HALF:, i * COLS : (i + 1) * COLS]
        pieces.append(jnp.concatenate([real * cos + imag * sin, imag * cos - real * sin], axis=1))
    return jnp.concatenate(pieces, axis=0).astype(BF)


def from_spectrum(spectrum, tables, twiddle):
    part = dot(spectrum.astype(BF), tables[256:512, :])
    cos, sin = twiddle[:, :COLS], twiddle[:, COLS:]
    reals, imags = [], []
    for i in range(spectrum.shape[0] // HALF):
        real = part[i * HALF : (i + 1) * HALF, :COLS]
        imag = part[i * HALF : (i + 1) * HALF, COLS:]
        reals.append(real * cos - imag * sin)
        imags.append(real * sin + imag * cos)
    turned = jnp.concatenate(
        [jnp.concatenate(reals, axis=1), jnp.concatenate(imags, axis=1)], axis=0
    )
    return dot(tables[656:720, : 2 * HALF], turned.astype(BF))


def kernel(
    tokens_hbm, norm_gain_hbm, gate0_hbm, gate1_hbm, gate2_hbm, short_w_hbm, short_b_hbm,
    embed_w_hbm, embed_b_hbm, inner_w_hbm, inner_b_hbm, freq_hbm, filter_w_hbm, skip_hbm,
    out_gain_hbm, out_w_hbm, twiddle_hbm, tables_hbm, feats_hbm,
    out_ref,
    tokens, norm_gain, gates, short_w, short_b, embed_w, lines, inner_w,
    filter_w, skip, out_gain, out_w, twiddle, tables, feats,
    normed, flat, packed, send1, recv1, params, mixed_taps, spectra, smooth,
    send2, recv2, send3, recv3, gate_own, gate_in, edge_out, edge_in, total, load_sem, send_sems, recv_sems,
):
    me = lax.axis_index("row")
    col = lax.axis_index("col")
    n_col = 8

    copies = [
        (tokens_hbm, tokens, 0),
        (norm_gain_hbm, norm_gain, 1),
        (gate0_hbm, gates.at[:, 0:128], 2),
        (gate1_hbm, gates.at[:, 128:256], 2),
        (gate2_hbm, gates.at[:, 256:384], 2),
        (embed_w_hbm, embed_w, 3),
        (embed_b_hbm, lines.at[0], 4),
        (inner_b_hbm, lines.at[1], 4),
        (freq_hbm, lines.at[2], 4),
        (inner_w_hbm, inner_w, 5),
        (filter_w_hbm, filter_w, 6),
        (feats_hbm, feats, 7),
        (tables_hbm, tables, 8),
        (twiddle_hbm, twiddle, 9),
        (short_w_hbm, short_w, 10),
        (short_b_hbm, short_b, 11),
        (skip_hbm, skip, 12),
        (out_gain_hbm, out_gain, 13),
        (out_w_hbm, out_w, 14),
    ]
    for source, target, number in copies:
        pltpu.make_async_copy(source, target, load_sem.at[number]).start()

    def loaded(*targets):
        for target, number in targets:
            pltpu.make_async_copy(target, target, load_sem.at[number]).wait()

    barrier = pltpu.get_barrier_semaphore()

    z, x = lax.div(me, 4), lax.rem(me, 4)
    row_peers = [lax.rem(z + dz, 8) * 4 + lax.rem(x + dx, 4) for dz, dx in FAR_ROWS]
    y, core = lax.div(col, 2), lax.rem(col, 2)
    partner = y * 2 + 1 - core
    col_peers = [lax.rem(y + dy, 4) * 2 + lax.rem(core + dc, 2) for dy, dc in FAR_COLS]
    for there in row_peers:
        pl.semaphore_signal(barrier, inc=1, device_id=(there, col), device_id_type=MESH)
    for there in col_peers:
        pl.semaphore_signal(barrier, inc=1, device_id=(me, there), device_id_type=MESH)

    loaded((tokens, 0), (norm_gain, 1))

    def normalise(j, carry):
        rows = pl.ds(pl.multiple_of(j * 64, 64), 64)
        wide_tokens = tokens[rows, :].astype(F32)
        mean = jnp.mean(wide_tokens * wide_tokens, axis=1, keepdims=True)
        normed[rows, :] = (wide_tokens * lax.rsqrt(mean + NORM_EPS) * norm_gain[...]).astype(BF)
        return carry

    lax.fori_loop(0, 4, normalise, 0)
    loaded((gates, 2))
    projected = dot(normed[...], gates[...])
    projected = projected.astype(BF).astype(F32)
    gate_own[0:256, :] = projected[:, 128:256]
    edge_out[0] = projected[248:256, 128:256].astype(BF)
    edge_out[1] = projected[0:8, 128:256].astype(BF)
    for b in range(2):
        turned = projected[:, b * 256 : b * 256 + 128].T
        for half in range(2):
            flat[pl.ds(half * 128, 128), :] = turned[:, half * 128 : (half + 1) * 128]
        for half in range(2):
            for i in range(OWN):
                packed[pl.ds(4 * half + i, ROWS, stride=8), :] = flat[
                    pl.ds(128 * half + i, ROWS, stride=4), :
                ]
        send1[b] = packed[...].reshape(ROWS, 8, COLS).astype(BF)

    pl.semaphore_wait(barrier, ROWS - 1 + n_col - 1)

    def send_rows(source, target, number):
        for there in row_peers:
            pltpu.make_async_remote_copy(
                src_ref=source.at[there],
                dst_ref=target.at[me],
                send_sem=send_sems.at[0],
                recv_sem=recv_sems.at[number],
                device_id=(there, col),
                device_id_type=MESH,
            ).start()
        target[me] = source[me]

    send_rows(send1.at[1], recv1.at[1], 2)
    send_rows(send1.at[0], recv1.at[0], 0)
    for side, there in ((0, lax.rem(me + 1, ROWS)), (1, lax.rem(me + ROWS - 1, ROWS))):
        pltpu.make_async_remote_copy(
            src_ref=edge_out.at[side],
            dst_ref=edge_in.at[side],
            send_sem=send_sems.at[1],
            recv_sem=recv_sems.at[1],
            device_id=(there, col),
            device_id_type=MESH,
        ).start()

    loaded((embed_w, 3), (lines, 4), (inner_w, 5), (filter_w, 6), (feats, 7), (tables, 8))
    loaded((twiddle, 9))
    params[...] = jnp.zeros_like(params)
    scale = lines[2] * (1.0 / (2.0 * math.pi))
    params[0:33, 0:64] = embed_w[...] * scale
    params[33:34, 0:64] = lines[0] * scale - 0.25
    params[48:49, 0:64] = lines[1] * scale - 0.25
    params[64:128, 0:64] = inner_w[...] * scale
    turned = params[...].T
    embed_t = wide(turned[0:64, 0:FEATS])
    inner_bias = turned[0:64, 48:49]
    inner_t = wide(turned[0:64, 64:128])
    filter_t = wide(
        jnp.concatenate([filter_w[o, e] for o in range(2) for e in range(2)], axis=0)
    )

    row8 = lax.broadcasted_iota(jnp.int32, (8, 1), 0)
    channel = (col * ROWS + me) * OWN + lax.rem(row8, OWN)
    fastest = math.log(DECAY_TARGET) / FAST_SPAN
    slowest = math.log(DECAY_TARGET) / SLOW_SPAN
    place = channel.astype(F32) * (1.0 / (CHANNELS - 1))
    decay = jnp.abs(slowest * (1.0 - place) + fastest * place)

    def taps_of(j, carry):
        start = pl.multiple_of(j * CHUNK, CHUNK)
        lanes = pl.ds(start, CHUNK)
        high, low = feats[0:FEATS, lanes], feats[FEATS:, lanes]
        hidden = sine_of_turns(dot(embed_t, jnp.concatenate([high, high, low], axis=0)))
        hidden = sine_of_turns(dot(inner_t, tall(hidden)) + inner_bias)
        taps = dot(filter_t, tall(hidden))
        lag = start + lax.broadcasted_iota(jnp.int32, (8, CHUNK), 1)
        row = lax.broadcasted_iota(jnp.int32, (8, CHUNK), 0)
        window = jnp.exp(-(lag.astype(F32) * (1.0 / (LENGTH - 1))) * decay)
        window = jnp.where((lag == 0) & (row >= OWN), 0.0, window)
        for o in range(2):
            both = taps[8 * o : 8 * o + 8] * window
            other = pltpu.roll(both, OWN, axis=0)
            both = jnp.where(row < OWN, both + other, other - both)
            for q in range(CHUNK // COLS):
                at = pl.multiple_of(start // COLS * 8, 8) + o * LIVE * 8 + q * 8
                mixed_taps[pl.ds(pl.multiple_of(at, 8), 8), :] = both[:, q * COLS : (q + 1) * COLS]
        return carry

    lax.fori_loop(0, LENGTH // CHUNK, taps_of, 0)
    for o in range(2):
        for part in range(2):
            signal = jnp.concatenate(
                [
                    mixed_taps[pl.ds(o * LIVE * 8 + part * OWN + i, LIVE, stride=8), :]
                    for i in range(OWN)
                ],
                axis=1,
            )
            spectra[o, :, part * COLS : (part + 1) * COLS] = dot(
                into_spectrum(signal, tables, twiddle),
                tables[0:256, part * COLS : (part + 1) * COLS],
            )

    loaded((short_w, 10), (short_b, 11), (skip, 12), (out_gain, 13))
    lane8 = lax.broadcasted_iota(jnp.int32, (8, COLS), 1)
    mine = lane8 == OWN * me + lax.rem(lax.broadcasted_iota(jnp.int32, (8, COLS), 0), OWN)

    def own_column(line):
        return jnp.sum(
            jnp.where(mine, jnp.broadcast_to(line, (8, COLS)), 0.0), axis=1, keepdims=True
        )

    all_short = short_w[...].astype(F32)
    columns = [
        [own_column(all_short[b, j : j + 1]) for j in range(3)] + [own_column(short_b[b : b + 1, :])]
        for b in (0, 2)
    ]

    def wait_row(target, number):
        pltpu.make_async_copy(
            target.at[pl.ds(0, ROWS - 1)], target.at[pl.ds(0, ROWS - 1)], recv_sems.at[number]
        ).wait()

    pltpu.make_async_copy(edge_in, edge_in, recv_sems.at[1]).wait()
    position = lax.broadcasted_iota(jnp.int32, (256, COLS), 0)
    here = gate_own[0:256, :]
    first_edge = edge_in[0].astype(F32)[7:8] * jnp.where(me == 0, 0.0, 1.0)
    last_edge = edge_in[1].astype(F32)[0:1] * jnp.where(me == ROWS - 1, 0.0, 1.0)
    before = jnp.where(position == 0, first_edge, pltpu.roll(here, 1, axis=0))
    after = jnp.where(position == 255, last_edge, pltpu.roll(here, 255, axis=0))
    value = short_b[1:2, :] + before * all_short[1, 0:1]
    value = value + here * all_short[1, 1:2]
    gate_own[0:256, :] = value + after * all_short[1, 2:3]
    gate_own[256:264, :] = jnp.broadcast_to(out_gain[...], (8, COLS))
    pltpu.make_async_remote_copy(
        src_ref=gate_own,
        dst_ref=gate_in,
        send_sem=send_sems.at[4],
        recv_sem=recv_sems.at[8],
        device_id=(me, partner),
        device_id_type=MESH,
    ).start()

    row = lax.broadcasted_iota(jnp.int32, (256, COLS), 0)
    lane = lax.broadcasted_iota(jnp.int32, (256, COLS), 1)

    def smoothed(b):
        wait_row(recv1.at[b], 2 * b)
        here = recv1[b].astype(F32).reshape(256, COLS)
        before = pltpu.roll(here, 1, axis=1)
        before = jnp.where(lane == 0, pltpu.roll(before, OWN, axis=0), before)
        before = jnp.where((lane == 0) & (row < OWN), 0.0, before)
        after = pltpu.roll(here, COLS - 1, axis=1)
        after = jnp.where(lane == COLS - 1, pltpu.roll(after, 256 - OWN, axis=0), after)
        after = jnp.where((lane == COLS - 1) & (row >= 256 - OWN), 0.0, after)
        tap = [jnp.broadcast_to(c, (8, COLS))[None] for c in columns[b]]
        shape = (ROWS, 8, COLS)
        value = tap[3] + before.reshape(shape) * tap[0]
        value = value + here.reshape(shape) * tap[1]
        value = value + after.reshape(shape) * tap[2]
        smooth[b] = value.reshape(256, COLS)
        return jnp.concatenate(
            [smooth[b, pl.ds(i, LIVE, stride=OWN), :] for i in range(OWN)], axis=1
        )

    pairs = 2
    value = smoothed(1)
    signals = [value[:, p * COLS : (p + pairs) * COLS] for p in range(0, OWN, pairs)]
    for o in range(2):
        spectrum = [
            dot(into_spectrum(signal, tables, twiddle), tables[0:256, :])
            for signal in signals
        ]
        products = []
        for p, found in enumerate(spectrum):
            real, imag = found[:, :COLS], found[:, COLS:]
            rows = slice(p * pairs * HALF, (p + 1) * pairs * HALF)
            t_real, t_imag = spectra[o, rows, :COLS], spectra[o, rows, COLS:]
            products.append(
                jnp.concatenate(
                    [real * t_real - imag * t_imag, real * t_imag + imag * t_real], axis=1
                )
            )
        convolved = [from_spectrum(product, tables, twiddle) for product in products]
        signals = [
            found
            + jnp.concatenate(
                [
                    signal[:, i * COLS : (i + 1) * COLS]
                    * jnp.broadcast_to(
                        skip[o : o + 1, p * pairs + i : p * pairs + i + 1], (LIVE, COLS)
                    )
                    for i in range(pairs)
                ],
                axis=1,
            )
            for p, (found, signal) in enumerate(zip(convolved, signals))
        ]
        if o == 0:
            gate = smoothed(0)
            signals = [
                signal * gate[:, p * pairs * COLS : (p + 1) * pairs * COLS]
                for p, signal in enumerate(signals)
            ]
    signal = jnp.concatenate(signals, axis=1)

    for i in range(OWN):
        flat[pl.ds(i * LIVE, LIVE), :] = signal[:, i * COLS : (i + 1) * COLS]
    for i in range(OWN):
        for half in range(2):
            packed[pl.ds(2 * i + half, ROWS, stride=8), :] = flat[
                pl.ds(i * LIVE + half, ROWS, stride=2), :
            ]
    send2[...] = packed[...].reshape(ROWS, 8, COLS).astype(BF)

    for there in row_peers + [me]:
        pltpu.make_async_remote_copy(
            src_ref=send2.at[there],
            dst_ref=recv2.at[me],
            send_sem=send_sems.at[2],
            recv_sem=recv_sems.at[3],
            device_id=(there, partner),
            device_id_type=MESH,
        ).start()
    pltpu.make_async_copy(recv2, recv2, recv_sems.at[3]).wait()
    pltpu.make_async_copy(gate_in, gate_in, recv_sems.at[8]).wait()

    def send_over(there, dy):
        pltpu.make_async_remote_copy(
            src_ref=send3.at[there],
            dst_ref=recv3.at[partner],
            send_sem=send_sems.at[3],
            recv_sem=recv_sems.at[4 + dy],
            device_id=(me, there),
            device_id_type=MESH,
        ).start()

    flat[...] = recv2[...].astype(F32).reshape(256, COLS)
    for half in range(2):
        gated = flat[pl.ds(half, COLS, stride=2), :].T * gate_in[half * 128 : half * 128 + 128]
        mean = jnp.mean(gated * gated, axis=1, keepdims=True)
        gated = gated * lax.rsqrt(mean + NORM_EPS) * gate_in[256:257]
        send3[4 * half : 4 * half + 4] = gated.reshape(4, 32, COLS).astype(BF)
        if half == EAGER // 4:
            pl.when(col != EAGER)(lambda: send_over(EAGER, lax.rem(EAGER // 2 + 4 - y, 4)))

    for (dy, _), there in zip(FAR_COLS, col_peers):
        pl.when(there != EAGER)(lambda there=there, dy=dy: send_over(there, dy))
    recv3[partner] = send3[col]
    loaded((out_w, 14))
    for dy in (0, 3, 2, 1):
        count = 2 if dy else 1
        pltpu.make_async_copy(
            recv3.at[pl.ds(0, count)], recv3.at[pl.ds(0, count)], recv_sems.at[4 + dy]
        ).wait()
        source = lax.rem(y + 4 - dy, 4)
        mixed = jnp.concatenate([recv3[2 * source], recv3[2 * source + 1]], axis=1)
        part = dot(mixed, out_w[pl.ds(pl.multiple_of(source * 256, 256), 256), :])
        if dy == 0:
            total[...] = part
        elif dy != 1:
            total[...] += part
        else:
            out_ref[...] = (total[...] + part).astype(BF)

    for number, source in enumerate(
        [
            send1.at[:, pl.ds(0, ROWS - 1)], edge_out, send2, send3.at[pl.ds(0, n_col - 1)],
            gate_own,
        ]
    ):
        pltpu.make_async_copy(source, source, send_sems.at[number]).wait()


def local(
    tokens, norm_gain, first_gate, second_gate, value_weight, short_weight, short_bias,
    embed_weight, embed_bias, inner_weight, inner_bias, filter_freq, filter_weight, filter_skip,
    output_gain, output_weight,
):
    constants = make_constants()
    operands = [
        tokens, norm_gain[None], first_gate, second_gate, value_weight, short_weight, short_bias,
        embed_weight, embed_bias[None], inner_weight, inner_bias[None], filter_freq[None],
        jnp.swapaxes(filter_weight, 2, 3), filter_skip, output_gain[None], output_weight,
    ] + [
        jnp.asarray(constants[name])
        for name in ("twiddle", "tables", "feats")
    ]
    vmem = pltpu.VMEM
    scratch = [vmem(x.shape, x.dtype) for x in operands[0:2]]
    scratch += [vmem((WIDTH, 384), BF)]
    scratch += [vmem(x.shape, x.dtype) for x in operands[5:8]]
    scratch += [vmem((3, 1, 64), F32), vmem((64, 64), F32)]
    scratch += [vmem(x.shape, x.dtype) for x in operands[12:]]
    scratch += [
        vmem((256, WIDTH), BF),
        vmem((256, COLS), F32),
        vmem((256, COLS), F32),
        vmem((2, ROWS, 8, COLS), BF),
        vmem((2, ROWS, 8, COLS), BF),
        vmem((128, 128), F32),
        vmem((2 * LIVE * 8, COLS), F32),
        vmem((2, OWN * HALF, 2 * COLS), F32),
        vmem((2, 256, COLS), F32),
        vmem((ROWS, 8, COLS), BF),
        vmem((ROWS, 8, COLS), BF),
        vmem((8, 32, COLS), BF),
        vmem((8, 32, COLS), BF),
        vmem((264, COLS), F32),
        vmem((264, COLS), F32),
        vmem((2, 8, COLS), BF),
        vmem((2, 8, COLS), BF),
        vmem((32, WIDTH), F32),
        pltpu.SemaphoreType.DMA((15,)),
        pltpu.SemaphoreType.DMA((5,)),
        pltpu.SemaphoreType.DMA((9,)),
    ]
    return pl.pallas_call(
        kernel,
        out_shape=pltpu.VMEM((32, WIDTH), BF),
        in_specs=[pl.BlockSpec(memory_space=pltpu.HBM)] * len(operands),
        out_specs=pl.BlockSpec(memory_space=pltpu.VMEM),
        scratch_shapes=scratch,
        compiler_params=pltpu.CompilerParams(
            collective_id=0, has_side_effects=True, vmem_limit_bytes=66_912_256
        ),
    )(*operands)


def solution(mesh):
    in_specs = (
        P("row", None),
        P(),
        P(None, "col"),
        P(None, "col"),
        P(None, "col"),
        P(None, None, "col"),
        P(None, "col"),
        P(),
        P(),
        P(),
        P(),
        P(),
        P(None, None, None, ("col", "row")),
        P(None, ("col", "row")),
        P("col"),
        P(),
    )
    out_specs = P(("row", "col"), None)
    return jax.shard_map(local, mesh=mesh, in_specs=in_specs, out_specs=out_specs, check_vma=False)
```

```python
import math

import jax
import jax.numpy as jnp
import ml_dtypes
import numpy as np
from jax import lax
from jax.experimental import pallas as pl
from jax.experimental.pallas import tpu as pltpu
from jax.sharding import PartitionSpec as P

CHANNELS = 1024
GROUPS = 8
FREQ_BANDS = 16
NORM_EPS = 1e-06
DECAY_TARGET = 0.01
FAST_SPAN = 0.3
SLOW_SPAN = 1.5

LENGTH = 8192
WIDTH = 2048
COLS = 128
LIVE = 64
EAGER = 1
HALF = 72
TOTAL = 16384
ROWS = 32
OWN = 4
FEATS = 48
CHUNK = 2048


def farthest_first(steps):
    return [step for step in sorted(steps, reverse=True) if any(step[1])]


ROW_HOPS = farthest_first(
    [(min(dz, 8 - dz) + min(dx, 4 - dx), (dz, dx)) for dz in range(8) for dx in range(4)]
)
FAR_ROWS = [offset for _, offset in ROW_HOPS]
COL_HOPS = farthest_first(
    [(2 * min(dy, 4 - dy) + dc, (dy, dc)) for dy in range(4) for dc in range(2)]
)
FAR_COLS = [offset for _, offset in COL_HOPS]

BF = jnp.bfloat16
F32 = jnp.float32
MESH = pl.DeviceIdType.MESH


def split_np(matrix):
    high = matrix.astype(np.float32).astype(ml_dtypes.bfloat16)
    low = (matrix - high.astype(np.float64)).astype(np.float32).astype(ml_dtypes.bfloat16)
    return high, low


def make_constants():
    k1 = np.arange(HALF)
    a = np.arange(LIVE)
    b = np.arange(COLS)
    cos_in = np.cos(2 * np.pi * np.outer(k1, a) / COLS)
    sin_in = np.sin(2 * np.pi * np.outer(k1, a) / COLS)
    first = np.concatenate([cos_in, -sin_in], 0)
    turn = 2 * np.pi * np.outer(k1, b) / TOTAL
    twiddle = np.concatenate([np.cos(turn), np.sin(turn)], 1).astype(np.float32)
    cos_out = np.cos(2 * np.pi * (np.outer(b, b) % COLS) / COLS)
    sin_out = np.sin(2 * np.pi * (np.outer(b, b) % COLS) / COLS)
    second = np.block([[cos_out, -sin_out], [sin_out, cos_out]])
    back = np.block([[cos_out, sin_out], [-sin_out, cos_out]])
    weight = np.where((k1 == 0) | (k1 == COLS // 2), 1.0, 2.0) * (k1 <= COLS // 2)
    last = np.concatenate([cos_in.T * weight, -sin_in.T * weight], 1) / TOTAL
    tables = np.zeros((720, 2 * COLS))
    tables[0:256] = second
    tables[256:512] = back
    tables[512 : 512 + 2 * HALF, :LIVE] = first
    tables[656:720, : 2 * HALF] = last
    n = np.arange(LENGTH)
    ramp = np.linspace(0.0, 1.0, LENGTH)[None, :]
    bands = np.linspace(0.0001, FREQ_BANDS - 1, FREQ_BANDS, dtype=np.float32).astype(np.float64)
    angle = bands[:, None] * (2 * np.pi * n / LENGTH)[None, :]
    feats = np.zeros((FEATS, LENGTH))
    feats[0:1] = ramp
    feats[1 : 1 + FREQ_BANDS] = np.cos(angle)
    feats[1 + FREQ_BANDS : 1 + 2 * FREQ_BANDS] = -np.sin(angle)
    feats[1 + 2 * FREQ_BANDS] = 1.0
    return dict(
        twiddle=twiddle,
        tables=split_np(tables)[0],
        feats=np.concatenate(split_np(feats), 0),
    )


def sine_coefficients():
    v = 0.25 * np.cos(np.pi * (np.arange(400) + 0.5) / 800)
    basis = np.stack([v ** (2 * j + 1) for j in range(5)], 1)
    scale = 1.0 / np.sin(2 * np.pi * v)
    found = np.linalg.lstsq(basis * scale[:, None], np.ones_like(v), rcond=None)[0]
    return [float(c) for c in found]


SINE = sine_coefficients()


def sine_of_turns(turns):
    v = 0.25 - jnp.abs(turns - jnp.round(turns))
    square = v * v
    result = SINE[4]
    for c in SINE[3::-1]:
        result = result * square + c
    return result * v


def split(value):
    high = value.astype(BF)
    return high, (value - high.astype(F32)).astype(BF)


def dot(left, right):
    return jnp.dot(left, right, preferred_element_type=F32)


def tall(value):
    high, low = split(value)
    return jnp.concatenate([high, high, low], axis=0)


def wide(value):
    high, low = split(value)
    return jnp.concatenate([high, low, high], axis=1)


def into_spectrum(signal, tables, twiddle):
    part = dot(tables[512:656, :LIVE], signal.astype(BF))
    cos, sin = twiddle[:, :COLS], twiddle[:, COLS:]
    pieces = []
    for i in range(signal.shape[1] // COLS):
        real = part[:HALF, i * COLS : (i + 1) * COLS]
        imag = part[HALF:, i * COLS : (i + 1) * COLS]
        pieces.append(jnp.concatenate([real * cos + imag * sin, imag * cos - real * sin], axis=1))
    return jnp.concatenate(pieces, axis=0).astype(BF)


def from_spectrum(spectrum, tables, twiddle):
    part = dot(spectrum.astype(BF), tables[256:512, :])
    cos, sin = twiddle[:, :COLS], twiddle[:, COLS:]
    reals, imags = [], []
    for i in range(spectrum.shape[0] // HALF):
        real = part[i * HALF : (i + 1) * HALF, :COLS]
        imag = part[i * HALF : (i + 1) * HALF, COLS:]
        reals.append(real * cos - imag * sin)
        imags.append(real * sin + imag * cos)
    turned = jnp.concatenate(
        [jnp.concatenate(reals, axis=1), jnp.concatenate(imags, axis=1)], axis=0
    )
    return dot(tables[656:720, : 2 * HALF], turned.astype(BF))


def kernel(
    tokens_hbm, norm_gain_hbm, gate0_hbm, gate1_hbm, gate2_hbm, short_w_hbm, short_b_hbm,
    embed_w_hbm, embed_b_hbm, inner_w_hbm, inner_b_hbm, freq_hbm, filter_w_hbm, skip_hbm,
    out_gain_hbm, out_w_hbm, twiddle_hbm, tables_hbm, feats_hbm,
    out_ref,
    tokens, norm_gain, gates, short_w, short_b, embed_w, lines, inner_w,
    filter_w, skip, out_gain, out_w, twiddle, tables, feats,
    normed, flat, packed, send1, recv1, params, mixed_taps, spectra, smooth,
    send2, recv2, send3, recv3, gate_own, gate_in, edge_out, edge_in, total, load_sem, send_sems, recv_sems,
):
    me = lax.axis_index("row")
    col = lax.axis_index("col")
    n_col = 8

    def loaded(*targets):
        for target, number in targets:
            pltpu.make_async_copy(target, target, load_sem.at[number]).wait()

    barrier = pltpu.get_barrier_semaphore()

    z, x = lax.div(me, 4), lax.rem(me, 4)
    row_peers = [lax.rem(z + dz, 8) * 4 + lax.rem(x + dx, 4) for dz, dx in FAR_ROWS]
    y, core = lax.div(col, 2), lax.rem(col, 2)
    partner = y * 2 + 1 - core
    col_peers = [lax.rem(y + dy, 4) * 2 + lax.rem(core + dc, 2) for dy, dc in FAR_COLS]
    for there in row_peers:
        pl.semaphore_signal(barrier, inc=1, device_id=(there, col), device_id_type=MESH)
    copies = [
        (tokens_hbm, tokens, 0),
        (norm_gain_hbm, norm_gain, 1),
        (gate0_hbm, gates.at[:, 0:128], 2),
        (gate1_hbm, gates.at[:, 128:256], 2),
        (gate2_hbm, gates.at[:, 256:384], 2),
        (embed_w_hbm, embed_w, 3),
        (embed_b_hbm, lines.at[0], 4),
        (inner_b_hbm, lines.at[1], 4),
        (freq_hbm, lines.at[2], 4),
        (inner_w_hbm, inner_w, 5),
        (filter_w_hbm, filter_w, 6),
        (feats_hbm, feats, 7),
        (tables_hbm, tables, 8),
        (twiddle_hbm, twiddle, 9),
        (short_w_hbm, short_w, 10),
        (short_b_hbm, short_b, 11),
        (skip_hbm, skip, 12),
        (out_gain_hbm, out_gain, 13),
        (out_w_hbm, out_w, 14),
    ]
    for source, target, number in copies:
        pltpu.make_async_copy(source, target, load_sem.at[number]).start()

    for there in col_peers:
        pl.semaphore_signal(barrier, inc=1, device_id=(me, there), device_id_type=MESH)

    loaded((tokens, 0), (norm_gain, 1))

    def normalise(j, carry):
        rows = pl.ds(pl.multiple_of(j * 64, 64), 64)
        wide_tokens = tokens[rows, :].astype(F32)
        mean = jnp.mean(wide_tokens * wide_tokens, axis=1, keepdims=True)
        normed[rows, :] = (wide_tokens * lax.rsqrt(mean + NORM_EPS) * norm_gain[...]).astype(BF)
        return carry

    lax.fori_loop(0, 4, normalise, 0)
    loaded((gates, 2))
    projected = dot(normed[...], gates[...])
    projected = projected.astype(BF).astype(F32)
    gate_own[0:256, :] = projected[:, 128:256]
    edge_out[0] = projected[248:256, 128:256].astype(BF)
    edge_out[1] = projected[0:8, 128:256].astype(BF)
    for b in range(2):
        turned = projected[:, b * 256 : b * 256 + 128].T
        for half in range(2):
            flat[pl.ds(half * 128, 128), :] = turned[:, half * 128 : (half + 1) * 128]
        for half in range(2):
            for i in range(OWN):
                packed[pl.ds(4 * half + i, ROWS, stride=8), :] = flat[
                    pl.ds(128 * half + i, ROWS, stride=4), :
                ]
        send1[b] = packed[...].reshape(ROWS, 8, COLS).astype(BF)

    pl.semaphore_wait(barrier, ROWS - 1 + n_col - 1)

    urgency = [(hops - 1 + b, b, k) for k, (hops, _) in enumerate(ROW_HOPS) for b in range(2)]
    for _, b, k in sorted(urgency, key=lambda item: (-item[0], -item[1], item[2])):
        there = row_peers[k]
        pltpu.make_async_remote_copy(
            src_ref=send1.at[b, there],
            dst_ref=recv1.at[b, me],
            send_sem=send_sems.at[0],
            recv_sem=recv_sems.at[2 * b],
            device_id=(there, col),
            device_id_type=MESH,
        ).start()
    for b in range(2):
        recv1[b, me] = send1[b, me]
    for side, there in ((0, lax.rem(me + 1, ROWS)), (1, lax.rem(me + ROWS - 1, ROWS))):
        pltpu.make_async_remote_copy(
            src_ref=edge_out.at[side],
            dst_ref=edge_in.at[side],
            send_sem=send_sems.at[1],
            recv_sem=recv_sems.at[1],
            device_id=(there, col),
            device_id_type=MESH,
        ).start()

    loaded((embed_w, 3), (lines, 4), (inner_w, 5), (filter_w, 6), (feats, 7), (tables, 8))
    loaded((twiddle, 9))
    params[...] = jnp.zeros_like(params)
    scale = lines[2] * (1.0 / (2.0 * math.pi))
    params[0:33, 0:64] = embed_w[...] * scale
    params[33:34, 0:64] = lines[0] * scale - 0.25
    params[48:49, 0:64] = lines[1] * scale - 0.25
    params[64:128, 0:64] = inner_w[...] * scale
    turned = params[...].T
    embed_t = wide(turned[0:64, 0:FEATS])
    inner_bias = turned[0:64, 48:49]
    inner_t = wide(turned[0:64, 64:128])
    filter_t = wide(
        jnp.concatenate([filter_w[o, e] for o in range(2) for e in range(2)], axis=0)
    )

    row8 = lax.broadcasted_iota(jnp.int32, (8, 1), 0)
    channel = (col * ROWS + me) * OWN + lax.rem(row8, OWN)
    fastest = math.log(DECAY_TARGET) / FAST_SPAN
    slowest = math.log(DECAY_TARGET) / SLOW_SPAN
    place = channel.astype(F32) * (1.0 / (CHANNELS - 1))
    decay = jnp.abs(slowest * (1.0 - place) + fastest * place)

    def taps_of(j, carry):
        start = pl.multiple_of(j * CHUNK, CHUNK)
        lanes = pl.ds(start, CHUNK)
        high, low = feats[0:FEATS, lanes], feats[FEATS:, lanes]
        hidden = sine_of_turns(dot(embed_t, jnp.concatenate([high, high, low], axis=0)))
        hidden = sine_of_turns(dot(inner_t, tall(hidden)) + inner_bias)
        taps = dot(filter_t, tall(hidden))
        lag = start + lax.broadcasted_iota(jnp.int32, (8, CHUNK), 1)
        row = lax.broadcasted_iota(jnp.int32, (8, CHUNK), 0)
        window = jnp.exp(-(lag.astype(F32) * (1.0 / (LENGTH - 1))) * decay)
        window = jnp.where((lag == 0) & (row >= OWN), 0.0, window)
        for o in range(2):
            both = taps[8 * o : 8 * o + 8] * window
            other = pltpu.roll(both, OWN, axis=0)
            both = jnp.where(row < OWN, both + other, other - both)
            for q in range(CHUNK // COLS):
                at = pl.multiple_of(start // COLS * 8, 8) + o * LIVE * 8 + q * 8
                mixed_taps[pl.ds(pl.multiple_of(at, 8), 8), :] = both[:, q * COLS : (q + 1) * COLS]
        return carry

    lax.fori_loop(0, LENGTH // CHUNK, taps_of, 0)
    for o in range(2):
        for part in range(2):
            signal = jnp.concatenate(
                [
                    mixed_taps[pl.ds(o * LIVE * 8 + part * OWN + i, LIVE, stride=8), :]
                    for i in range(OWN)
                ],
                axis=1,
            )
            spectra[o, :, part * COLS : (part + 1) * COLS] = dot(
                into_spectrum(signal, tables, twiddle),
                tables[0:256, part * COLS : (part + 1) * COLS],
            )

    loaded((short_w, 10), (short_b, 11), (skip, 12), (out_gain, 13))
    lane8 = lax.broadcasted_iota(jnp.int32, (8, COLS), 1)
    mine = lane8 == OWN * me + lax.rem(lax.broadcasted_iota(jnp.int32, (8, COLS), 0), OWN)

    def own_column(line):
        return jnp.sum(
            jnp.where(mine, jnp.broadcast_to(line, (8, COLS)), 0.0), axis=1, keepdims=True
        )

    all_short = short_w[...].astype(F32)
    columns = [
        [own_column(all_short[b, j : j + 1]) for j in range(3)] + [own_column(short_b[b : b + 1, :])]
        for b in (0, 2)
    ]

    def wait_row(target, number):
        pltpu.make_async_copy(
            target.at[pl.ds(0, ROWS - 1)], target.at[pl.ds(0, ROWS - 1)], recv_sems.at[number]
        ).wait()

    pltpu.make_async_copy(edge_in, edge_in, recv_sems.at[1]).wait()
    position = lax.broadcasted_iota(jnp.int32, (256, COLS), 0)
    here = gate_own[0:256, :]
    first_edge = edge_in[0].astype(F32)[7:8] * jnp.where(me == 0, 0.0, 1.0)
    last_edge = edge_in[1].astype(F32)[0:1] * jnp.where(me == ROWS - 1, 0.0, 1.0)
    before = jnp.where(position == 0, first_edge, pltpu.roll(here, 1, axis=0))
    after = jnp.where(position == 255, last_edge, pltpu.roll(here, 255, axis=0))
    value = short_b[1:2, :] + before * all_short[1, 0:1]
    value = value + here * all_short[1, 1:2]
    gate_own[0:256, :] = value + after * all_short[1, 2:3]
    gate_own[256:264, :] = jnp.broadcast_to(out_gain[...], (8, COLS))
    pltpu.make_async_remote_copy(
        src_ref=gate_own,
        dst_ref=gate_in,
        send_sem=send_sems.at[4],
        recv_sem=recv_sems.at[4],
        device_id=(me, partner),
        device_id_type=MESH,
    ).start()

    row = lax.broadcasted_iota(jnp.int32, (256, COLS), 0)
    lane = lax.broadcasted_iota(jnp.int32, (256, COLS), 1)

    def smoothed(b):
        wait_row(recv1.at[b], 2 * b)
        here = recv1[b].astype(F32).reshape(256, COLS)
        before = pltpu.roll(here, 1, axis=1)
        before = jnp.where(lane == 0, pltpu.roll(before, OWN, axis=0), before)
        before = jnp.where((lane == 0) & (row < OWN), 0.0, before)
        after = pltpu.roll(here, COLS - 1, axis=1)
        after = jnp.where(lane == COLS - 1, pltpu.roll(after, 256 - OWN, axis=0), after)
        after = jnp.where((lane == COLS - 1) & (row >= 256 - OWN), 0.0, after)
        tap = [jnp.broadcast_to(c, (8, COLS))[None] for c in columns[b]]
        shape = (ROWS, 8, COLS)
        value = tap[3] + before.reshape(shape) * tap[0]
        value = value + here.reshape(shape) * tap[1]
        value = value + after.reshape(shape) * tap[2]
        smooth[b] = value.reshape(256, COLS)
        return jnp.concatenate(
            [smooth[b, pl.ds(i, LIVE, stride=OWN), :] for i in range(OWN)], axis=1
        )

    pairs = 2
    value = smoothed(1)
    signals = [value[:, p * COLS : (p + pairs) * COLS] for p in range(0, OWN, pairs)]
    for o in range(2):
        spectrum = [
            dot(into_spectrum(signal, tables, twiddle), tables[0:256, :])
            for signal in signals
        ]
        products = []
        for p, found in enumerate(spectrum):
            real, imag = found[:, :COLS], found[:, COLS:]
            rows = slice(p * pairs * HALF, (p + 1) * pairs * HALF)
            t_real, t_imag = spectra[o, rows, :COLS], spectra[o, rows, COLS:]
            products.append(
                jnp.concatenate(
                    [real * t_real - imag * t_imag, real * t_imag + imag * t_real], axis=1
                )
            )
        convolved = [from_spectrum(product, tables, twiddle) for product in products]
        signals = [
            found
            + jnp.concatenate(
                [
                    signal[:, i * COLS : (i + 1) * COLS]
                    * jnp.broadcast_to(
                        skip[o : o + 1, p * pairs + i : p * pairs + i + 1], (LIVE, COLS)
                    )
                    for i in range(pairs)
                ],
                axis=1,
            )
            for p, (found, signal) in enumerate(zip(convolved, signals))
        ]
        if o == 0:
            gate = smoothed(0)
            signals = [
                signal * gate[:, p * pairs * COLS : (p + 1) * pairs * COLS]
                for p, signal in enumerate(signals)
            ]
    signal = jnp.concatenate(signals, axis=1)

    for i in range(OWN):
        flat[pl.ds(i * LIVE, LIVE), :] = signal[:, i * COLS : (i + 1) * COLS]
    for i in range(OWN):
        for half in range(2):
            packed[pl.ds(2 * i + half, ROWS, stride=8), :] = flat[
                pl.ds(i * LIVE + half, ROWS, stride=2), :
            ]
    send2[...] = packed[...].reshape(ROWS, 8, COLS).astype(BF)

    for there in row_peers + [me]:
        pltpu.make_async_remote_copy(
            src_ref=send2.at[there],
            dst_ref=recv2.at[me],
            send_sem=send_sems.at[2],
            recv_sem=recv_sems.at[3],
            device_id=(there, partner),
            device_id_type=MESH,
        ).start()
    pltpu.make_async_copy(recv2, recv2, recv_sems.at[3]).wait()
    pltpu.make_async_copy(gate_in, gate_in, recv_sems.at[4]).wait()

    def send_over(there, back):
        pltpu.make_async_remote_copy(
            src_ref=send3.at[there],
            dst_ref=recv3.at[partner],
            send_sem=send_sems.at[3],
            recv_sem=recv_sems.at[5 + back + core * (back // 3)],
            device_id=(me, there),
            device_id_type=MESH,
        ).start()

    flat[...] = recv2[...].astype(F32).reshape(256, COLS)
    for half in range(2):
        gated = flat[pl.ds(half, COLS, stride=2), :].T * gate_in[half * 128 : half * 128 + 128]
        mean = jnp.mean(gated * gated, axis=1, keepdims=True)
        gated = gated * lax.rsqrt(mean + NORM_EPS) * gate_in[256:257]
        send3[4 * half : 4 * half + 4] = gated.reshape(4, 32, COLS).astype(BF)
        if half == EAGER // 4:
            pl.when(col != EAGER)(lambda: send_over(EAGER, lax.rem(y + 4 - EAGER // 2, 4)))

    for (dy, _), there in zip(FAR_COLS, col_peers):
        pl.when(there != EAGER)(lambda there=there, dy=dy: send_over(there, (4 - dy) % 4))
    recv3[partner] = send3[col]
    loaded((out_w, 14))

    def arrived(count, number):
        block = recv3.at[pl.ds(0, count)]
        pltpu.make_async_copy(block, block, recv_sems.at[number]).wait()

    for back in range(3):
        arrived(2 if back else 1, 5 + back)
        source = lax.rem(y + back, 4)
        mixed = jnp.concatenate([recv3[2 * source], recv3[2 * source + 1]], axis=1)
        part = dot(mixed, out_w[pl.ds(pl.multiple_of(source * 256, 256), 256), :])
        if back == 0:
            total[...] = part
        else:
            total[...] += part
    for sender in range(2):
        arrived(1, 8 + sender)
        group = 2 * lax.rem(y + 3, 4) + 1 - sender
        part = dot(recv3[group], out_w[pl.ds(pl.multiple_of(group * 128, 128), 128), :])
        if sender == 0:
            total[...] += part
        else:
            out_ref[...] = (total[...] + part).astype(BF)

    for number, source in enumerate(
        [
            send1.at[:, pl.ds(0, ROWS - 1)], edge_out, send2, send3.at[pl.ds(0, n_col - 1)],
            gate_own,
        ]
    ):
        pltpu.make_async_copy(source, source, send_sems.at[number]).wait()


def local(
    tokens, norm_gain, first_gate, second_gate, value_weight, short_weight, short_bias,
    embed_weight, embed_bias, inner_weight, inner_bias, filter_freq, filter_weight, filter_skip,
    output_gain, output_weight,
):
    constants = make_constants()
    operands = [
        tokens, norm_gain[None], first_gate, second_gate, value_weight, short_weight, short_bias,
        embed_weight, embed_bias[None], inner_weight, inner_bias[None], filter_freq[None],
        jnp.swapaxes(filter_weight, 2, 3), filter_skip, output_gain[None], output_weight,
    ] + [
        jnp.asarray(constants[name])
        for name in ("twiddle", "tables", "feats")
    ]
    vmem = pltpu.VMEM
    scratch = [vmem(x.shape, x.dtype) for x in operands[0:2]]
    scratch += [vmem((WIDTH, 384), BF)]
    scratch += [vmem(x.shape, x.dtype) for x in operands[5:8]]
    scratch += [vmem((3, 1, 64), F32), vmem((64, 64), F32)]
    scratch += [vmem(x.shape, x.dtype) for x in operands[12:]]
    scratch += [
        vmem((256, WIDTH), BF),
        vmem((256, COLS), F32),
        vmem((256, COLS), F32),
        vmem((2, ROWS, 8, COLS), BF),
        vmem((2, ROWS, 8, COLS), BF),
        vmem((128, 128), F32),
        vmem((2 * LIVE * 8, COLS), F32),
        vmem((2, OWN * HALF, 2 * COLS), F32),
        vmem((2, 256, COLS), F32),
        vmem((ROWS, 8, COLS), BF),
        vmem((ROWS, 8, COLS), BF),
        vmem((8, 32, COLS), BF),
        vmem((8, 32, COLS), BF),
        vmem((264, COLS), F32),
        vmem((264, COLS), F32),
        vmem((2, 8, COLS), BF),
        vmem((2, 8, COLS), BF),
        vmem((32, WIDTH), F32),
        pltpu.SemaphoreType.DMA((15,)),
        pltpu.SemaphoreType.DMA((5,)),
        pltpu.SemaphoreType.DMA((10,)),
    ]
    return pl.pallas_call(
        kernel,
        out_shape=pltpu.VMEM((32, WIDTH), BF),
        in_specs=[pl.BlockSpec(memory_space=pltpu.HBM)] * len(operands),
        out_specs=pl.BlockSpec(memory_space=pltpu.VMEM),
        scratch_shapes=scratch,
        compiler_params=pltpu.CompilerParams(
            collective_id=0, has_side_effects=True, vmem_limit_bytes=66_912_256
        ),
    )(*operands)


def solution(mesh):
    in_specs = (
        P("row", None),
        P(),
        P(None, "col"),
        P(None, "col"),
        P(None, "col"),
        P(None, None, "col"),
        P(None, "col"),
        P(),
        P(),
        P(),
        P(),
        P(),
        P(None, None, None, ("col", "row")),
        P(None, ("col", "row")),
        P("col"),
        P(),
    )
    out_specs = P(("row", "col"), None)
    return jax.shard_map(local, mesh=mesh, in_specs=in_specs, out_specs=out_specs, check_vma=False)
```

```python
import math

import jax
import jax.numpy as jnp
import ml_dtypes
import numpy as np
from jax import lax
from jax.experimental import pallas as pl
from jax.experimental.pallas import tpu as pltpu
from jax.sharding import PartitionSpec as P

CHANNELS = 1024
GROUPS = 8
FREQ_BANDS = 16
NORM_EPS = 1e-06
DECAY_TARGET = 0.01
FAST_SPAN = 0.3
SLOW_SPAN = 1.5

LENGTH = 8192
WIDTH = 2048
COLS = 128
LIVE = 64
EAGER = 1
HALF = 72
TOTAL = 16384
ROWS = 32
OWN = 4
FEATS = 48
CHUNK = 2048


def farthest_first(steps):
    return [step for step in sorted(steps, reverse=True) if any(step[1])]


ROW_HOPS = farthest_first(
    [(min(dz, 8 - dz) + min(dx, 4 - dx), (dz, dx)) for dz in range(8) for dx in range(4)]
)
FAR_ROWS = [offset for _, offset in ROW_HOPS]
COL_HOPS = farthest_first(
    [(2 * min(dy, 4 - dy) + dc, (dy, dc)) for dy in range(4) for dc in range(2)]
)
FAR_COLS = [offset for _, offset in COL_HOPS]

BF = jnp.bfloat16
F32 = jnp.float32
MESH = pl.DeviceIdType.MESH


def split_np(matrix):
    high = matrix.astype(np.float32).astype(ml_dtypes.bfloat16)
    low = (matrix - high.astype(np.float64)).astype(np.float32).astype(ml_dtypes.bfloat16)
    return high, low


def make_constants():
    k1 = np.arange(HALF)
    a = np.arange(LIVE)
    b = np.arange(COLS)
    cos_in = np.cos(2 * np.pi * np.outer(k1, a) / COLS)
    sin_in = np.sin(2 * np.pi * np.outer(k1, a) / COLS)
    first = np.concatenate([cos_in, -sin_in], 0)
    turn = 2 * np.pi * np.outer(k1, b) / TOTAL
    twiddle = np.concatenate([np.cos(turn), np.sin(turn)], 1).astype(np.float32)
    cos_out = np.cos(2 * np.pi * (np.outer(b, b) % COLS) / COLS)
    sin_out = np.sin(2 * np.pi * (np.outer(b, b) % COLS) / COLS)
    second = np.block([[cos_out, -sin_out], [sin_out, cos_out]])
    back = np.block([[cos_out, sin_out], [-sin_out, cos_out]])
    weight = np.where((k1 == 0) | (k1 == COLS // 2), 1.0, 2.0) * (k1 <= COLS // 2)
    last = np.concatenate([cos_in.T * weight, -sin_in.T * weight], 1) / TOTAL
    tables = np.zeros((720, 2 * COLS))
    tables[0:256] = second
    tables[256:512] = back
    tables[512 : 512 + 2 * HALF, :LIVE] = first
    tables[656:720, : 2 * HALF] = last
    n = np.arange(LENGTH)
    ramp = np.linspace(0.0, 1.0, LENGTH)[None, :]
    bands = np.linspace(0.0001, FREQ_BANDS - 1, FREQ_BANDS, dtype=np.float32).astype(np.float64)
    angle = bands[:, None] * (2 * np.pi * n / LENGTH)[None, :]
    feats = np.zeros((FEATS, LENGTH))
    feats[0:1] = ramp
    feats[1 : 1 + FREQ_BANDS] = np.cos(angle)
    feats[1 + FREQ_BANDS : 1 + 2 * FREQ_BANDS] = -np.sin(angle)
    feats[1 + 2 * FREQ_BANDS] = 1.0
    return dict(
        twiddle=twiddle,
        tables=split_np(tables)[0],
        feats=np.concatenate(split_np(feats), 0),
    )


def sine_coefficients():
    v = 0.25 * np.cos(np.pi * (np.arange(400) + 0.5) / 800)
    basis = np.stack([v ** (2 * j + 1) for j in range(5)], 1)
    scale = 1.0 / np.sin(2 * np.pi * v)
    found = np.linalg.lstsq(basis * scale[:, None], np.ones_like(v), rcond=None)[0]
    return [float(c) for c in found]


SINE = sine_coefficients()


def sine_of_turns(turns):
    v = 0.25 - jnp.abs(turns - jnp.round(turns))
    square = v * v
    result = SINE[4]
    for c in SINE[3::-1]:
        result = result * square + c
    return result * v


def split(value):
    high = value.astype(BF)
    return high, (value - high.astype(F32)).astype(BF)


def dot(left, right):
    return jnp.dot(left, right, preferred_element_type=F32)


def tall(value):
    high, low = split(value)
    return jnp.concatenate([high, high, low], axis=0)


def wide(value):
    high, low = split(value)
    return jnp.concatenate([high, low, high], axis=1)


def into_spectrum(signal, tables, twiddle):
    part = dot(tables[512:656, :LIVE], signal.astype(BF))
    cos, sin = twiddle[:, :COLS], twiddle[:, COLS:]
    pieces = []
    for i in range(signal.shape[1] // COLS):
        real = part[:HALF, i * COLS : (i + 1) * COLS]
        imag = part[HALF:, i * COLS : (i + 1) * COLS]
        pieces.append(jnp.concatenate([real * cos + imag * sin, imag * cos - real * sin], axis=1))
    return jnp.concatenate(pieces, axis=0).astype(BF)


def from_spectrum(spectrum, tables, twiddle):
    part = dot(spectrum.astype(BF), tables[256:512, :])
    cos, sin = twiddle[:, :COLS], twiddle[:, COLS:]
    reals, imags = [], []
    for i in range(spectrum.shape[0] // HALF):
        real = part[i * HALF : (i + 1) * HALF, :COLS]
        imag = part[i * HALF : (i + 1) * HALF, COLS:]
        reals.append(real * cos - imag * sin)
        imags.append(real * sin + imag * cos)
    turned = jnp.concatenate(
        [jnp.concatenate(reals, axis=1), jnp.concatenate(imags, axis=1)], axis=0
    )
    return dot(tables[656:720, : 2 * HALF], turned.astype(BF))


def kernel(
    tokens_hbm, norm_gain_hbm, gate0_hbm, gate1_hbm, gate2_hbm, short_w_hbm, short_b_hbm,
    embed_w_hbm, embed_b_hbm, inner_w_hbm, inner_b_hbm, freq_hbm, filter_w_hbm, skip_hbm,
    out_gain_hbm, out_w_hbm, twiddle_hbm, tables_hbm, feats_hbm,
    out_ref,
    tokens, gains, gates, short_w, short_b, layers, lines,
    filter_w, skip, out_w, twiddle, tables, feats,
    normed, flat, packed, send1, recv1, params, mixed_taps, spectra, smooth,
    send2, recv2, send3, recv3, gate_own, gate_in, gate_rows, edge_out, edge_in, total, load_sem, send_sem, recv_sems,
):
    me = lax.axis_index("row")
    col = lax.axis_index("col")
    n_col = 8

    def loaded(*targets):
        for target, number in targets:
            pltpu.make_async_copy(target, target, load_sem.at[number]).wait()

    barrier = pltpu.get_barrier_semaphore()

    z, x = lax.div(me, 4), lax.rem(me, 4)
    row_peers = [lax.rem(z + dz, 8) * 4 + lax.rem(x + dx, 4) for dz, dx in FAR_ROWS]
    y, core = lax.div(col, 2), lax.rem(col, 2)
    partner = y * 2 + 1 - core
    col_peers = [lax.rem(y + dy, 4) * 2 + lax.rem(core + dc, 2) for dy, dc in FAR_COLS]
    for there in row_peers:
        pl.semaphore_signal(barrier, inc=1, device_id=(there, col), device_id_type=MESH)
    copies = [
        (tokens_hbm, tokens, 0),
        (norm_gain_hbm, gains.at[:, 0:WIDTH], 1),
        (gate0_hbm, gates.at[:, 0:128], 2),
        (gate1_hbm, gates.at[:, 128:256], 2),
        (gate2_hbm, gates.at[:, 256:384], 2),
        (embed_w_hbm, layers.at[64:97], 3),
        (embed_b_hbm, lines.at[0], 4),
        (inner_b_hbm, lines.at[1], 4),
        (freq_hbm, lines.at[2], 4),
        (inner_w_hbm, layers.at[0:64], 3),
        (filter_w_hbm, filter_w, 6),
        (feats_hbm, feats, 7),
        (tables_hbm, tables, 8),
        (twiddle_hbm, twiddle, 9),
        (short_w_hbm, short_w, 10),
        (short_b_hbm, short_b, 11),
        (skip_hbm, skip, 12),
        (out_gain_hbm, gains.at[:, WIDTH : WIDTH + COLS], 1),
        (out_w_hbm, out_w, 5),
    ]
    for source, target, number in copies:
        pltpu.make_async_copy(source, target, load_sem.at[number]).start()

    for there in col_peers:
        pl.semaphore_signal(barrier, inc=1, device_id=(me, there), device_id_type=MESH)

    loaded((tokens, 0), (gains, 1))

    def normalise(j, carry):
        rows = pl.ds(pl.multiple_of(j * 64, 64), 64)
        wide_tokens = tokens[rows, :].astype(F32)
        mean = jnp.mean(wide_tokens * wide_tokens, axis=1, keepdims=True)
        normed[rows, :] = (wide_tokens * lax.rsqrt(mean + NORM_EPS) * gains[:, 0:WIDTH]).astype(BF)
        return carry

    lax.fori_loop(0, 4, normalise, 0)
    loaded((gates, 2))
    projected = dot(normed[...], gates[...])
    projected = projected.astype(BF).astype(F32)
    gate_own[0:256, :] = projected[:, 128:256]
    edge_out[0] = projected[248:256, 128:256].astype(BF)
    edge_out[1] = projected[0:8, 128:256].astype(BF)
    for b in range(2):
        turned = projected[:, b * 256 : b * 256 + 128].T
        for half in range(2):
            flat[pl.ds(half * 128, 128), :] = turned[:, half * 128 : (half + 1) * 128]
        for half in range(2):
            for i in range(OWN):
                packed[pl.ds(4 * half + i, ROWS, stride=8), :] = flat[
                    pl.ds(128 * half + i, ROWS, stride=4), :
                ]
        send1[b] = packed[...].reshape(ROWS, 8, COLS).astype(BF)

    pl.semaphore_wait(barrier, ROWS - 1 + n_col - 1)

    urgency = [(hops - 1 + b, b, k) for k, (hops, _) in enumerate(ROW_HOPS) for b in range(2)]
    for _, b, k in sorted(urgency, key=lambda item: (-item[0], -item[1], item[2])):
        there = row_peers[k]
        pltpu.make_async_remote_copy(
            src_ref=send1.at[b, there],
            dst_ref=recv1.at[b, me],
            send_sem=send_sem,
            recv_sem=recv_sems.at[2 * b],
            device_id=(there, col),
            device_id_type=MESH,
        ).start()
    for b in range(2):
        recv1[b, me] = send1[b, me]
    for side, there in ((0, lax.rem(me + 1, ROWS)), (1, lax.rem(me + ROWS - 1, ROWS))):
        pltpu.make_async_remote_copy(
            src_ref=edge_out.at[side],
            dst_ref=edge_in.at[side],
            send_sem=send_sem,
            recv_sem=recv_sems.at[1],
            device_id=(there, col),
            device_id_type=MESH,
        ).start()

    loaded((layers, 3), (lines, 4), (filter_w, 6), (feats, 7), (tables, 8))
    loaded((twiddle, 9))
    params[...] = jnp.zeros_like(params)
    scale = lines[2] * (1.0 / (2.0 * math.pi))
    params[0:33, 0:64] = layers[64:97] * scale
    params[33:34, 0:64] = lines[0] * scale - 0.25
    params[48:49, 0:64] = lines[1] * scale - 0.25
    params[64:128, 0:64] = layers[0:64] * scale
    turned = params[...].T
    embed_t = wide(turned[0:64, 0:FEATS])
    inner_bias = turned[0:64, 48:49]
    inner_t = wide(turned[0:64, 64:128])
    filter_t = wide(
        jnp.concatenate([filter_w[o, e] for o in range(2) for e in range(2)], axis=0)
    )

    row8 = lax.broadcasted_iota(jnp.int32, (8, 1), 0)
    channel = (col * ROWS + me) * OWN + lax.rem(row8, OWN)
    fastest = math.log(DECAY_TARGET) / FAST_SPAN
    slowest = math.log(DECAY_TARGET) / SLOW_SPAN
    place = channel.astype(F32) * (1.0 / (CHANNELS - 1))
    decay = jnp.abs(slowest * (1.0 - place) + fastest * place)

    def taps_of(j, carry):
        start = pl.multiple_of(j * CHUNK, CHUNK)
        lanes = pl.ds(start, CHUNK)
        high, low = feats[0:FEATS, lanes], feats[FEATS:, lanes]
        hidden = sine_of_turns(dot(embed_t, jnp.concatenate([high, high, low], axis=0)))
        hidden = sine_of_turns(dot(inner_t, tall(hidden)) + inner_bias)
        taps = dot(filter_t, tall(hidden))
        lag = start + lax.broadcasted_iota(jnp.int32, (8, CHUNK), 1)
        row = lax.broadcasted_iota(jnp.int32, (8, CHUNK), 0)
        window = jnp.exp(-(lag.astype(F32) * (1.0 / (LENGTH - 1))) * decay)
        window = jnp.where((lag == 0) & (row >= OWN), 0.0, window)
        for o in range(2):
            both = taps[8 * o : 8 * o + 8] * window
            other = pltpu.roll(both, OWN, axis=0)
            both = jnp.where(row < OWN, both + other, other - both)
            for q in range(CHUNK // COLS):
                at = pl.multiple_of(start // COLS * 8, 8) + o * LIVE * 8 + q * 8
                mixed_taps[pl.ds(pl.multiple_of(at, 8), 8), :] = both[:, q * COLS : (q + 1) * COLS]
        return carry

    lax.fori_loop(0, LENGTH // CHUNK, taps_of, 0)
    for o in range(2):
        for part in range(2):
            signal = jnp.concatenate(
                [
                    mixed_taps[pl.ds(o * LIVE * 8 + part * OWN + i, LIVE, stride=8), :]
                    for i in range(OWN)
                ],
                axis=1,
            )
            spectra[o, :, part * COLS : (part + 1) * COLS] = dot(
                into_spectrum(signal, tables, twiddle),
                tables[0:256, part * COLS : (part + 1) * COLS],
            )

    loaded((short_w, 10), (short_b, 11), (skip, 12))
    lane8 = lax.broadcasted_iota(jnp.int32, (8, COLS), 1)
    mine = lane8 == OWN * me + lax.rem(lax.broadcasted_iota(jnp.int32, (8, COLS), 0), OWN)

    def own_column(line):
        return jnp.sum(
            jnp.where(mine, jnp.broadcast_to(line, (8, COLS)), 0.0), axis=1, keepdims=True
        )

    all_short = short_w[...].astype(F32)
    columns = [
        [own_column(all_short[b, j : j + 1]) for j in range(3)] + [own_column(short_b[b : b + 1, :])]
        for b in (0, 2)
    ]

    def wait_row(target, number):
        pltpu.make_async_copy(
            target.at[pl.ds(0, ROWS - 1)], target.at[pl.ds(0, ROWS - 1)], recv_sems.at[number]
        ).wait()

    pltpu.make_async_copy(edge_in, edge_in, recv_sems.at[1]).wait()
    position = lax.broadcasted_iota(jnp.int32, (256, COLS), 0)
    here = gate_own[0:256, :]
    first_edge = edge_in[0].astype(F32)[7:8] * jnp.where(me == 0, 0.0, 1.0)
    last_edge = edge_in[1].astype(F32)[0:1] * jnp.where(me == ROWS - 1, 0.0, 1.0)
    before = jnp.where(position == 0, first_edge, pltpu.roll(here, 1, axis=0))
    after = jnp.where(position == 255, last_edge, pltpu.roll(here, 255, axis=0))
    value = short_b[1:2, :] + before * all_short[1, 0:1]
    value = value + here * all_short[1, 1:2]
    gate_own[0:256, :] = value + after * all_short[1, 2:3]
    gate_own[256:264, :] = jnp.broadcast_to(gains[:, WIDTH : WIDTH + COLS], (8, COLS))
    pltpu.make_async_remote_copy(
        src_ref=gate_own,
        dst_ref=gate_in,
        send_sem=send_sem,
        recv_sem=recv_sems.at[4],
        device_id=(me, partner),
        device_id_type=MESH,
    ).start()

    row = lax.broadcasted_iota(jnp.int32, (256, COLS), 0)
    lane = lax.broadcasted_iota(jnp.int32, (256, COLS), 1)

    def smoothed(b):
        wait_row(recv1.at[b], 2 * b)
        here = recv1[b].astype(F32).reshape(256, COLS)
        before = pltpu.roll(here, 1, axis=1)
        before = jnp.where(lane == 0, pltpu.roll(before, OWN, axis=0), before)
        before = jnp.where((lane == 0) & (row < OWN), 0.0, before)
        after = pltpu.roll(here, COLS - 1, axis=1)
        after = jnp.where(lane == COLS - 1, pltpu.roll(after, 256 - OWN, axis=0), after)
        after = jnp.where((lane == COLS - 1) & (row >= 256 - OWN), 0.0, after)
        tap = [jnp.broadcast_to(c, (8, COLS))[None] for c in columns[b]]
        shape = (ROWS, 8, COLS)
        value = tap[3] + before.reshape(shape) * tap[0]
        value = value + here.reshape(shape) * tap[1]
        value = value + after.reshape(shape) * tap[2]
        smooth[b] = value.reshape(256, COLS)
        return jnp.concatenate(
            [smooth[b, pl.ds(i, LIVE, stride=OWN), :] for i in range(OWN)], axis=1
        )

    pairs = 2
    value = smoothed(1)
    signals = [value[:, p * COLS : (p + pairs) * COLS] for p in range(0, OWN, pairs)]
    for o in range(2):
        spectrum = [
            dot(into_spectrum(signal, tables, twiddle), tables[0:256, :])
            for signal in signals
        ]
        products = []
        for p, found in enumerate(spectrum):
            real, imag = found[:, :COLS], found[:, COLS:]
            rows = slice(p * pairs * HALF, (p + 1) * pairs * HALF)
            t_real, t_imag = spectra[o, rows, :COLS], spectra[o, rows, COLS:]
            products.append(
                jnp.concatenate(
                    [real * t_real - imag * t_imag, real * t_imag + imag * t_real], axis=1
                )
            )
        convolved = [from_spectrum(product, tables, twiddle) for product in products]
        signals = [
            found
            + jnp.concatenate(
                [
                    signal[:, i * COLS : (i + 1) * COLS]
                    * jnp.broadcast_to(
                        skip[o : o + 1, p * pairs + i : p * pairs + i + 1], (LIVE, COLS)
                    )
                    for i in range(pairs)
                ],
                axis=1,
            )
            for p, (found, signal) in enumerate(zip(convolved, signals))
        ]
        if o == 0:
            gate = smoothed(0)
            signals = [
                signal * gate[:, p * pairs * COLS : (p + 1) * pairs * COLS]
                for p, signal in enumerate(signals)
            ]
    signal = jnp.concatenate(signals, axis=1)

    for i in range(OWN):
        flat[pl.ds(i * LIVE, LIVE), :] = signal[:, i * COLS : (i + 1) * COLS]
    for i in range(OWN):
        for half in range(2):
            packed[pl.ds(2 * i + half, ROWS, stride=8), :] = flat[
                pl.ds(i * LIVE + half, ROWS, stride=2), :
            ]
    send2[...] = packed[...].reshape(ROWS, 8, COLS).astype(BF)

    for there in row_peers + [me]:
        pltpu.make_async_remote_copy(
            src_ref=send2.at[there],
            dst_ref=recv2.at[me],
            send_sem=send_sem,
            recv_sem=recv_sems.at[3],
            device_id=(there, partner),
            device_id_type=MESH,
        ).start()
    pltpu.make_async_copy(gate_in, gate_in, recv_sems.at[4]).wait()
    gain = jnp.broadcast_to(gate_in[256:257], (COLS, COLS)).T
    for half in range(2):
        gate_rows[0, pl.ds(half, COLS, stride=2), :] = gate_in[half * 128 : half * 128 + 128].T
        gate_rows[1, pl.ds(half, COLS, stride=2), :] = gain

    pltpu.make_async_copy(recv2, recv2, recv_sems.at[3]).wait()

    def send_over(there, back):
        pltpu.make_async_remote_copy(
            src_ref=send3.at[there],
            dst_ref=recv3.at[partner],
            send_sem=send_sem,
            recv_sem=recv_sems.at[5 + back + core * (back // 3)],
            device_id=(me, there),
            device_id_type=MESH,
        ).start()

    gated = recv2[...].astype(F32) * gate_rows[0].reshape(ROWS, 8, COLS)
    squares = jnp.sum(gated * gated, axis=0)
    squares = squares + pltpu.roll(squares, 4, axis=0)
    squares = squares + pltpu.roll(squares, 2, axis=0)
    factor = lax.rsqrt(squares * (GROUPS / CHANNELS) + NORM_EPS)
    gated = gated * factor[None] * gate_rows[1].reshape(ROWS, 8, COLS)
    flat[...] = gated.reshape(256, COLS)
    for half in range(2):
        gated = flat[pl.ds(half, COLS, stride=2), :].T
        send3[4 * half : 4 * half + 4] = gated.reshape(4, 32, COLS).astype(BF)
        if half == EAGER // 4:
            pl.when(col != EAGER)(lambda: send_over(EAGER, lax.rem(y + 4 - EAGER // 2, 4)))

    for (dy, _), there in zip(FAR_COLS, col_peers):
        pl.when(there != EAGER)(lambda there=there, dy=dy: send_over(there, (4 - dy) % 4))
    recv3[partner] = send3[col]
    loaded((out_w, 5))

    def arrived(count, number):
        block = recv3.at[pl.ds(0, count)]
        pltpu.make_async_copy(block, block, recv_sems.at[number]).wait()

    for back in range(3):
        arrived(2 if back else 1, 5 + back)
        source = lax.rem(y + back, 4)
        mixed = jnp.concatenate([recv3[2 * source], recv3[2 * source + 1]], axis=1)
        part = dot(mixed, out_w[pl.ds(pl.multiple_of(source * 256, 256), 256), :])
        if back == 0:
            total[...] = part
        else:
            total[...] += part
    for sender in range(2):
        arrived(1, 8 + sender)
        group = 2 * lax.rem(y + 3, 4) + 1 - sender
        part = dot(recv3[group], out_w[pl.ds(pl.multiple_of(group * 128, 128), 128), :])
        if sender == 0:
            total[...] += part
        else:
            out_ref[...] = (total[...] + part).astype(BF)

    sent = mixed_taps.at[pl.ds(0, 760)]
    pltpu.make_async_copy(sent, sent, send_sem).wait()


def local(
    tokens, norm_gain, first_gate, second_gate, value_weight, short_weight, short_bias,
    embed_weight, embed_bias, inner_weight, inner_bias, filter_freq, filter_weight, filter_skip,
    output_gain, output_weight,
):
    constants = make_constants()
    operands = [
        tokens, norm_gain[None], first_gate, second_gate, value_weight, short_weight, short_bias,
        embed_weight, embed_bias[None], inner_weight, inner_bias[None], filter_freq[None],
        jnp.swapaxes(filter_weight, 2, 3), filter_skip, output_gain[None], output_weight,
    ] + [
        jnp.asarray(constants[name])
        for name in ("twiddle", "tables", "feats")
    ]
    vmem = pltpu.VMEM
    scratch = [vmem(tokens.shape, BF), vmem((1, WIDTH + COLS), F32), vmem((WIDTH, 384), BF)]
    scratch += [vmem(x.shape, x.dtype) for x in operands[5:7]]
    scratch += [vmem((97, 64), F32), vmem((3, 1, 64), F32)]
    scratch += [vmem(x.shape, x.dtype) for x in operands[12:14] + operands[15:]]
    scratch += [
        vmem((256, WIDTH), BF),
        vmem((256, COLS), F32),
        vmem((256, COLS), F32),
        vmem((2, ROWS, 8, COLS), BF),
        vmem((2, ROWS, 8, COLS), BF),
        vmem((128, 128), F32),
        vmem((2 * LIVE * 8, COLS), F32),
        vmem((2, OWN * HALF, 2 * COLS), F32),
        vmem((2, 256, COLS), F32),
        vmem((ROWS, 8, COLS), BF),
        vmem((ROWS, 8, COLS), BF),
        vmem((8, 32, COLS), BF),
        vmem((8, 32, COLS), BF),
        vmem((264, COLS), F32),
        vmem((264, COLS), F32),
        vmem((2, 256, COLS), F32),
        vmem((2, 8, COLS), BF),
        vmem((2, 8, COLS), BF),
        vmem((32, WIDTH), F32),
        pltpu.SemaphoreType.DMA((13,)),
        pltpu.SemaphoreType.DMA(()),
        pltpu.SemaphoreType.DMA((10,)),
    ]
    return pl.pallas_call(
        kernel,
        out_shape=pltpu.VMEM((32, WIDTH), BF),
        in_specs=[pl.BlockSpec(memory_space=pltpu.HBM)] * len(operands),
        out_specs=pl.BlockSpec(memory_space=pltpu.VMEM),
        scratch_shapes=scratch,
        compiler_params=pltpu.CompilerParams(
            collective_id=0, has_side_effects=True, vmem_limit_bytes=66_912_256
        ),
    )(*operands)


def solution(mesh):
    in_specs = (
        P("row", None),
        P(),
        P(None, "col"),
        P(None, "col"),
        P(None, "col"),
        P(None, None, "col"),
        P(None, "col"),
        P(),
        P(),
        P(),
        P(),
        P(),
        P(None, None, None, ("col", "row")),
        P(None, ("col", "row")),
        P("col"),
        P(),
    )
    out_specs = P(("row", "col"), None)
    return jax.shard_map(local, mesh=mesh, in_specs=in_specs, out_specs=out_specs, check_vma=False)
```

```python
import math

import jax
import jax.numpy as jnp
import ml_dtypes
import numpy as np
from jax import lax
from jax.experimental import pallas as pl
from jax.experimental.pallas import tpu as pltpu
from jax.sharding import PartitionSpec as P

CHANNELS = 1024
GROUPS = 8
FREQ_BANDS = 16
NORM_EPS = 1e-06
DECAY_TARGET = 0.01
FAST_SPAN = 0.3
SLOW_SPAN = 1.5

LENGTH = 8192
WIDTH = 2048
COLS = 128
LIVE = 64
EAGER = 1
HALF = 72
TOTAL = 16384
ROWS = 32
OWN = 4
FEATS = 48
CHUNK = 2048


def farthest_first(steps):
    return [step for step in sorted(steps, reverse=True) if any(step[1])]


ROW_HOPS = farthest_first(
    [(min(dz, 8 - dz) + min(dx, 4 - dx), (dz, dx)) for dz in range(8) for dx in range(4)]
)
FAR_ROWS = [offset for _, offset in ROW_HOPS]
COL_HOPS = farthest_first(
    [(2 * min(dy, 4 - dy) + dc, (dy, dc)) for dy in range(4) for dc in range(2)]
)
FAR_COLS = [offset for _, offset in COL_HOPS]

BF = jnp.bfloat16
F32 = jnp.float32
MESH = pl.DeviceIdType.MESH


def split_np(matrix):
    high = matrix.astype(np.float32).astype(ml_dtypes.bfloat16)
    low = (matrix - high.astype(np.float64)).astype(np.float32).astype(ml_dtypes.bfloat16)
    return high, low


def make_constants():
    k1 = np.arange(HALF)
    a = np.arange(LIVE)
    b = np.arange(COLS)
    cos_in = np.cos(2 * np.pi * np.outer(k1, a) / COLS)
    sin_in = np.sin(2 * np.pi * np.outer(k1, a) / COLS)
    first = np.concatenate([cos_in, -sin_in], 0)
    turn = 2 * np.pi * np.outer(k1, b) / TOTAL
    twiddle = np.concatenate([np.cos(turn), np.sin(turn)], 1).astype(np.float32)
    cos_out = np.cos(2 * np.pi * (np.outer(b, b) % COLS) / COLS)
    sin_out = np.sin(2 * np.pi * (np.outer(b, b) % COLS) / COLS)
    second = np.block([[cos_out, -sin_out], [sin_out, cos_out]])
    back = np.block([[cos_out, sin_out], [-sin_out, cos_out]])
    weight = np.where((k1 == 0) | (k1 == COLS // 2), 1.0, 2.0) * (k1 <= COLS // 2)
    last = np.concatenate([cos_in.T * weight, -sin_in.T * weight], 1) / TOTAL
    tables = np.zeros((720, 2 * COLS))
    tables[0:256] = second
    tables[256:512] = back
    tables[512 : 512 + 2 * HALF, :LIVE] = first
    tables[656:720, : 2 * HALF] = last
    n = np.arange(LENGTH)
    ramp = np.linspace(0.0, 1.0, LENGTH)[None, :]
    bands = np.linspace(0.0001, FREQ_BANDS - 1, FREQ_BANDS, dtype=np.float32).astype(np.float64)
    angle = bands[:, None] * (2 * np.pi * n / LENGTH)[None, :]
    feats = np.zeros((FEATS, LENGTH))
    feats[0:1] = ramp
    feats[1 : 1 + FREQ_BANDS] = np.cos(angle)
    feats[1 + FREQ_BANDS : 1 + 2 * FREQ_BANDS] = -np.sin(angle)
    feats[1 + 2 * FREQ_BANDS] = 1.0
    return dict(
        twiddle=twiddle,
        tables=split_np(tables)[0],
        feats=np.concatenate(split_np(feats), 0),
    )


def sine_coefficients():
    v = 0.25 * np.cos(np.pi * (np.arange(400) + 0.5) / 800)
    basis = np.stack([v ** (2 * j + 1) for j in range(5)], 1)
    scale = 1.0 / np.sin(2 * np.pi * v)
    found = np.linalg.lstsq(basis * scale[:, None], np.ones_like(v), rcond=None)[0]
    return [float(c) for c in found]


SINE = sine_coefficients()


def sine_of_turns(turns):
    v = 0.25 - jnp.abs(turns - jnp.round(turns))
    square = v * v
    result = SINE[4]
    for c in SINE[3::-1]:
        result = result * square + c
    return result * v


def split(value):
    high = value.astype(BF)
    return high, (value - high.astype(F32)).astype(BF)


def dot(left, right):
    return jnp.dot(left, right, preferred_element_type=F32)


def tall(value):
    high, low = split(value)
    return jnp.concatenate([high, high, low], axis=0)


def wide(value):
    high, low = split(value)
    return jnp.concatenate([high, low, high], axis=1)


def into_spectrum(signal, tables, twiddle):
    part = dot(tables[512:656, :LIVE], signal.astype(BF))
    cos, sin = twiddle[:, :COLS], twiddle[:, COLS:]
    pieces = []
    for i in range(signal.shape[1] // COLS):
        real = part[:HALF, i * COLS : (i + 1) * COLS]
        imag = part[HALF:, i * COLS : (i + 1) * COLS]
        pieces.append(jnp.concatenate([real * cos + imag * sin, imag * cos - real * sin], axis=1))
    return jnp.concatenate(pieces, axis=0).astype(BF)


def from_spectrum(spectrum, tables, twiddle):
    part = dot(spectrum.astype(BF), tables[256:512, :])
    cos, sin = twiddle[:, :COLS], twiddle[:, COLS:]
    reals, imags = [], []
    for i in range(spectrum.shape[0] // HALF):
        real = part[i * HALF : (i + 1) * HALF, :COLS]
        imag = part[i * HALF : (i + 1) * HALF, COLS:]
        reals.append(real * cos - imag * sin)
        imags.append(real * sin + imag * cos)
    turned = jnp.concatenate(
        [jnp.concatenate(reals, axis=1), jnp.concatenate(imags, axis=1)], axis=0
    )
    return dot(tables[656:720, : 2 * HALF], turned.astype(BF))


def kernel(
    tokens_hbm, norm_gain_hbm, gate0_hbm, gate1_hbm, gate2_hbm, short_w_hbm, short_b_hbm,
    embed_w_hbm, embed_b_hbm, inner_w_hbm, inner_b_hbm, freq_hbm, filter_w_hbm, skip_hbm,
    out_gain_hbm, out_w_hbm, twiddle_hbm, tables_hbm, feats_hbm,
    out_ref,
    tokens, gains, gates, short_w, short_b, layers, lines,
    filter_w, skip, out_w, twiddle, tables, feats,
    normed, flat, packed, send1, recv1, params, mixed_taps, spectra, smooth,
    send2, recv2, send3, recv3, gate_own, gate_in, gate_rows, edge_out, edge_in, total, load_sem, send_sem, recv_sems,
):
    me = lax.axis_index("row")
    col = lax.axis_index("col")
    n_col = 8

    def loaded(*targets):
        for target, number in targets:
            pltpu.make_async_copy(target, target, load_sem.at[number]).wait()

    barrier = pltpu.get_barrier_semaphore()

    z, x = lax.div(me, 4), lax.rem(me, 4)
    row_peers = [lax.rem(z + dz, 8) * 4 + lax.rem(x + dx, 4) for dz, dx in FAR_ROWS]
    y, core = lax.div(col, 2), lax.rem(col, 2)
    partner = y * 2 + 1 - core
    col_peers = [lax.rem(y + dy, 4) * 2 + lax.rem(core + dc, 2) for dy, dc in FAR_COLS]
    for there in row_peers:
        pl.semaphore_signal(barrier, inc=1, device_id=(there, col), device_id_type=MESH)
    copies = [
        (tokens_hbm, tokens, 0),
        (norm_gain_hbm, gains.at[:, 0:WIDTH], 1),
        (gate0_hbm, gates.at[:, 0:128], 2),
        (gate1_hbm, gates.at[:, 128:256], 2),
        (gate2_hbm, gates.at[:, 256:384], 2),
        (embed_w_hbm, layers.at[64:97], 3),
        (embed_b_hbm, lines.at[0], 4),
        (inner_b_hbm, lines.at[1], 4),
        (freq_hbm, lines.at[2], 4),
        (inner_w_hbm, layers.at[0:64], 3),
        (filter_w_hbm, filter_w, 6),
        (feats_hbm, feats, 7),
        (tables_hbm, tables, 8),
        (twiddle_hbm, twiddle, 9),
        (short_w_hbm, short_w, 10),
        (short_b_hbm, short_b, 11),
        (skip_hbm, skip, 12),
        (out_gain_hbm, gains.at[:, WIDTH : WIDTH + COLS], 1),
        (out_w_hbm, out_w, 5),
    ]
    for source, target, number in copies:
        pltpu.make_async_copy(source, target, load_sem.at[number]).start()

    for there in col_peers:
        pl.semaphore_signal(barrier, inc=1, device_id=(me, there), device_id_type=MESH)

    loaded((tokens, 0), (gains, 1))

    def normalise(j, carry):
        rows = pl.ds(pl.multiple_of(j * 64, 64), 64)
        wide_tokens = tokens[rows, :].astype(F32)
        mean = jnp.mean(wide_tokens * wide_tokens, axis=1, keepdims=True)
        normed[rows, :] = (wide_tokens * lax.rsqrt(mean + NORM_EPS) * gains[:, 0:WIDTH]).astype(BF)
        return carry

    lax.fori_loop(0, 4, normalise, 0)
    loaded((gates, 2))
    projected = dot(normed[...], gates[...])
    projected = projected.astype(BF).astype(F32)
    gate_own[0:256, :] = projected[:, 128:256]
    edge_out[0] = projected[248:256, 128:256].astype(BF)
    edge_out[1] = projected[0:8, 128:256].astype(BF)
    for b in range(2):
        turned = projected[:, b * 256 : b * 256 + 128].T
        for half in range(2):
            flat[pl.ds(half * 128, 128), :] = turned[:, half * 128 : (half + 1) * 128]
        for half in range(2):
            for i in range(OWN):
                packed[pl.ds(4 * half + i, ROWS, stride=8), :] = flat[
                    pl.ds(128 * half + i, ROWS, stride=4), :
                ]
        send1[b] = packed[...].reshape(ROWS, 8, COLS).astype(BF)

    pl.semaphore_wait(barrier, ROWS - 1 + n_col - 1)

    urgency = [(hops - 1 + b, b, k) for k, (hops, _) in enumerate(ROW_HOPS) for b in range(2)]
    for _, b, k in sorted(urgency, key=lambda item: (-item[0], -item[1], item[2])):
        there = row_peers[k]
        pltpu.make_async_remote_copy(
            src_ref=send1.at[b, there],
            dst_ref=recv1.at[b, me],
            send_sem=send_sem,
            recv_sem=recv_sems.at[2 * b],
            device_id=(there, col),
            device_id_type=MESH,
        ).start()
    for b in range(2):
        recv1[b, me] = send1[b, me]
    for side, there in ((0, lax.rem(me + 1, ROWS)), (1, lax.rem(me + ROWS - 1, ROWS))):
        pltpu.make_async_remote_copy(
            src_ref=edge_out.at[side],
            dst_ref=edge_in.at[side],
            send_sem=send_sem,
            recv_sem=recv_sems.at[1],
            device_id=(there, col),
            device_id_type=MESH,
        ).start()

    loaded((layers, 3), (lines, 4), (filter_w, 6), (feats, 7), (tables, 8))
    loaded((twiddle, 9))
    params[...] = jnp.zeros_like(params)
    scale = lines[2] * (1.0 / (2.0 * math.pi))
    params[0:33, 0:64] = layers[64:97] * scale
    params[33:34, 0:64] = lines[0] * scale - 0.25
    params[48:49, 0:64] = lines[1] * scale - 0.25
    params[64:128, 0:64] = layers[0:64] * scale
    turned = params[...].T
    embed_t = wide(turned[0:64, 0:FEATS])
    inner_bias = turned[0:64, 48:49]
    inner_t = wide(turned[0:64, 64:128])
    filter_t = wide(
        jnp.concatenate([filter_w[o, e] for o in range(2) for e in range(2)], axis=0)
    )

    row8 = lax.broadcasted_iota(jnp.int32, (8, 1), 0)
    channel = (col * ROWS + me) * OWN + lax.rem(row8, OWN)
    fastest = math.log(DECAY_TARGET) / FAST_SPAN
    slowest = math.log(DECAY_TARGET) / SLOW_SPAN
    place = channel.astype(F32) * (1.0 / (CHANNELS - 1))
    decay = jnp.abs(slowest * (1.0 - place) + fastest * place)

    def taps_of(j, carry):
        start = pl.multiple_of(j * CHUNK, CHUNK)
        lanes = pl.ds(start, CHUNK)
        high, low = feats[0:FEATS, lanes], feats[FEATS:, lanes]
        hidden = sine_of_turns(dot(embed_t, jnp.concatenate([high, high, low], axis=0)))
        hidden = sine_of_turns(dot(inner_t, tall(hidden)) + inner_bias)
        taps = dot(filter_t, tall(hidden))
        lag = start + lax.broadcasted_iota(jnp.int32, (8, CHUNK), 1)
        row = lax.broadcasted_iota(jnp.int32, (8, CHUNK), 0)
        window = jnp.exp(-(lag.astype(F32) * (1.0 / (LENGTH - 1))) * decay)
        window = jnp.where((lag == 0) & (row >= OWN), 0.0, window)
        for o in range(2):
            both = taps[8 * o : 8 * o + 8] * window
            other = pltpu.roll(both, OWN, axis=0)
            both = jnp.where(row < OWN, both + other, other - both)
            for q in range(CHUNK // COLS):
                at = pl.multiple_of(start // COLS * 8, 8) + o * LIVE * 8 + q * 8
                mixed_taps[pl.ds(pl.multiple_of(at, 8), 8), :] = both[:, q * COLS : (q + 1) * COLS]
        return carry

    lax.fori_loop(0, LENGTH // CHUNK, taps_of, 0)
    for o in range(2):
        for part in range(2):
            signal = jnp.concatenate(
                [
                    mixed_taps[pl.ds(o * LIVE * 8 + part * OWN + i, LIVE, stride=8), :]
                    for i in range(OWN)
                ],
                axis=1,
            )
            spectra[o, :, part * COLS : (part + 1) * COLS] = dot(
                into_spectrum(signal, tables, twiddle),
                tables[0:256, part * COLS : (part + 1) * COLS],
            )

    loaded((short_w, 10), (short_b, 11), (skip, 12))
    lane8 = lax.broadcasted_iota(jnp.int32, (8, COLS), 1)
    mine = lane8 == OWN * me + lax.rem(lax.broadcasted_iota(jnp.int32, (8, COLS), 0), OWN)

    def own_column(line):
        return jnp.sum(
            jnp.where(mine, jnp.broadcast_to(line, (8, COLS)), 0.0), axis=1, keepdims=True
        )

    all_short = short_w[...].astype(F32)
    columns = [
        [own_column(all_short[b, j : j + 1]) for j in range(3)] + [own_column(short_b[b : b + 1, :])]
        for b in (0, 2)
    ]

    def wait_row(target, number):
        pltpu.make_async_copy(
            target.at[pl.ds(0, ROWS - 1)], target.at[pl.ds(0, ROWS - 1)], recv_sems.at[number]
        ).wait()

    row = lax.broadcasted_iota(jnp.int32, (256, COLS), 0)
    lane = lax.broadcasted_iota(jnp.int32, (256, COLS), 1)

    def smoothed(b):
        wait_row(recv1.at[b], 2 * b)
        here = recv1[b].astype(F32).reshape(256, COLS)
        before = pltpu.roll(here, 1, axis=1)
        before = jnp.where(lane == 0, pltpu.roll(before, OWN, axis=0), before)
        before = jnp.where((lane == 0) & (row < OWN), 0.0, before)
        after = pltpu.roll(here, COLS - 1, axis=1)
        after = jnp.where(lane == COLS - 1, pltpu.roll(after, 256 - OWN, axis=0), after)
        after = jnp.where((lane == COLS - 1) & (row >= 256 - OWN), 0.0, after)
        tap = [jnp.broadcast_to(c, (8, COLS))[None] for c in columns[b]]
        shape = (ROWS, 8, COLS)
        value = tap[3] + before.reshape(shape) * tap[0]
        value = value + here.reshape(shape) * tap[1]
        value = value + after.reshape(shape) * tap[2]
        smooth[b] = value.reshape(256, COLS)
        return jnp.concatenate(
            [smooth[b, pl.ds(i, LIVE, stride=OWN), :] for i in range(OWN)], axis=1
        )

    pairs = 2
    value = smoothed(1)
    signals = [value[:, p * COLS : (p + pairs) * COLS] for p in range(0, OWN, pairs)]
    for o in range(2):
        spectrum = [
            dot(into_spectrum(signal, tables, twiddle), tables[0:256, :])
            for signal in signals
        ]
        products = []
        for p, found in enumerate(spectrum):
            real, imag = found[:, :COLS], found[:, COLS:]
            rows = slice(p * pairs * HALF, (p + 1) * pairs * HALF)
            t_real, t_imag = spectra[o, rows, :COLS], spectra[o, rows, COLS:]
            products.append(
                jnp.concatenate(
                    [real * t_real - imag * t_imag, real * t_imag + imag * t_real], axis=1
                )
            )
        convolved = [from_spectrum(product, tables, twiddle) for product in products]
        signals = [
            found
            + jnp.concatenate(
                [
                    signal[:, i * COLS : (i + 1) * COLS]
                    * jnp.broadcast_to(
                        skip[o : o + 1, p * pairs + i : p * pairs + i + 1], (LIVE, COLS)
                    )
                    for i in range(pairs)
                ],
                axis=1,
            )
            for p, (found, signal) in enumerate(zip(convolved, signals))
        ]
        if o == 0:
            gate = smoothed(0)
            signals = [
                signal * gate[:, p * pairs * COLS : (p + 1) * pairs * COLS]
                for p, signal in enumerate(signals)
            ]
    signal = jnp.concatenate(signals, axis=1)

    for i in range(OWN):
        flat[pl.ds(i * LIVE, LIVE), :] = signal[:, i * COLS : (i + 1) * COLS]
    for i in range(OWN):
        for half in range(2):
            packed[pl.ds(2 * i + half, ROWS, stride=8), :] = flat[
                pl.ds(i * LIVE + half, ROWS, stride=2), :
            ]
    send2[...] = packed[...].reshape(ROWS, 8, COLS).astype(BF)

    for there in row_peers + [me]:
        pltpu.make_async_remote_copy(
            src_ref=send2.at[there],
            dst_ref=recv2.at[me],
            send_sem=send_sem,
            recv_sem=recv_sems.at[3],
            device_id=(there, partner),
            device_id_type=MESH,
        ).start()
    pltpu.make_async_copy(edge_in, edge_in, recv_sems.at[1]).wait()
    position = lax.broadcasted_iota(jnp.int32, (256, COLS), 0)
    here = gate_own[0:256, :]
    first_edge = edge_in[0].astype(F32)[7:8] * jnp.where(me == 0, 0.0, 1.0)
    last_edge = edge_in[1].astype(F32)[0:1] * jnp.where(me == ROWS - 1, 0.0, 1.0)
    before = jnp.where(position == 0, first_edge, pltpu.roll(here, 1, axis=0))
    after = jnp.where(position == 255, last_edge, pltpu.roll(here, 255, axis=0))
    value = short_b[1:2, :] + before * all_short[1, 0:1]
    value = value + here * all_short[1, 1:2]
    gate_own[0:256, :] = value + after * all_short[1, 2:3]
    gate_own[256:264, :] = jnp.broadcast_to(gains[:, WIDTH : WIDTH + COLS], (8, COLS))
    pltpu.make_async_remote_copy(
        src_ref=gate_own,
        dst_ref=gate_in,
        send_sem=send_sem,
        recv_sem=recv_sems.at[4],
        device_id=(me, partner),
        device_id_type=MESH,
    ).start()

    pltpu.make_async_copy(gate_in, gate_in, recv_sems.at[4]).wait()
    gain = jnp.broadcast_to(gate_in[256:257], (COLS, COLS)).T
    for half in range(2):
        gate_rows[0, pl.ds(half, COLS, stride=2), :] = gate_in[half * 128 : half * 128 + 128].T
        gate_rows[1, pl.ds(half, COLS, stride=2), :] = gain

    pltpu.make_async_copy(recv2, recv2, recv_sems.at[3]).wait()

    def send_over(there, back):
        pltpu.make_async_remote_copy(
            src_ref=send3.at[there],
            dst_ref=recv3.at[partner],
            send_sem=send_sem,
            recv_sem=recv_sems.at[5 + back + core * (back // 3)],
            device_id=(me, there),
            device_id_type=MESH,
        ).start()

    gated = recv2[...].astype(F32) * gate_rows[0].reshape(ROWS, 8, COLS)
    squares = jnp.sum(gated * gated, axis=0)
    squares = squares + pltpu.roll(squares, 4, axis=0)
    squares = squares + pltpu.roll(squares, 2, axis=0)
    factor = lax.rsqrt(squares * (GROUPS / CHANNELS) + NORM_EPS)
    gated = gated * factor[None] * gate_rows[1].reshape(ROWS, 8, COLS)
    flat[...] = gated.reshape(256, COLS)
    for half in range(2):
        gated = flat[pl.ds(half, COLS, stride=2), :].T
        send3[4 * half : 4 * half + 4] = gated.reshape(4, 32, COLS).astype(BF)
        if half == EAGER // 4:
            pl.when(col != EAGER)(lambda: send_over(EAGER, lax.rem(y + 4 - EAGER // 2, 4)))

    for (dy, _), there in zip(FAR_COLS, col_peers):
        pl.when(there != EAGER)(lambda there=there, dy=dy: send_over(there, (4 - dy) % 4))
    recv3[partner] = send3[col]
    loaded((out_w, 5))

    def arrived(count, number):
        block = recv3.at[pl.ds(0, count)]
        pltpu.make_async_copy(block, block, recv_sems.at[number]).wait()

    for back in range(3):
        arrived(2 if back else 1, 5 + back)
        source = lax.rem(y + back, 4)
        mixed = jnp.concatenate([recv3[2 * source], recv3[2 * source + 1]], axis=1)
        part = dot(mixed, out_w[pl.ds(pl.multiple_of(source * 256, 256), 256), :])
        if back == 0:
            total[...] = part
        else:
            total[...] += part
    for sender in range(2):
        arrived(1, 8 + sender)
        group = 2 * lax.rem(y + 3, 4) + 1 - sender
        part = dot(recv3[group], out_w[pl.ds(pl.multiple_of(group * 128, 128), 128), :])
        if sender == 0:
            total[...] += part
        else:
            out_ref[...] = (total[...] + part).astype(BF)

    sent = mixed_taps.at[pl.ds(0, 760)]
    pltpu.make_async_copy(sent, sent, send_sem).wait()


def local(
    tokens, norm_gain, first_gate, second_gate, value_weight, short_weight, short_bias,
    embed_weight, embed_bias, inner_weight, inner_bias, filter_freq, filter_weight, filter_skip,
    output_gain, output_weight,
):
    constants = make_constants()
    operands = [
        tokens, norm_gain[None], first_gate, second_gate, value_weight, short_weight, short_bias,
        embed_weight, embed_bias[None], inner_weight, inner_bias[None], filter_freq[None],
        jnp.swapaxes(filter_weight, 2, 3), filter_skip, output_gain[None], output_weight,
    ] + [
        jnp.asarray(constants[name])
        for name in ("twiddle", "tables", "feats")
    ]
    vmem = pltpu.VMEM
    scratch = [vmem(tokens.shape, BF), vmem((1, WIDTH + COLS), F32), vmem((WIDTH, 384), BF)]
    scratch += [vmem(x.shape, x.dtype) for x in operands[5:7]]
    scratch += [vmem((97, 64), F32), vmem((3, 1, 64), F32)]
    scratch += [vmem(x.shape, x.dtype) for x in operands[12:14] + operands[15:]]
    scratch += [
        vmem((256, WIDTH), BF),
        vmem((256, COLS), F32),
        vmem((256, COLS), F32),
        vmem((2, ROWS, 8, COLS), BF),
        vmem((2, ROWS, 8, COLS), BF),
        vmem((128, 128), F32),
        vmem((2 * LIVE * 8, COLS), F32),
        vmem((2, OWN * HALF, 2 * COLS), F32),
        vmem((2, 256, COLS), F32),
        vmem((ROWS, 8, COLS), BF),
        vmem((ROWS, 8, COLS), BF),
        vmem((8, 32, COLS), BF),
        vmem((8, 32, COLS), BF),
        vmem((264, COLS), F32),
        vmem((264, COLS), F32),
        vmem((2, 256, COLS), F32),
        vmem((2, 8, COLS), BF),
        vmem((2, 8, COLS), BF),
        vmem((32, WIDTH), F32),
        pltpu.SemaphoreType.DMA((13,)),
        pltpu.SemaphoreType.DMA(()),
        pltpu.SemaphoreType.DMA((10,)),
    ]
    return pl.pallas_call(
        kernel,
        out_shape=pltpu.VMEM((32, WIDTH), BF),
        in_specs=[pl.BlockSpec(memory_space=pltpu.HBM)] * len(operands),
        out_specs=pl.BlockSpec(memory_space=pltpu.VMEM),
        scratch_shapes=scratch,
        compiler_params=pltpu.CompilerParams(
            collective_id=0, has_side_effects=True, vmem_limit_bytes=66_912_256
        ),
    )(*operands)


def solution(mesh):
    in_specs = (
        P("row", None),
        P(),
        P(None, "col"),
        P(None, "col"),
        P(None, "col"),
        P(None, None, "col"),
        P(None, "col"),
        P(),
        P(),
        P(),
        P(),
        P(),
        P(None, None, None, ("col", "row")),
        P(None, ("col", "row")),
        P("col"),
        P(),
    )
    out_specs = P(("row", "col"), None)
    return jax.shard_map(local, mesh=mesh, in_specs=in_specs, out_specs=out_specs, check_vma=False)
```

```python
import math

import jax
import jax.numpy as jnp
import ml_dtypes
import numpy as np
from jax import lax
from jax.experimental import pallas as pl
from jax.experimental.pallas import tpu as pltpu
from jax.sharding import PartitionSpec as P

CHANNELS = 1024
GROUPS = 8
FREQ_BANDS = 16
NORM_EPS = 1e-06
DECAY_TARGET = 0.01
FAST_SPAN = 0.3
SLOW_SPAN = 1.5

LENGTH = 8192
WIDTH = 2048
COLS = 128
LIVE = 64
EAGER = 1
HALF = 72
TOTAL = 16384
ROWS = 32
OWN = 4
FEATS = 48
CHUNK = 2048


def farthest_first(steps):
    return [step for step in sorted(steps, reverse=True) if any(step[1])]


ROW_HOPS = farthest_first(
    [(min(dz, 8 - dz) + min(dx, 4 - dx), (dz, dx)) for dz in range(8) for dx in range(4)]
)
FAR_ROWS = [offset for _, offset in ROW_HOPS]
COL_HOPS = farthest_first(
    [(2 * min(dy, 4 - dy) + dc, (dy, dc)) for dy in range(4) for dc in range(2)]
)
FAR_COLS = [offset for _, offset in COL_HOPS]

BF = jnp.bfloat16
F32 = jnp.float32
MESH = pl.DeviceIdType.MESH


def split_np(matrix):
    high = matrix.astype(np.float32).astype(ml_dtypes.bfloat16)
    low = (matrix - high.astype(np.float64)).astype(np.float32).astype(ml_dtypes.bfloat16)
    return high, low


def make_constants():
    k1 = np.arange(HALF)
    a = np.arange(LIVE)
    b = np.arange(COLS)
    cos_in = np.cos(2 * np.pi * np.outer(k1, a) / COLS)
    sin_in = np.sin(2 * np.pi * np.outer(k1, a) / COLS)
    first = np.concatenate([cos_in, -sin_in], 0)
    turn = 2 * np.pi * np.outer(k1, b) / TOTAL
    twiddle = np.concatenate([np.cos(turn), np.sin(turn)], 1).astype(np.float32)
    cos_out = np.cos(2 * np.pi * (np.outer(b, b) % COLS) / COLS)
    sin_out = np.sin(2 * np.pi * (np.outer(b, b) % COLS) / COLS)
    second = np.block([[cos_out, -sin_out], [sin_out, cos_out]])
    back = np.block([[cos_out, sin_out], [-sin_out, cos_out]])
    weight = np.where((k1 == 0) | (k1 == COLS // 2), 1.0, 2.0) * (k1 <= COLS // 2)
    last = np.concatenate([cos_in.T * weight, -sin_in.T * weight], 1) / TOTAL
    tables = np.zeros((720, 2 * COLS))
    tables[0:256] = second
    tables[256:512] = back
    tables[512 : 512 + 2 * HALF, :LIVE] = first
    tables[656:720, : 2 * HALF] = last
    n = np.arange(LENGTH)
    ramp = np.linspace(0.0, 1.0, LENGTH)[None, :]
    bands = np.linspace(0.0001, FREQ_BANDS - 1, FREQ_BANDS, dtype=np.float32).astype(np.float64)
    angle = bands[:, None] * (2 * np.pi * n / LENGTH)[None, :]
    feats = np.zeros((FEATS, LENGTH))
    feats[0:1] = ramp
    feats[1 : 1 + FREQ_BANDS] = np.cos(angle)
    feats[1 + FREQ_BANDS : 1 + 2 * FREQ_BANDS] = -np.sin(angle)
    feats[1 + 2 * FREQ_BANDS] = 1.0
    return dict(
        twiddle=twiddle,
        tables=split_np(tables)[0],
        feats=np.concatenate(split_np(feats), 0),
    )


def sine_coefficients():
    v = 0.25 * np.cos(np.pi * (np.arange(400) + 0.5) / 800)
    basis = np.stack([v ** (2 * j + 1) for j in range(5)], 1)
    scale = 1.0 / np.sin(2 * np.pi * v)
    found = np.linalg.lstsq(basis * scale[:, None], np.ones_like(v), rcond=None)[0]
    return [float(c) for c in found]


SINE = sine_coefficients()


def sine_of_turns(turns):
    v = 0.25 - jnp.abs(turns - jnp.round(turns))
    square = v * v
    result = SINE[4]
    for c in SINE[3::-1]:
        result = result * square + c
    return result * v


def split(value):
    high = value.astype(BF)
    return high, (value - high.astype(F32)).astype(BF)


def dot(left, right):
    return jnp.dot(left, right, preferred_element_type=F32)


def tall(value):
    high, low = split(value)
    return jnp.concatenate([high, high, low], axis=0)


def wide(value):
    high, low = split(value)
    return jnp.concatenate([high, low, high], axis=1)


def into_spectrum(signal, tables, twiddle):
    part = dot(tables[512:656, :LIVE], signal.astype(BF))
    cos, sin = twiddle[:, :COLS], twiddle[:, COLS:]
    pieces = []
    for i in range(signal.shape[1] // COLS):
        real = part[:HALF, i * COLS : (i + 1) * COLS]
        imag = part[HALF:, i * COLS : (i + 1) * COLS]
        pieces.append(jnp.concatenate([real * cos + imag * sin, imag * cos - real * sin], axis=1))
    return jnp.concatenate(pieces, axis=0).astype(BF)


def from_spectrum(spectrum, tables, twiddle):
    part = dot(spectrum.astype(BF), tables[256:512, :])
    cos, sin = twiddle[:, :COLS], twiddle[:, COLS:]
    reals, imags = [], []
    for i in range(spectrum.shape[0] // HALF):
        real = part[i * HALF : (i + 1) * HALF, :COLS]
        imag = part[i * HALF : (i + 1) * HALF, COLS:]
        reals.append(real * cos - imag * sin)
        imags.append(real * sin + imag * cos)
    turned = jnp.concatenate(
        [jnp.concatenate(reals, axis=1), jnp.concatenate(imags, axis=1)], axis=0
    )
    return dot(tables[656:720, : 2 * HALF], turned.astype(BF))


def kernel(
    tokens_hbm, norm_gain_hbm, gate0_hbm, gate1_hbm, gate2_hbm, short_w_hbm, short_b_hbm,
    embed_w_hbm, embed_b_hbm, inner_w_hbm, inner_b_hbm, freq_hbm, filter_w_hbm, skip_hbm,
    out_gain_hbm, out_w_hbm, twiddle_hbm, tables_hbm, feats_hbm,
    out_ref,
    tokens, gains, gates, short_w, short_b, layers, lines,
    filter_w, skip, out_w, twiddle, tables, feats,
    normed, flat, packed, send1, recv1, params, mixed_taps, spectra, smooth,
    send2, recv2, send3, recv3, gate_own, gate_in, gate_rows, edge_out, edge_in, total, load_sem, send_sem, recv_sems,
):
    me = lax.axis_index("row")
    col = lax.axis_index("col")
    n_col = 8

    def loaded(*targets):
        for target, number in targets:
            pltpu.make_async_copy(target, target, load_sem.at[number]).wait()

    barrier = pltpu.get_barrier_semaphore()

    z, x = lax.div(me, 4), lax.rem(me, 4)
    row_peers = [lax.rem(z + dz, 8) * 4 + lax.rem(x + dx, 4) for dz, dx in FAR_ROWS]
    y, core = lax.div(col, 2), lax.rem(col, 2)
    partner = y * 2 + 1 - core
    col_peers = [lax.rem(y + dy, 4) * 2 + lax.rem(core + dc, 2) for dy, dc in FAR_COLS]
    for there in row_peers:
        pl.semaphore_signal(barrier, inc=1, device_id=(there, col), device_id_type=MESH)
    copies = [
        (tokens_hbm, tokens, 0),
        (norm_gain_hbm, gains.at[:, 0:WIDTH], 1),
        (gate0_hbm, gates.at[:, 0:128], 2),
        (gate1_hbm, gates.at[:, 128:256], 2),
        (gate2_hbm, gates.at[:, 256:384], 2),
        (embed_w_hbm, layers.at[64:97], 3),
        (embed_b_hbm, lines.at[0], 4),
        (inner_b_hbm, lines.at[1], 4),
        (freq_hbm, lines.at[2], 4),
        (inner_w_hbm, layers.at[0:64], 3),
        (filter_w_hbm, filter_w, 6),
        (feats_hbm, feats, 7),
        (tables_hbm, tables, 8),
        (twiddle_hbm, twiddle, 9),
        (short_w_hbm, short_w, 10),
        (short_b_hbm, short_b, 11),
        (skip_hbm, skip, 12),
        (out_gain_hbm, gains.at[:, WIDTH : WIDTH + COLS], 1),
        (out_w_hbm, out_w, 5),
    ]
    for source, target, number in copies:
        pltpu.make_async_copy(source, target, load_sem.at[number]).start()

    for there in col_peers:
        pl.semaphore_signal(barrier, inc=1, device_id=(me, there), device_id_type=MESH)

    loaded((tokens, 0), (gains, 1))

    def normalise(j, carry):
        rows = pl.ds(pl.multiple_of(j * 64, 64), 64)
        wide_tokens = tokens[rows, :].astype(F32)
        mean = jnp.mean(wide_tokens * wide_tokens, axis=1, keepdims=True)
        normed[rows, :] = (wide_tokens * lax.rsqrt(mean + NORM_EPS) * gains[:, 0:WIDTH]).astype(BF)
        return carry

    lax.fori_loop(0, 4, normalise, 0)
    loaded((gates, 2))
    projected = dot(normed[...], gates[...])
    projected = projected.astype(BF).astype(F32)
    gate_own[0:256, :] = projected[:, 128:256]
    edge_out[0] = projected[248:256, 128:256].astype(BF)
    edge_out[1] = projected[0:8, 128:256].astype(BF)
    for b in range(2):
        turned = projected[:, b * 256 : b * 256 + 128].T
        for half in range(2):
            flat[pl.ds(half * 128, 128), :] = turned[:, half * 128 : (half + 1) * 128]
        for half in range(2):
            for i in range(OWN):
                packed[pl.ds(4 * half + i, ROWS, stride=8), :] = flat[
                    pl.ds(128 * half + i, ROWS, stride=4), :
                ]
        send1[b] = packed[...].reshape(ROWS, 8, COLS).astype(BF)

    pl.semaphore_wait(barrier, ROWS - 1 + n_col - 1)

    urgency = [(hops - 1 + b, b, k) for k, (hops, _) in enumerate(ROW_HOPS) for b in range(2)]
    for _, b, k in sorted(urgency, key=lambda item: (-item[0], -item[1], item[2])):
        there = row_peers[k]
        pltpu.make_async_remote_copy(
            src_ref=send1.at[b, there],
            dst_ref=recv1.at[b, me],
            send_sem=send_sem,
            recv_sem=recv_sems.at[2 * b],
            device_id=(there, col),
            device_id_type=MESH,
        ).start()
    for b in range(2):
        recv1[b, me] = send1[b, me]
    for side, there in ((0, lax.rem(me + 1, ROWS)), (1, lax.rem(me + ROWS - 1, ROWS))):
        pltpu.make_async_remote_copy(
            src_ref=edge_out.at[side],
            dst_ref=edge_in.at[side],
            send_sem=send_sem,
            recv_sem=recv_sems.at[1],
            device_id=(there, col),
            device_id_type=MESH,
        ).start()

    loaded((layers, 3), (lines, 4), (filter_w, 6), (feats, 7), (tables, 8))
    loaded((twiddle, 9))
    params[...] = jnp.zeros_like(params)
    scale = lines[2] * (1.0 / (2.0 * math.pi))
    params[0:33, 0:64] = layers[64:97] * scale
    params[33:34, 0:64] = lines[0] * scale - 0.25
    params[48:49, 0:64] = lines[1] * scale - 0.25
    params[64:128, 0:64] = layers[0:64] * scale
    turned = params[...].T
    embed_t = wide(turned[0:64, 0:FEATS])
    inner_bias = turned[0:64, 48:49]
    inner_t = wide(turned[0:64, 64:128])
    filter_t = wide(
        jnp.concatenate([filter_w[o, e] for o in range(2) for e in range(2)], axis=0)
    )

    row8 = lax.broadcasted_iota(jnp.int32, (8, 1), 0)
    channel = (col * ROWS + me) * OWN + lax.rem(row8, OWN)
    fastest = math.log(DECAY_TARGET) / FAST_SPAN
    slowest = math.log(DECAY_TARGET) / SLOW_SPAN
    place = channel.astype(F32) * (1.0 / (CHANNELS - 1))
    decay = jnp.abs(slowest * (1.0 - place) + fastest * place)

    def taps_of(j, carry):
        start = pl.multiple_of(j * CHUNK, CHUNK)
        lanes = pl.ds(start, CHUNK)
        high, low = feats[0:FEATS, lanes], feats[FEATS:, lanes]
        hidden = sine_of_turns(dot(embed_t, jnp.concatenate([high, high, low], axis=0)))
        hidden = sine_of_turns(dot(inner_t, tall(hidden)) + inner_bias)
        taps = dot(filter_t, tall(hidden))
        lag = start + lax.broadcasted_iota(jnp.int32, (8, CHUNK), 1)
        row = lax.broadcasted_iota(jnp.int32, (8, CHUNK), 0)
        window = jnp.exp(-(lag.astype(F32) * (1.0 / (LENGTH - 1))) * decay)
        window = jnp.where((lag == 0) & (row >= OWN), 0.0, window)
        for o in range(2):
            both = taps[8 * o : 8 * o + 8] * window
            other = pltpu.roll(both, OWN, axis=0)
            both = jnp.where(row < OWN, both + other, other - both)
            for q in range(CHUNK // COLS):
                at = pl.multiple_of(start // COLS * 8, 8) + o * LIVE * 8 + q * 8
                mixed_taps[pl.ds(pl.multiple_of(at, 8), 8), :] = both[:, q * COLS : (q + 1) * COLS]
        return carry

    lax.fori_loop(0, LENGTH // CHUNK, taps_of, 0)
    for o in range(2):
        for part in range(2):
            signal = jnp.concatenate(
                [
                    mixed_taps[pl.ds(o * LIVE * 8 + part * OWN + i, LIVE, stride=8), :]
                    for i in range(OWN)
                ],
                axis=1,
            )
            spectra[o, :, part * COLS : (part + 1) * COLS] = dot(
                into_spectrum(signal, tables, twiddle),
                tables[0:256, part * COLS : (part + 1) * COLS],
            )

    loaded((short_w, 10), (short_b, 11), (skip, 12))
    lane8 = lax.broadcasted_iota(jnp.int32, (8, COLS), 1)
    mine = lane8 == OWN * me + lax.rem(lax.broadcasted_iota(jnp.int32, (8, COLS), 0), OWN)

    def own_column(line):
        return jnp.sum(
            jnp.where(mine, jnp.broadcast_to(line, (8, COLS)), 0.0), axis=1, keepdims=True
        )

    all_short = short_w[...].astype(F32)
    columns = [
        [own_column(all_short[b, j : j + 1]) for j in range(3)] + [own_column(short_b[b : b + 1, :])]
        for b in (0, 2)
    ]

    def wait_row(target, number):
        pltpu.make_async_copy(
            target.at[pl.ds(0, ROWS - 1)], target.at[pl.ds(0, ROWS - 1)], recv_sems.at[number]
        ).wait()

    row = lax.broadcasted_iota(jnp.int32, (256, COLS), 0)
    lane = lax.broadcasted_iota(jnp.int32, (256, COLS), 1)

    def smoothed(b):
        wait_row(recv1.at[b], 2 * b)
        here = recv1[b].astype(F32).reshape(256, COLS)
        before = pltpu.roll(here, 1, axis=1)
        before = jnp.where(lane == 0, pltpu.roll(before, OWN, axis=0), before)
        before = jnp.where((lane == 0) & (row < OWN), 0.0, before)
        after = pltpu.roll(here, COLS - 1, axis=1)
        after = jnp.where(lane == COLS - 1, pltpu.roll(after, 256 - OWN, axis=0), after)
        after = jnp.where((lane == COLS - 1) & (row >= 256 - OWN), 0.0, after)
        tap = [jnp.broadcast_to(c, (8, COLS))[None] for c in columns[b]]
        shape = (ROWS, 8, COLS)
        value = tap[3] + before.reshape(shape) * tap[0]
        value = value + here.reshape(shape) * tap[1]
        value = value + after.reshape(shape) * tap[2]
        smooth[b] = value.reshape(256, COLS)
        return jnp.concatenate(
            [smooth[b, pl.ds(i, LIVE, stride=OWN), :] for i in range(OWN)], axis=1
        )

    pairs = 2
    value = smoothed(1)
    signals = [value[:, p * COLS : (p + pairs) * COLS] for p in range(0, OWN, pairs)]
    for o in range(2):
        spectrum = [
            dot(into_spectrum(signal, tables, twiddle), tables[0:256, :])
            for signal in signals
        ]
        products = []
        for p, found in enumerate(spectrum):
            real, imag = found[:, :COLS], found[:, COLS:]
            rows = slice(p * pairs * HALF, (p + 1) * pairs * HALF)
            t_real, t_imag = spectra[o, rows, :COLS], spectra[o, rows, COLS:]
            products.append(
                jnp.concatenate(
                    [real * t_real - imag * t_imag, real * t_imag + imag * t_real], axis=1
                )
            )
        convolved = [from_spectrum(product, tables, twiddle) for product in products]
        signals = [
            found
            + jnp.concatenate(
                [
                    signal[:, i * COLS : (i + 1) * COLS]
                    * jnp.broadcast_to(
                        skip[o : o + 1, p * pairs + i : p * pairs + i + 1], (LIVE, COLS)
                    )
                    for i in range(pairs)
                ],
                axis=1,
            )
            for p, (found, signal) in enumerate(zip(convolved, signals))
        ]
        if o == 0:
            gate = smoothed(0)
            signals = [
                signal * gate[:, p * pairs * COLS : (p + 1) * pairs * COLS]
                for p, signal in enumerate(signals)
            ]
    signal = jnp.concatenate(signals, axis=1)

    for i in range(OWN):
        flat[pl.ds(i * LIVE, LIVE), :] = signal[:, i * COLS : (i + 1) * COLS]
    for i in range(OWN):
        for half in range(2):
            packed[pl.ds(2 * i + half, ROWS, stride=8), :] = flat[
                pl.ds(i * LIVE + half, ROWS, stride=2), :
            ]
    send2[...] = packed[...].reshape(ROWS, 8, COLS).astype(BF)

    for there in row_peers + [me]:
        pltpu.make_async_remote_copy(
            src_ref=send2.at[there],
            dst_ref=recv2.at[me],
            send_sem=send_sem,
            recv_sem=recv_sems.at[3],
            device_id=(there, partner),
            device_id_type=MESH,
        ).start()
    pltpu.make_async_copy(edge_in, edge_in, recv_sems.at[1]).wait()
    position = lax.broadcasted_iota(jnp.int32, (256, COLS), 0)
    here = gate_own[0:256, :]
    first_edge = edge_in[0].astype(F32)[7:8] * jnp.where(me == 0, 0.0, 1.0)
    last_edge = edge_in[1].astype(F32)[0:1] * jnp.where(me == ROWS - 1, 0.0, 1.0)
    before = jnp.where(position == 0, first_edge, pltpu.roll(here, 1, axis=0))
    after = jnp.where(position == 255, last_edge, pltpu.roll(here, 255, axis=0))
    value = short_b[1:2, :] + before * all_short[1, 0:1]
    value = value + here * all_short[1, 1:2]
    gate_own[0:256, :] = value + after * all_short[1, 2:3]
    gate_own[256:264, :] = jnp.broadcast_to(gains[:, WIDTH : WIDTH + COLS], (8, COLS))
    pltpu.make_async_remote_copy(
        src_ref=gate_own,
        dst_ref=gate_in,
        send_sem=send_sem,
        recv_sem=recv_sems.at[4],
        device_id=(me, partner),
        device_id_type=MESH,
    ).start()

    pltpu.make_async_copy(gate_in, gate_in, recv_sems.at[4]).wait()
    gain = jnp.broadcast_to(gate_in[256:257], (COLS, COLS)).T
    for half in range(2):
        gate_rows[0, pl.ds(half, COLS, stride=2), :] = gate_in[half * 128 : half * 128 + 128].T
        gate_rows[1, pl.ds(half, COLS, stride=2), :] = gain

    pltpu.make_async_copy(recv2, recv2, recv_sems.at[3]).wait()

    def send_over(there, back):
        pltpu.make_async_remote_copy(
            src_ref=send3.at[there],
            dst_ref=recv3.at[partner],
            send_sem=send_sem,
            recv_sem=recv_sems.at[5 + back + core * (back // 3)],
            device_id=(me, there),
            device_id_type=MESH,
        ).start()

    gated = recv2[...].astype(F32) * gate_rows[0].reshape(ROWS, 8, COLS)
    squares = jnp.sum(gated * gated, axis=0)
    squares = squares + pltpu.roll(squares, 4, axis=0)
    squares = squares + pltpu.roll(squares, 2, axis=0)
    factor = lax.rsqrt(squares * (GROUPS / CHANNELS) + NORM_EPS)
    gated = gated * factor[None] * gate_rows[1].reshape(ROWS, 8, COLS)
    flat[...] = gated.reshape(256, COLS)
    for half in range(2):
        gated = flat[pl.ds(half, COLS, stride=2), :].T
        send3[4 * half : 4 * half + 4] = gated.reshape(4, 32, COLS).astype(BF)
        if half == EAGER // 4:
            pl.when(col != EAGER)(lambda: send_over(EAGER, lax.rem(y + 4 - EAGER // 2, 4)))

    for (dy, _), there in zip(FAR_COLS, col_peers):
        pl.when(there != EAGER)(lambda there=there, dy=dy: send_over(there, (4 - dy) % 4))
    recv3[partner] = send3[col]
    loaded((out_w, 5))

    def arrived(count, number):
        block = recv3.at[pl.ds(0, count)]
        pltpu.make_async_copy(block, block, recv_sems.at[number]).wait()

    for back, sender in ((0, None), (1, None), (3, 0), (2, None), (3, 1)):
        source = lax.rem(y + back, 4)
        if sender is None:
            arrived(2 if back else 1, 5 + back)
            mixed = jnp.concatenate([recv3[2 * source], recv3[2 * source + 1]], axis=1)
            rows = pl.ds(pl.multiple_of(source * 256, 256), 256)
        else:
            arrived(1, 8 + sender)
            group = 2 * source + 1 - sender
            mixed = recv3[group]
            rows = pl.ds(pl.multiple_of(group * 128, 128), 128)
        part = dot(mixed, out_w[rows, :])
        if back == 0:
            total[...] = part
        elif sender != 1:
            total[...] += part
        else:
            out_ref[...] = (total[...] + part).astype(BF)

    sent = mixed_taps.at[pl.ds(0, 760)]
    pltpu.make_async_copy(sent, sent, send_sem).wait()


def local(
    tokens, norm_gain, first_gate, second_gate, value_weight, short_weight, short_bias,
    embed_weight, embed_bias, inner_weight, inner_bias, filter_freq, filter_weight, filter_skip,
    output_gain, output_weight,
):
    constants = make_constants()
    operands = [
        tokens, norm_gain[None], first_gate, second_gate, value_weight, short_weight, short_bias,
        embed_weight, embed_bias[None], inner_weight, inner_bias[None], filter_freq[None],
        jnp.swapaxes(filter_weight, 2, 3), filter_skip, output_gain[None], output_weight,
    ] + [
        jnp.asarray(constants[name])
        for name in ("twiddle", "tables", "feats")
    ]
    vmem = pltpu.VMEM
    scratch = [vmem(tokens.shape, BF), vmem((1, WIDTH + COLS), F32), vmem((WIDTH, 384), BF)]
    scratch += [vmem(x.shape, x.dtype) for x in operands[5:7]]
    scratch += [vmem((97, 64), F32), vmem((3, 1, 64), F32)]
    scratch += [vmem(x.shape, x.dtype) for x in operands[12:14] + operands[15:]]
    scratch += [
        vmem((256, WIDTH), BF),
        vmem((256, COLS), F32),
        vmem((256, COLS), F32),
        vmem((2, ROWS, 8, COLS), BF),
        vmem((2, ROWS, 8, COLS), BF),
        vmem((128, 128), F32),
        vmem((2 * LIVE * 8, COLS), F32),
        vmem((2, OWN * HALF, 2 * COLS), F32),
        vmem((2, 256, COLS), F32),
        vmem((ROWS, 8, COLS), BF),
        vmem((ROWS, 8, COLS), BF),
        vmem((8, 32, COLS), BF),
        vmem((8, 32, COLS), BF),
        vmem((264, COLS), F32),
        vmem((264, COLS), F32),
        vmem((2, 256, COLS), F32),
        vmem((2, 8, COLS), BF),
        vmem((2, 8, COLS), BF),
        vmem((32, WIDTH), F32),
        pltpu.SemaphoreType.DMA((13,)),
        pltpu.SemaphoreType.DMA(()),
        pltpu.SemaphoreType.DMA((10,)),
    ]
    return pl.pallas_call(
        kernel,
        out_shape=pltpu.VMEM((32, WIDTH), BF),
        in_specs=[pl.BlockSpec(memory_space=pltpu.HBM)] * len(operands),
        out_specs=pl.BlockSpec(memory_space=pltpu.VMEM),
        scratch_shapes=scratch,
        compiler_params=pltpu.CompilerParams(
            collective_id=0, has_side_effects=True, vmem_limit_bytes=66_912_256
        ),
    )(*operands)


def solution(mesh):
    in_specs = (
        P("row", None),
        P(),
        P(None, "col"),
        P(None, "col"),
        P(None, "col"),
        P(None, None, "col"),
        P(None, "col"),
        P(),
        P(),
        P(),
        P(),
        P(),
        P(None, None, None, ("col", "row")),
        P(None, ("col", "row")),
        P("col"),
        P(),
    )
    out_specs = P(("row", "col"), None)
    return jax.shard_map(local, mesh=mesh, in_specs=in_specs, out_specs=out_specs, check_vma=False)
```

```python
import math

import jax
import jax.numpy as jnp
import ml_dtypes
import numpy as np
from jax import lax
from jax.experimental import pallas as pl
from jax.experimental.pallas import tpu as pltpu
from jax.sharding import PartitionSpec as P

CHANNELS = 1024
GROUPS = 8
FREQ_BANDS = 16
NORM_EPS = 1e-06
DECAY_TARGET = 0.01
FAST_SPAN = 0.3
SLOW_SPAN = 1.5

LENGTH = 8192
WIDTH = 2048
COLS = 128
LIVE = 64
EAGER = 1
HALF = 72
TOTAL = 16384
ROWS = 32
OWN = 4
FEATS = 48
CHUNK = 2048


def farthest_first(steps):
    return [step for step in sorted(steps, reverse=True) if any(step[1])]


ROW_HOPS = farthest_first(
    [(min(dz, 8 - dz) + min(dx, 4 - dx), (dz, dx)) for dz in range(8) for dx in range(4)]
)
FAR_ROWS = [offset for _, offset in ROW_HOPS]
COL_HOPS = farthest_first(
    [(2 * min(dy, 4 - dy) + dc, (dy, dc)) for dy in range(4) for dc in range(2)]
)
FAR_COLS = [offset for _, offset in COL_HOPS]

BF = jnp.bfloat16
F32 = jnp.float32
MESH = pl.DeviceIdType.MESH


def split_np(matrix):
    high = matrix.astype(np.float32).astype(ml_dtypes.bfloat16)
    low = (matrix - high.astype(np.float64)).astype(np.float32).astype(ml_dtypes.bfloat16)
    return high, low


def make_constants():
    k1 = np.arange(HALF)
    a = np.arange(LIVE)
    b = np.arange(COLS)
    cos_in = np.cos(2 * np.pi * np.outer(k1, a) / COLS)
    sin_in = np.sin(2 * np.pi * np.outer(k1, a) / COLS)
    first = np.concatenate([cos_in, -sin_in], 0)
    turn = 2 * np.pi * np.outer(k1, b) / TOTAL
    twiddle = np.concatenate([np.cos(turn), np.sin(turn)], 1).astype(np.float32)
    cos_out = np.cos(2 * np.pi * (np.outer(b, b) % COLS) / COLS)
    sin_out = np.sin(2 * np.pi * (np.outer(b, b) % COLS) / COLS)
    second = np.block([[cos_out, -sin_out], [sin_out, cos_out]])
    back = np.block([[cos_out, sin_out], [-sin_out, cos_out]])
    weight = np.where((k1 == 0) | (k1 == COLS // 2), 1.0, 2.0) * (k1 <= COLS // 2)
    last = np.concatenate([cos_in.T * weight, -sin_in.T * weight], 1) / TOTAL
    tables = np.zeros((720, 2 * COLS))
    tables[0:256] = second
    tables[256:512] = back
    tables[512 : 512 + 2 * HALF, :LIVE] = first
    tables[656:720, : 2 * HALF] = last
    n = np.arange(LENGTH)
    ramp = np.linspace(0.0, 1.0, LENGTH)[None, :]
    bands = np.linspace(0.0001, FREQ_BANDS - 1, FREQ_BANDS, dtype=np.float32).astype(np.float64)
    angle = bands[:, None] * (2 * np.pi * n / LENGTH)[None, :]
    feats = np.zeros((FEATS, LENGTH))
    feats[0:1] = ramp
    feats[1 : 1 + FREQ_BANDS] = np.cos(angle)
    feats[1 + FREQ_BANDS : 1 + 2 * FREQ_BANDS] = -np.sin(angle)
    feats[1 + 2 * FREQ_BANDS] = 1.0
    return dict(
        twiddle=twiddle,
        tables=split_np(tables)[0],
        feats=np.concatenate(split_np(feats), 0),
    )


def sine_coefficients():
    v = 0.25 * np.cos(np.pi * (np.arange(400) + 0.5) / 800)
    basis = np.stack([v ** (2 * j + 1) for j in range(5)], 1)
    scale = 1.0 / np.sin(2 * np.pi * v)
    found = np.linalg.lstsq(basis * scale[:, None], np.ones_like(v), rcond=None)[0]
    return [float(c) for c in found]


SINE = sine_coefficients()


def sine_of_turns(turns):
    v = 0.25 - jnp.abs(turns - jnp.round(turns))
    square = v * v
    result = SINE[4]
    for c in SINE[3::-1]:
        result = result * square + c
    return result * v


def split(value):
    high = value.astype(BF)
    return high, (value - high.astype(F32)).astype(BF)


def dot(left, right):
    return jnp.dot(left, right, preferred_element_type=F32)


def tall(value):
    high, low = split(value)
    return jnp.concatenate([high, high, low], axis=0)


def wide(value):
    high, low = split(value)
    return jnp.concatenate([high, low, high], axis=1)


def into_spectrum(signal, tables, twiddle):
    part = dot(tables[512:656, :LIVE], signal.astype(BF))
    cos, sin = twiddle[:, :COLS], twiddle[:, COLS:]
    pieces = []
    for i in range(signal.shape[1] // COLS):
        real = part[:HALF, i * COLS : (i + 1) * COLS]
        imag = part[HALF:, i * COLS : (i + 1) * COLS]
        pieces.append(jnp.concatenate([real * cos + imag * sin, imag * cos - real * sin], axis=1))
    return jnp.concatenate(pieces, axis=0).astype(BF)


def from_spectrum(spectrum, tables, twiddle):
    part = dot(spectrum.astype(BF), tables[256:512, :])
    cos, sin = twiddle[:, :COLS], twiddle[:, COLS:]
    reals, imags = [], []
    for i in range(spectrum.shape[0] // HALF):
        real = part[i * HALF : (i + 1) * HALF, :COLS]
        imag = part[i * HALF : (i + 1) * HALF, COLS:]
        reals.append(real * cos - imag * sin)
        imags.append(real * sin + imag * cos)
    turned = jnp.concatenate(
        [jnp.concatenate(reals, axis=1), jnp.concatenate(imags, axis=1)], axis=0
    )
    return dot(tables[656:720, : 2 * HALF], turned.astype(BF))


def kernel(
    tokens_hbm, norm_gain_hbm, gate0_hbm, gate1_hbm, gate2_hbm, short_w_hbm, short_b_hbm,
    embed_w_hbm, embed_b_hbm, inner_w_hbm, inner_b_hbm, freq_hbm, filter_w_hbm, skip_hbm,
    out_gain_hbm, out_w_hbm, twiddle_hbm, tables_hbm, feats_hbm,
    out_ref,
    tokens, gains, gates, short_w, short_b, layers, lines,
    filter_w, skip, out_w, twiddle, tables, feats,
    normed, flat, packed, send1, recv1, params, mixed_taps, spectra, smooth,
    send2, recv2, send3, recv3, gate_own, gate_in, gate_rows, edge_out, edge_in, total, load_sem, send_sem, recv_sems,
):
    me = lax.axis_index("row")
    col = lax.axis_index("col")
    n_col = 8

    def loaded(*targets):
        for target, number in targets:
            pltpu.make_async_copy(target, target, load_sem.at[number]).wait()

    barrier = pltpu.get_barrier_semaphore()

    z, x = lax.div(me, 4), lax.rem(me, 4)
    row_peers = [lax.rem(z + dz, 8) * 4 + lax.rem(x + dx, 4) for dz, dx in FAR_ROWS]
    y, core = lax.div(col, 2), lax.rem(col, 2)
    partner = y * 2 + 1 - core
    col_peers = [lax.rem(y + dy, 4) * 2 + lax.rem(core + dc, 2) for dy, dc in FAR_COLS]
    for there in row_peers:
        pl.semaphore_signal(barrier, inc=1, device_id=(there, col), device_id_type=MESH)
    copies = [
        (tokens_hbm, tokens, 0),
        (norm_gain_hbm, gains.at[:, 0:WIDTH], 1),
        (gate0_hbm, gates.at[:, 0:128], 2),
        (gate1_hbm, gates.at[:, 128:256], 2),
        (gate2_hbm, gates.at[:, 256:384], 2),
        (embed_w_hbm, layers.at[64:97], 3),
        (embed_b_hbm, lines.at[0], 4),
        (inner_b_hbm, lines.at[1], 4),
        (freq_hbm, lines.at[2], 4),
        (inner_w_hbm, layers.at[0:64], 3),
        (filter_w_hbm, filter_w, 6),
        (feats_hbm, feats, 7),
        (tables_hbm, tables, 8),
        (twiddle_hbm, twiddle, 9),
        (short_w_hbm, short_w, 10),
        (short_b_hbm, short_b, 11),
        (skip_hbm, skip, 12),
        (out_gain_hbm, gains.at[:, WIDTH : WIDTH + COLS], 1),
        (out_w_hbm, out_w, 5),
    ]
    for source, target, number in copies:
        pltpu.make_async_copy(source, target, load_sem.at[number]).start()

    for there in col_peers:
        pl.semaphore_signal(barrier, inc=1, device_id=(me, there), device_id_type=MESH)

    loaded((tokens, 0), (gains, 1))

    def normalise(j, carry):
        rows = pl.ds(pl.multiple_of(j * 64, 64), 64)
        wide_tokens = tokens[rows, :].astype(F32)
        mean = jnp.mean(wide_tokens * wide_tokens, axis=1, keepdims=True)
        normed[rows, :] = (wide_tokens * lax.rsqrt(mean + NORM_EPS) * gains[:, 0:WIDTH]).astype(BF)
        return carry

    lax.fori_loop(0, 4, normalise, 0)
    loaded((gates, 2))
    projected = dot(normed[...], gates[...])
    projected = projected.astype(BF).astype(F32)
    gate_own[0:256, :] = projected[:, 128:256]
    edge_out[0] = projected[248:256, 128:256].astype(BF)
    edge_out[1] = projected[0:8, 128:256].astype(BF)
    for b in range(2):
        turned = projected[:, b * 256 : b * 256 + 128].T
        for half in range(2):
            flat[pl.ds(half * 128, 128), :] = turned[:, half * 128 : (half + 1) * 128]
        for half in range(2):
            for i in range(OWN):
                packed[pl.ds(4 * half + i, ROWS, stride=8), :] = flat[
                    pl.ds(128 * half + i, ROWS, stride=4), :
                ]
        send1[b] = packed[...].reshape(ROWS, 8, COLS).astype(BF)

    pl.semaphore_wait(barrier, ROWS - 1 + n_col - 1)

    urgency = [(hops - 1 + b, b, k) for k, (hops, _) in enumerate(ROW_HOPS) for b in range(2)]
    for _, b, k in sorted(urgency, key=lambda item: (-item[0], -item[1], item[2])):
        there = row_peers[k]
        pltpu.make_async_remote_copy(
            src_ref=send1.at[b, there],
            dst_ref=recv1.at[b, me],
            send_sem=send_sem,
            recv_sem=recv_sems.at[2 * b],
            device_id=(there, col),
            device_id_type=MESH,
        ).start()
    for b in range(2):
        recv1[b, me] = send1[b, me]
    for side, there in ((0, lax.rem(me + 1, ROWS)), (1, lax.rem(me + ROWS - 1, ROWS))):
        pltpu.make_async_remote_copy(
            src_ref=edge_out.at[side],
            dst_ref=edge_in.at[side],
            send_sem=send_sem,
            recv_sem=recv_sems.at[1],
            device_id=(there, col),
            device_id_type=MESH,
        ).start()

    loaded((layers, 3), (lines, 4), (filter_w, 6), (feats, 7), (tables, 8))
    loaded((twiddle, 9))
    params[...] = jnp.zeros_like(params)
    scale = lines[2] * (1.0 / (2.0 * math.pi))
    params[0:33, 0:64] = layers[64:97] * scale
    params[33:34, 0:64] = lines[0] * scale - 0.25
    params[48:49, 0:64] = lines[1] * scale - 0.25
    params[64:128, 0:64] = layers[0:64] * scale
    turned = params[...].T
    embed_t = wide(turned[0:64, 0:FEATS])
    inner_bias = turned[0:64, 48:49]
    inner_t = wide(turned[0:64, 64:128])
    filter_t = wide(
        jnp.concatenate([filter_w[o, e] for o in range(2) for e in range(2)], axis=0)
    )

    row8 = lax.broadcasted_iota(jnp.int32, (8, 1), 0)
    channel = (col * ROWS + me) * OWN + lax.rem(row8, OWN)
    fastest = math.log(DECAY_TARGET) / FAST_SPAN
    slowest = math.log(DECAY_TARGET) / SLOW_SPAN
    place = channel.astype(F32) * (1.0 / (CHANNELS - 1))
    decay = jnp.abs(slowest * (1.0 - place) + fastest * place)

    def taps_of(j, carry):
        start = pl.multiple_of(j * CHUNK, CHUNK)
        lanes = pl.ds(start, CHUNK)
        high, low = feats[0:FEATS, lanes], feats[FEATS:, lanes]
        hidden = sine_of_turns(dot(embed_t, jnp.concatenate([high, high, low], axis=0)))
        hidden = sine_of_turns(dot(inner_t, tall(hidden)) + inner_bias)
        taps = dot(filter_t, tall(hidden))
        lag = start + lax.broadcasted_iota(jnp.int32, (8, CHUNK), 1)
        row = lax.broadcasted_iota(jnp.int32, (8, CHUNK), 0)
        window = jnp.exp(-(lag.astype(F32) * (1.0 / (LENGTH - 1))) * decay)
        window = jnp.where((lag == 0) & (row >= OWN), 0.0, window)
        for o in range(2):
            both = taps[8 * o : 8 * o + 8] * window
            other = pltpu.roll(both, OWN, axis=0)
            both = jnp.where(row < OWN, both + other, other - both)
            for q in range(CHUNK // COLS):
                at = pl.multiple_of(start // COLS * 8, 8) + o * LIVE * 8 + q * 8
                mixed_taps[pl.ds(pl.multiple_of(at, 8), 8), :] = both[:, q * COLS : (q + 1) * COLS]
        return carry

    lax.fori_loop(0, LENGTH // CHUNK, taps_of, 0)
    for o in range(2):
        for part in range(2):
            signal = jnp.concatenate(
                [
                    mixed_taps[pl.ds(o * LIVE * 8 + part * OWN + i, LIVE, stride=8), :]
                    for i in range(OWN)
                ],
                axis=1,
            )
            spectra[o, :, part * COLS : (part + 1) * COLS] = dot(
                into_spectrum(signal, tables, twiddle),
                tables[0:256, part * COLS : (part + 1) * COLS],
            )

    loaded((short_w, 10), (short_b, 11), (skip, 12))
    lane8 = lax.broadcasted_iota(jnp.int32, (8, COLS), 1)
    mine = lane8 == OWN * me + lax.rem(lax.broadcasted_iota(jnp.int32, (8, COLS), 0), OWN)

    def own_column(line):
        return jnp.sum(
            jnp.where(mine, jnp.broadcast_to(line, (8, COLS)), 0.0), axis=1, keepdims=True
        )

    all_short = short_w[...].astype(F32)
    columns = [
        [own_column(all_short[b, j : j + 1]) for j in range(3)] + [own_column(short_b[b : b + 1, :])]
        for b in (0, 2)
    ]

    def wait_row(target, number):
        pltpu.make_async_copy(
            target.at[pl.ds(0, ROWS - 1)], target.at[pl.ds(0, ROWS - 1)], recv_sems.at[number]
        ).wait()

    row = lax.broadcasted_iota(jnp.int32, (256, COLS), 0)
    lane = lax.broadcasted_iota(jnp.int32, (256, COLS), 1)

    def smoothed(b):
        wait_row(recv1.at[b], 2 * b)
        here = recv1[b].astype(F32).reshape(256, COLS)
        before = pltpu.roll(here, 1, axis=1)
        before = jnp.where(lane == 0, pltpu.roll(before, OWN, axis=0), before)
        before = jnp.where((lane == 0) & (row < OWN), 0.0, before)
        after = pltpu.roll(here, COLS - 1, axis=1)
        after = jnp.where(lane == COLS - 1, pltpu.roll(after, 256 - OWN, axis=0), after)
        after = jnp.where((lane == COLS - 1) & (row >= 256 - OWN), 0.0, after)
        tap = [jnp.broadcast_to(c, (8, COLS))[None] for c in columns[b]]
        shape = (ROWS, 8, COLS)
        value = tap[3] + before.reshape(shape) * tap[0]
        value = value + here.reshape(shape) * tap[1]
        value = value + after.reshape(shape) * tap[2]
        smooth[b] = value.reshape(256, COLS)
        return jnp.concatenate(
            [smooth[b, pl.ds(i, LIVE, stride=OWN), :] for i in range(OWN)], axis=1
        )

    pairs = 2
    value = smoothed(1)
    signals = [value[:, p * COLS : (p + pairs) * COLS] for p in range(0, OWN, pairs)]
    for o in range(2):
        spectrum = [
            dot(into_spectrum(signal, tables, twiddle), tables[0:256, :])
            for signal in signals
        ]
        products = []
        for p, found in enumerate(spectrum):
            real, imag = found[:, :COLS], found[:, COLS:]
            rows = slice(p * pairs * HALF, (p + 1) * pairs * HALF)
            t_real, t_imag = spectra[o, rows, :COLS], spectra[o, rows, COLS:]
            products.append(
                jnp.concatenate(
                    [real * t_real - imag * t_imag, real * t_imag + imag * t_real], axis=1
                )
            )
        convolved = [from_spectrum(product, tables, twiddle) for product in products]
        signals = [
            found
            + jnp.concatenate(
                [
                    signal[:, i * COLS : (i + 1) * COLS]
                    * jnp.broadcast_to(
                        skip[o : o + 1, p * pairs + i : p * pairs + i + 1], (LIVE, COLS)
                    )
                    for i in range(pairs)
                ],
                axis=1,
            )
            for p, (found, signal) in enumerate(zip(convolved, signals))
        ]
        if o == 0:
            gate = smoothed(0)
            signals = [
                signal * gate[:, p * pairs * COLS : (p + 1) * pairs * COLS]
                for p, signal in enumerate(signals)
            ]
    signal = jnp.concatenate(signals, axis=1)

    for i in range(OWN):
        flat[pl.ds(i * LIVE, LIVE), :] = signal[:, i * COLS : (i + 1) * COLS]
    for i in range(OWN):
        for half in range(2):
            packed[pl.ds(2 * i + half, ROWS, stride=8), :] = flat[
                pl.ds(i * LIVE + half, ROWS, stride=2), :
            ]
    send2[...] = packed[...].reshape(ROWS, 8, COLS).astype(BF)

    def send_back(there):
        pltpu.make_async_remote_copy(
            src_ref=send2.at[there],
            dst_ref=recv2.at[me],
            send_sem=send_sem,
            recv_sem=recv_sems.at[3],
            device_id=(there, partner),
            device_id_type=MESH,
        ).start()

    send_back(0)
    for there in row_peers + [me]:
        pl.when(there != 0)(lambda there=there: send_back(there))
    pltpu.make_async_copy(edge_in, edge_in, recv_sems.at[1]).wait()
    position = lax.broadcasted_iota(jnp.int32, (256, COLS), 0)
    here = gate_own[0:256, :]
    first_edge = edge_in[0].astype(F32)[7:8] * jnp.where(me == 0, 0.0, 1.0)
    last_edge = edge_in[1].astype(F32)[0:1] * jnp.where(me == ROWS - 1, 0.0, 1.0)
    before = jnp.where(position == 0, first_edge, pltpu.roll(here, 1, axis=0))
    after = jnp.where(position == 255, last_edge, pltpu.roll(here, 255, axis=0))
    value = short_b[1:2, :] + before * all_short[1, 0:1]
    value = value + here * all_short[1, 1:2]
    gate_own[0:256, :] = value + after * all_short[1, 2:3]
    gate_own[256:264, :] = jnp.broadcast_to(gains[:, WIDTH : WIDTH + COLS], (8, COLS))
    pltpu.make_async_remote_copy(
        src_ref=gate_own,
        dst_ref=gate_in,
        send_sem=send_sem,
        recv_sem=recv_sems.at[4],
        device_id=(me, partner),
        device_id_type=MESH,
    ).start()

    pltpu.make_async_copy(gate_in, gate_in, recv_sems.at[4]).wait()
    gain = jnp.broadcast_to(gate_in[256:257], (COLS, COLS)).T
    for half in range(2):
        gate_rows[0, pl.ds(half, COLS, stride=2), :] = gate_in[half * 128 : half * 128 + 128].T
        gate_rows[1, pl.ds(half, COLS, stride=2), :] = gain

    pltpu.make_async_copy(recv2, recv2, recv_sems.at[3]).wait()

    def send_over(there, back):
        pltpu.make_async_remote_copy(
            src_ref=send3.at[there],
            dst_ref=recv3.at[partner],
            send_sem=send_sem,
            recv_sem=recv_sems.at[5 + back + core * (back // 3)],
            device_id=(me, there),
            device_id_type=MESH,
        ).start()

    gated = recv2[...].astype(F32) * gate_rows[0].reshape(ROWS, 8, COLS)
    squares = jnp.sum(gated * gated, axis=0)
    squares = squares + pltpu.roll(squares, 4, axis=0)
    squares = squares + pltpu.roll(squares, 2, axis=0)
    factor = lax.rsqrt(squares * (GROUPS / CHANNELS) + NORM_EPS)
    gated = gated * factor[None] * gate_rows[1].reshape(ROWS, 8, COLS)
    flat[...] = gated.reshape(256, COLS)
    for half in range(2):
        gated = flat[pl.ds(half, COLS, stride=2), :].T
        send3[4 * half : 4 * half + 4] = gated.reshape(4, 32, COLS).astype(BF)
        if half == EAGER // 4:
            pl.when(col != EAGER)(lambda: send_over(EAGER, lax.rem(y + 4 - EAGER // 2, 4)))

    for (dy, _), there in zip(FAR_COLS, col_peers):
        pl.when(there != EAGER)(lambda there=there, dy=dy: send_over(there, (4 - dy) % 4))
    recv3[partner] = send3[col]
    loaded((out_w, 5))

    def arrived(count, number):
        block = recv3.at[pl.ds(0, count)]
        pltpu.make_async_copy(block, block, recv_sems.at[number]).wait()

    for back, sender in ((0, None), (1, None), (3, 0), (2, None), (3, 1)):
        source = lax.rem(y + back, 4)
        if sender is None:
            arrived(2 if back else 1, 5 + back)
            mixed = jnp.concatenate([recv3[2 * source], recv3[2 * source + 1]], axis=1)
            rows = pl.ds(pl.multiple_of(source * 256, 256), 256)
        else:
            arrived(1, 8 + sender)
            group = 2 * source + 1 - sender
            mixed = recv3[group]
            rows = pl.ds(pl.multiple_of(group * 128, 128), 128)
        part = dot(mixed, out_w[rows, :])
        if back == 0:
            total[...] = part
        elif sender != 1:
            total[...] += part
        else:
            out_ref[...] = (total[...] + part).astype(BF)

    sent = mixed_taps.at[pl.ds(0, 760)]
    pltpu.make_async_copy(sent, sent, send_sem).wait()


def local(
    tokens, norm_gain, first_gate, second_gate, value_weight, short_weight, short_bias,
    embed_weight, embed_bias, inner_weight, inner_bias, filter_freq, filter_weight, filter_skip,
    output_gain, output_weight,
):
    constants = make_constants()
    operands = [
        tokens, norm_gain[None], first_gate, second_gate, value_weight, short_weight, short_bias,
        embed_weight, embed_bias[None], inner_weight, inner_bias[None], filter_freq[None],
        jnp.swapaxes(filter_weight, 2, 3), filter_skip, output_gain[None], output_weight,
    ] + [
        jnp.asarray(constants[name])
        for name in ("twiddle", "tables", "feats")
    ]
    vmem = pltpu.VMEM
    scratch = [vmem(tokens.shape, BF), vmem((1, WIDTH + COLS), F32), vmem((WIDTH, 384), BF)]
    scratch += [vmem(x.shape, x.dtype) for x in operands[5:7]]
    scratch += [vmem((97, 64), F32), vmem((3, 1, 64), F32)]
    scratch += [vmem(x.shape, x.dtype) for x in operands[12:14] + operands[15:]]
    scratch += [
        vmem((256, WIDTH), BF),
        vmem((256, COLS), F32),
        vmem((256, COLS), F32),
        vmem((2, ROWS, 8, COLS), BF),
        vmem((2, ROWS, 8, COLS), BF),
        vmem((128, 128), F32),
        vmem((2 * LIVE * 8, COLS), F32),
        vmem((2, OWN * HALF, 2 * COLS), F32),
        vmem((2, 256, COLS), F32),
        vmem((ROWS, 8, COLS), BF),
        vmem((ROWS, 8, COLS), BF),
        vmem((8, 32, COLS), BF),
        vmem((8, 32, COLS), BF),
        vmem((264, COLS), F32),
        vmem((264, COLS), F32),
        vmem((2, 256, COLS), F32),
        vmem((2, 8, COLS), BF),
        vmem((2, 8, COLS), BF),
        vmem((32, WIDTH), F32),
        pltpu.SemaphoreType.DMA((13,)),
        pltpu.SemaphoreType.DMA(()),
        pltpu.SemaphoreType.DMA((10,)),
    ]
    return pl.pallas_call(
        kernel,
        out_shape=pltpu.VMEM((32, WIDTH), BF),
        in_specs=[pl.BlockSpec(memory_space=pltpu.HBM)] * len(operands),
        out_specs=pl.BlockSpec(memory_space=pltpu.VMEM),
        scratch_shapes=scratch,
        compiler_params=pltpu.CompilerParams(
            collective_id=0, has_side_effects=True, vmem_limit_bytes=66_912_256
        ),
    )(*operands)


def solution(mesh):
    in_specs = (
        P("row", None),
        P(),
        P(None, "col"),
        P(None, "col"),
        P(None, "col"),
        P(None, None, "col"),
        P(None, "col"),
        P(),
        P(),
        P(),
        P(),
        P(),
        P(None, None, None, ("col", "row")),
        P(None, ("col", "row")),
        P("col"),
        P(),
    )
    out_specs = P(("row", "col"), None)
    return jax.shard_map(local, mesh=mesh, in_specs=in_specs, out_specs=out_specs, check_vma=False)
```

```python
import math

import jax
import jax.numpy as jnp
import ml_dtypes
import numpy as np
from jax import lax
from jax.experimental import pallas as pl
from jax.experimental.pallas import tpu as pltpu
from jax.sharding import PartitionSpec as P

CHANNELS = 1024
GROUPS = 8
FREQ_BANDS = 16
NORM_EPS = 1e-06
DECAY_TARGET = 0.01
FAST_SPAN = 0.3
SLOW_SPAN = 1.5

LENGTH = 8192
WIDTH = 2048
COLS = 128
LIVE = 64
EAGER = 1
HALF = 72
TOTAL = 16384
ROWS = 32
OWN = 4
FEATS = 48
CHUNK = 2048


def farthest_first(steps):
    return [step for step in sorted(steps, reverse=True) if any(step[1])]


ROW_HOPS = farthest_first(
    [(min(dz, 8 - dz) + min(dx, 4 - dx), (dz, dx)) for dz in range(8) for dx in range(4)]
)
FAR_ROWS = [offset for _, offset in ROW_HOPS]
COL_HOPS = farthest_first(
    [(2 * min(dy, 4 - dy) + dc, (dy, dc)) for dy in range(4) for dc in range(2)]
)
FAR_COLS = [offset for _, offset in COL_HOPS]

BF = jnp.bfloat16
F32 = jnp.float32
MESH = pl.DeviceIdType.MESH


def split_np(matrix):
    high = matrix.astype(np.float32).astype(ml_dtypes.bfloat16)
    low = (matrix - high.astype(np.float64)).astype(np.float32).astype(ml_dtypes.bfloat16)
    return high, low


def make_constants():
    k1 = np.arange(HALF)
    a = np.arange(LIVE)
    b = np.arange(COLS)
    cos_in = np.cos(2 * np.pi * np.outer(k1, a) / COLS)
    sin_in = np.sin(2 * np.pi * np.outer(k1, a) / COLS)
    first = np.concatenate([cos_in, -sin_in], 0)
    turn = 2 * np.pi * np.outer(k1, b) / TOTAL
    twiddle = np.concatenate([np.cos(turn), np.sin(turn)], 1).astype(np.float32)
    cos_out = np.cos(2 * np.pi * (np.outer(b, b) % COLS) / COLS)
    sin_out = np.sin(2 * np.pi * (np.outer(b, b) % COLS) / COLS)
    second = np.block([[cos_out, -sin_out], [sin_out, cos_out]])
    back = np.block([[cos_out, sin_out], [-sin_out, cos_out]])
    weight = np.where((k1 == 0) | (k1 == COLS // 2), 1.0, 2.0) * (k1 <= COLS // 2)
    last = np.concatenate([cos_in.T * weight, -sin_in.T * weight], 1) / TOTAL
    tables = np.zeros((720, 2 * COLS))
    tables[0:256] = second
    tables[256:512] = back
    tables[512 : 512 + 2 * HALF, :LIVE] = first
    tables[656:720, : 2 * HALF] = last
    n = np.arange(LENGTH)
    ramp = np.linspace(0.0, 1.0, LENGTH)[None, :]
    bands = np.linspace(0.0001, FREQ_BANDS - 1, FREQ_BANDS, dtype=np.float32).astype(np.float64)
    angle = bands[:, None] * (2 * np.pi * n / LENGTH)[None, :]
    feats = np.zeros((FEATS, LENGTH))
    feats[0:1] = ramp
    feats[1 : 1 + FREQ_BANDS] = np.cos(angle)
    feats[1 + FREQ_BANDS : 1 + 2 * FREQ_BANDS] = -np.sin(angle)
    feats[1 + 2 * FREQ_BANDS] = 1.0
    return dict(
        twiddle=twiddle,
        tables=split_np(tables)[0],
        feats=np.concatenate(split_np(feats), 0),
    )


def sine_coefficients():
    v = 0.25 * np.cos(np.pi * (np.arange(400) + 0.5) / 800)
    basis = np.stack([v ** (2 * j + 1) for j in range(5)], 1)
    scale = 1.0 / np.sin(2 * np.pi * v)
    found = np.linalg.lstsq(basis * scale[:, None], np.ones_like(v), rcond=None)[0]
    return [float(c) for c in found]


SINE = sine_coefficients()


def sine_of_turns(turns):
    v = 0.25 - jnp.abs(turns - jnp.round(turns))
    square = v * v
    result = SINE[4]
    for c in SINE[3::-1]:
        result = result * square + c
    return result * v


def split(value):
    high = value.astype(BF)
    return high, (value - high.astype(F32)).astype(BF)


def dot(left, right):
    return jnp.dot(left, right, preferred_element_type=F32)


def tall(value):
    high, low = split(value)
    return jnp.concatenate([high, high, low], axis=0)


def wide(value):
    high, low = split(value)
    return jnp.concatenate([high, low, high], axis=1)


def into_spectrum(signal, tables, twiddle):
    part = dot(tables[512:656, :LIVE], signal.astype(BF))
    cos, sin = twiddle[:, :COLS], twiddle[:, COLS:]
    pieces = []
    for i in range(signal.shape[1] // COLS):
        real = part[:HALF, i * COLS : (i + 1) * COLS]
        imag = part[HALF:, i * COLS : (i + 1) * COLS]
        pieces.append(jnp.concatenate([real * cos + imag * sin, imag * cos - real * sin], axis=1))
    return jnp.concatenate(pieces, axis=0).astype(BF)


def from_spectrum(spectrum, tables, twiddle):
    part = dot(spectrum.astype(BF), tables[256:512, :])
    cos, sin = twiddle[:, :COLS], twiddle[:, COLS:]
    reals, imags = [], []
    for i in range(spectrum.shape[0] // HALF):
        real = part[i * HALF : (i + 1) * HALF, :COLS]
        imag = part[i * HALF : (i + 1) * HALF, COLS:]
        reals.append(real * cos - imag * sin)
        imags.append(real * sin + imag * cos)
    turned = jnp.concatenate(
        [jnp.concatenate(reals, axis=1), jnp.concatenate(imags, axis=1)], axis=0
    )
    return dot(tables[656:720, : 2 * HALF], turned.astype(BF))


def kernel(
    tokens_hbm, norm_gain_hbm, gate0_hbm, gate1_hbm, gate2_hbm, short_w_hbm, short_b_hbm,
    embed_w_hbm, embed_b_hbm, inner_w_hbm, inner_b_hbm, freq_hbm, filter_w_hbm, skip_hbm,
    out_gain_hbm, out_w_hbm, twiddle_hbm, tables_hbm, feats_hbm,
    out_ref,
    tokens, gains, gates, short_w, short_b, layers, lines,
    filter_w, skip, out_w, twiddle, tables, feats,
    normed, flat, packed, send1, recv1, params, mixed_taps, spectra, smooth,
    send2, recv2, send3, recv3, gate_own, gate_in, gate_rows, edge_out, edge_in, total, load_sem, send_sem, recv_sems,
):
    me = lax.axis_index("row")
    col = lax.axis_index("col")
    n_col = 8

    def loaded(*targets):
        for target, number in targets:
            pltpu.make_async_copy(target, target, load_sem.at[number]).wait()

    barrier = pltpu.get_barrier_semaphore()

    z, x = lax.div(me, 4), lax.rem(me, 4)
    row_peers = [lax.rem(z + dz, 8) * 4 + lax.rem(x + dx, 4) for dz, dx in FAR_ROWS]
    y, core = lax.div(col, 2), lax.rem(col, 2)
    partner = y * 2 + 1 - core
    col_peers = [lax.rem(y + dy, 4) * 2 + lax.rem(core + dc, 2) for dy, dc in FAR_COLS]
    for there in row_peers:
        pl.semaphore_signal(barrier, inc=1, device_id=(there, col), device_id_type=MESH)
    copies = [
        (tokens_hbm, tokens, 0),
        (norm_gain_hbm, gains.at[:, 0:WIDTH], 1),
        (gate0_hbm, gates.at[:, 0:128], 2),
        (gate1_hbm, gates.at[:, 128:256], 2),
        (gate2_hbm, gates.at[:, 256:384], 2),
        (embed_w_hbm, layers.at[64:97], 3),
        (embed_b_hbm, lines.at[0], 4),
        (inner_b_hbm, lines.at[1], 4),
        (freq_hbm, lines.at[2], 4),
        (inner_w_hbm, layers.at[0:64], 3),
        (filter_w_hbm, filter_w, 6),
        (feats_hbm, feats, 7),
        (tables_hbm, tables, 8),
        (twiddle_hbm, twiddle, 9),
        (short_w_hbm, short_w, 10),
        (short_b_hbm, short_b, 11),
        (skip_hbm, skip, 12),
        (out_gain_hbm, gains.at[:, WIDTH : WIDTH + COLS], 1),
        (out_w_hbm, out_w, 5),
    ]
    for source, target, number in copies:
        pltpu.make_async_copy(source, target, load_sem.at[number]).start()

    for there in col_peers:
        pl.semaphore_signal(barrier, inc=1, device_id=(me, there), device_id_type=MESH)

    loaded((tokens, 0), (gains, 1))

    def normalise(j, carry):
        rows = pl.ds(pl.multiple_of(j * 64, 64), 64)
        wide_tokens = tokens[rows, :].astype(F32)
        mean = jnp.mean(wide_tokens * wide_tokens, axis=1, keepdims=True)
        normed[rows, :] = (wide_tokens * lax.rsqrt(mean + NORM_EPS) * gains[:, 0:WIDTH]).astype(BF)
        return carry

    lax.fori_loop(0, 4, normalise, 0)
    loaded((gates, 2))
    projected = dot(normed[...], gates[...])
    projected = projected.astype(BF).astype(F32)
    gate_own[0:256, :] = projected[:, 128:256]
    edge_out[0] = projected[248:256, 128:256].astype(BF)
    edge_out[1] = projected[0:8, 128:256].astype(BF)
    for b in range(2):
        turned = projected[:, b * 256 : b * 256 + 128].T
        for half in range(2):
            flat[pl.ds(half * 128, 128), :] = turned[:, half * 128 : (half + 1) * 128]
        for half in range(2):
            for i in range(OWN):
                packed[pl.ds(4 * half + i, ROWS, stride=8), :] = flat[
                    pl.ds(128 * half + i, ROWS, stride=4), :
                ]
        send1[b] = packed[...].reshape(ROWS, 8, COLS).astype(BF)

    pl.semaphore_wait(barrier, ROWS - 1 + n_col - 1)

    urgency = [(hops - 1 + b, b, k) for k, (hops, _) in enumerate(ROW_HOPS) for b in range(2)]
    for _, b, k in sorted(urgency, key=lambda item: (-item[0], -item[1], item[2])):
        there = row_peers[k]
        pltpu.make_async_remote_copy(
            src_ref=send1.at[b, there],
            dst_ref=recv1.at[b, me],
            send_sem=send_sem,
            recv_sem=recv_sems.at[2 * b],
            device_id=(there, col),
            device_id_type=MESH,
        ).start()
    for b in range(2):
        recv1[b, me] = send1[b, me]
    for side, there in ((0, lax.rem(me + 1, ROWS)), (1, lax.rem(me + ROWS - 1, ROWS))):
        pltpu.make_async_remote_copy(
            src_ref=edge_out.at[side],
            dst_ref=edge_in.at[side],
            send_sem=send_sem,
            recv_sem=recv_sems.at[1],
            device_id=(there, col),
            device_id_type=MESH,
        ).start()

    loaded((layers, 3), (lines, 4), (filter_w, 6), (feats, 7), (tables, 8))
    loaded((twiddle, 9))
    params[...] = jnp.zeros_like(params)
    scale = lines[2] * (1.0 / (2.0 * math.pi))
    params[0:33, 0:64] = layers[64:97] * scale
    params[33:34, 0:64] = lines[0] * scale - 0.25
    params[48:49, 0:64] = lines[1] * scale - 0.25
    params[64:128, 0:64] = layers[0:64] * scale
    turned = params[...].T
    embed_t = wide(turned[0:64, 0:FEATS])
    inner_bias = turned[0:64, 48:49]
    inner_t = wide(turned[0:64, 64:128])
    filter_t = wide(
        jnp.concatenate([filter_w[o, e] for o in range(2) for e in range(2)], axis=0)
    )

    row8 = lax.broadcasted_iota(jnp.int32, (8, 1), 0)
    channel = (col * ROWS + me) * OWN + lax.rem(row8, OWN)
    fastest = math.log(DECAY_TARGET) / FAST_SPAN
    slowest = math.log(DECAY_TARGET) / SLOW_SPAN
    place = channel.astype(F32) * (1.0 / (CHANNELS - 1))
    decay = jnp.abs(slowest * (1.0 - place) + fastest * place)

    def taps_of(j, carry):
        start = pl.multiple_of(j * CHUNK, CHUNK)
        lanes = pl.ds(start, CHUNK)
        high, low = feats[0:FEATS, lanes], feats[FEATS:, lanes]
        hidden = sine_of_turns(dot(embed_t, jnp.concatenate([high, high, low], axis=0)))
        hidden = sine_of_turns(dot(inner_t, tall(hidden)) + inner_bias)
        taps = dot(filter_t, tall(hidden))
        lag = start + lax.broadcasted_iota(jnp.int32, (8, CHUNK), 1)
        row = lax.broadcasted_iota(jnp.int32, (8, CHUNK), 0)
        window = jnp.exp(-(lag.astype(F32) * (1.0 / (LENGTH - 1))) * decay)
        window = jnp.where((lag == 0) & (row >= OWN), 0.0, window)
        for o in range(2):
            both = taps[8 * o : 8 * o + 8] * window
            other = pltpu.roll(both, OWN, axis=0)
            both = jnp.where(row < OWN, both + other, other - both)
            for q in range(CHUNK // COLS):
                at = pl.multiple_of(start // COLS * 8, 8) + o * LIVE * 8 + q * 8
                mixed_taps[pl.ds(pl.multiple_of(at, 8), 8), :] = both[:, q * COLS : (q + 1) * COLS]
        return carry

    lax.fori_loop(0, LENGTH // CHUNK, taps_of, 0)
    for o in range(2):
        for part in range(2):
            signal = jnp.concatenate(
                [
                    mixed_taps[pl.ds(o * LIVE * 8 + part * OWN + i, LIVE, stride=8), :]
                    for i in range(OWN)
                ],
                axis=1,
            )
            spectra[o, :, part * COLS : (part + 1) * COLS] = dot(
                into_spectrum(signal, tables, twiddle),
                tables[0:256, part * COLS : (part + 1) * COLS],
            )

    loaded((short_w, 10), (short_b, 11), (skip, 12))
    lane8 = lax.broadcasted_iota(jnp.int32, (8, COLS), 1)
    mine = lane8 == OWN * me + lax.rem(lax.broadcasted_iota(jnp.int32, (8, COLS), 0), OWN)

    def own_column(line):
        return jnp.sum(
            jnp.where(mine, jnp.broadcast_to(line, (8, COLS)), 0.0), axis=1, keepdims=True
        )

    all_short = short_w[...].astype(F32)
    columns = [
        [own_column(all_short[b, j : j + 1]) for j in range(3)] + [own_column(short_b[b : b + 1, :])]
        for b in (0, 2)
    ]

    def wait_row(target, number):
        pltpu.make_async_copy(
            target.at[pl.ds(0, ROWS - 1)], target.at[pl.ds(0, ROWS - 1)], recv_sems.at[number]
        ).wait()

    row = lax.broadcasted_iota(jnp.int32, (256, COLS), 0)
    lane = lax.broadcasted_iota(jnp.int32, (256, COLS), 1)

    def smoothed(b):
        wait_row(recv1.at[b], 2 * b)
        here = recv1[b].astype(F32).reshape(256, COLS)
        before = pltpu.roll(here, 1, axis=1)
        before = jnp.where(lane == 0, pltpu.roll(before, OWN, axis=0), before)
        before = jnp.where((lane == 0) & (row < OWN), 0.0, before)
        after = pltpu.roll(here, COLS - 1, axis=1)
        after = jnp.where(lane == COLS - 1, pltpu.roll(after, 256 - OWN, axis=0), after)
        after = jnp.where((lane == COLS - 1) & (row >= 256 - OWN), 0.0, after)
        tap = [jnp.broadcast_to(c, (8, COLS))[None] for c in columns[b]]
        shape = (ROWS, 8, COLS)
        value = tap[3] + before.reshape(shape) * tap[0]
        value = value + here.reshape(shape) * tap[1]
        value = value + after.reshape(shape) * tap[2]
        smooth[b] = value.reshape(256, COLS)
        return jnp.concatenate(
            [smooth[b, pl.ds(i, LIVE, stride=OWN), :] for i in range(OWN)], axis=1
        )

    pairs = 4
    value = smoothed(1)
    signals = [value[:, p * COLS : (p + pairs) * COLS] for p in range(0, OWN, pairs)]
    for o in range(2):
        spectrum = [
            dot(into_spectrum(signal, tables, twiddle), tables[0:256, :])
            for signal in signals
        ]
        products = []
        for p, found in enumerate(spectrum):
            real, imag = found[:, :COLS], found[:, COLS:]
            rows = slice(p * pairs * HALF, (p + 1) * pairs * HALF)
            t_real, t_imag = spectra[o, rows, :COLS], spectra[o, rows, COLS:]
            products.append(
                jnp.concatenate(
                    [real * t_real - imag * t_imag, real * t_imag + imag * t_real], axis=1
                )
            )
        convolved = [from_spectrum(product, tables, twiddle) for product in products]
        signals = [
            found
            + jnp.concatenate(
                [
                    signal[:, i * COLS : (i + 1) * COLS]
                    * jnp.broadcast_to(
                        skip[o : o + 1, p * pairs + i : p * pairs + i + 1], (LIVE, COLS)
                    )
                    for i in range(pairs)
                ],
                axis=1,
            )
            for p, (found, signal) in enumerate(zip(convolved, signals))
        ]
        if o == 0:
            gate = smoothed(0)
            signals = [
                signal * gate[:, p * pairs * COLS : (p + 1) * pairs * COLS]
                for p, signal in enumerate(signals)
            ]
    signal = jnp.concatenate(signals, axis=1)

    for i in range(OWN):
        flat[pl.ds(i * LIVE, LIVE), :] = signal[:, i * COLS : (i + 1) * COLS]
    for i in range(OWN):
        for half in range(2):
            packed[pl.ds(2 * i + half, ROWS, stride=8), :] = flat[
                pl.ds(i * LIVE + half, ROWS, stride=2), :
            ]
    send2[...] = packed[...].reshape(ROWS, 8, COLS).astype(BF)

    def send_back(there):
        pltpu.make_async_remote_copy(
            src_ref=send2.at[there],
            dst_ref=recv2.at[me],
            send_sem=send_sem,
            recv_sem=recv_sems.at[3],
            device_id=(there, partner),
            device_id_type=MESH,
        ).start()

    send_back(0)
    for there in row_peers + [me]:
        pl.when(there != 0)(lambda there=there: send_back(there))
    pltpu.make_async_copy(edge_in, edge_in, recv_sems.at[1]).wait()
    position = lax.broadcasted_iota(jnp.int32, (256, COLS), 0)
    here = gate_own[0:256, :]
    first_edge = edge_in[0].astype(F32)[7:8] * jnp.where(me == 0, 0.0, 1.0)
    last_edge = edge_in[1].astype(F32)[0:1] * jnp.where(me == ROWS - 1, 0.0, 1.0)
    before = jnp.where(position == 0, first_edge, pltpu.roll(here, 1, axis=0))
    after = jnp.where(position == 255, last_edge, pltpu.roll(here, 255, axis=0))
    value = short_b[1:2, :] + before * all_short[1, 0:1]
    value = value + here * all_short[1, 1:2]
    gate_own[0:256, :] = value + after * all_short[1, 2:3]
    gate_own[256:264, :] = jnp.broadcast_to(gains[:, WIDTH : WIDTH + COLS], (8, COLS))
    pltpu.make_async_remote_copy(
        src_ref=gate_own,
        dst_ref=gate_in,
        send_sem=send_sem,
        recv_sem=recv_sems.at[4],
        device_id=(me, partner),
        device_id_type=MESH,
    ).start()

    pltpu.make_async_copy(gate_in, gate_in, recv_sems.at[4]).wait()
    gain = jnp.broadcast_to(gate_in[256:257], (COLS, COLS)).T
    for half in range(2):
        gate_rows[0, pl.ds(half, COLS, stride=2), :] = gate_in[half * 128 : half * 128 + 128].T
        gate_rows[1, pl.ds(half, COLS, stride=2), :] = gain

    pltpu.make_async_copy(recv2, recv2, recv_sems.at[3]).wait()

    def send_over(there, back):
        pltpu.make_async_remote_copy(
            src_ref=send3.at[there],
            dst_ref=recv3.at[partner],
            send_sem=send_sem,
            recv_sem=recv_sems.at[5 + back + core * (back // 3)],
            device_id=(me, there),
            device_id_type=MESH,
        ).start()

    gated = recv2[...].astype(F32) * gate_rows[0].reshape(ROWS, 8, COLS)
    squares = jnp.sum(gated * gated, axis=0)
    squares = squares + pltpu.roll(squares, 4, axis=0)
    squares = squares + pltpu.roll(squares, 2, axis=0)
    factor = lax.rsqrt(squares * (GROUPS / CHANNELS) + NORM_EPS)
    gated = gated * factor[None] * gate_rows[1].reshape(ROWS, 8, COLS)
    flat[...] = gated.reshape(256, COLS)
    for half in range(2):
        gated = flat[pl.ds(half, COLS, stride=2), :].T
        send3[4 * half : 4 * half + 4] = gated.reshape(4, 32, COLS).astype(BF)
        if half == EAGER // 4:
            pl.when(col != EAGER)(lambda: send_over(EAGER, lax.rem(y + 4 - EAGER // 2, 4)))

    for (dy, _), there in zip(FAR_COLS, col_peers):
        pl.when(there != EAGER)(lambda there=there, dy=dy: send_over(there, (4 - dy) % 4))
    recv3[partner] = send3[col]
    loaded((out_w, 5))

    def arrived(count, number):
        block = recv3.at[pl.ds(0, count)]
        pltpu.make_async_copy(block, block, recv_sems.at[number]).wait()

    for back, sender in ((0, None), (1, None), (3, 0), (2, None), (3, 1)):
        source = lax.rem(y + back, 4)
        if sender is None:
            arrived(2 if back else 1, 5 + back)
            mixed = jnp.concatenate([recv3[2 * source], recv3[2 * source + 1]], axis=1)
            rows = pl.ds(pl.multiple_of(source * 256, 256), 256)
        else:
            arrived(1, 8 + sender)
            group = 2 * source + 1 - sender
            mixed = recv3[group]
            rows = pl.ds(pl.multiple_of(group * 128, 128), 128)
        part = dot(mixed, out_w[rows, :])
        if back == 0:
            total[...] = part
        elif sender != 1:
            total[...] += part
        else:
            out_ref[...] = (total[...] + part).astype(BF)

    sent = mixed_taps.at[pl.ds(0, 760)]
    pltpu.make_async_copy(sent, sent, send_sem).wait()


def local(
    tokens, norm_gain, first_gate, second_gate, value_weight, short_weight, short_bias,
    embed_weight, embed_bias, inner_weight, inner_bias, filter_freq, filter_weight, filter_skip,
    output_gain, output_weight,
):
    constants = make_constants()
    operands = [
        tokens, norm_gain[None], first_gate, second_gate, value_weight, short_weight, short_bias,
        embed_weight, embed_bias[None], inner_weight, inner_bias[None], filter_freq[None],
        jnp.swapaxes(filter_weight, 2, 3), filter_skip, output_gain[None], output_weight,
    ] + [
        jnp.asarray(constants[name])
        for name in ("twiddle", "tables", "feats")
    ]
    vmem = pltpu.VMEM
    scratch = [vmem(tokens.shape, BF), vmem((1, WIDTH + COLS), F32), vmem((WIDTH, 384), BF)]
    scratch += [vmem(x.shape, x.dtype) for x in operands[5:7]]
    scratch += [vmem((97, 64), F32), vmem((3, 1, 64), F32)]
    scratch += [vmem(x.shape, x.dtype) for x in operands[12:14] + operands[15:]]
    scratch += [
        vmem((256, WIDTH), BF),
        vmem((256, COLS), F32),
        vmem((256, COLS), F32),
        vmem((2, ROWS, 8, COLS), BF),
        vmem((2, ROWS, 8, COLS), BF),
        vmem((128, 128), F32),
        vmem((2 * LIVE * 8, COLS), F32),
        vmem((2, OWN * HALF, 2 * COLS), F32),
        vmem((2, 256, COLS), F32),
        vmem((ROWS, 8, COLS), BF),
        vmem((ROWS, 8, COLS), BF),
        vmem((8, 32, COLS), BF),
        vmem((8, 32, COLS), BF),
        vmem((264, COLS), F32),
        vmem((264, COLS), F32),
        vmem((2, 256, COLS), F32),
        vmem((2, 8, COLS), BF),
        vmem((2, 8, COLS), BF),
        vmem((32, WIDTH), F32),
        pltpu.SemaphoreType.DMA((13,)),
        pltpu.SemaphoreType.DMA(()),
        pltpu.SemaphoreType.DMA((10,)),
    ]
    return pl.pallas_call(
        kernel,
        out_shape=pltpu.VMEM((32, WIDTH), BF),
        in_specs=[pl.BlockSpec(memory_space=pltpu.HBM)] * len(operands),
        out_specs=pl.BlockSpec(memory_space=pltpu.VMEM),
        scratch_shapes=scratch,
        compiler_params=pltpu.CompilerParams(
            collective_id=0, has_side_effects=True, vmem_limit_bytes=66_912_256
        ),
    )(*operands)


def solution(mesh):
    in_specs = (
        P("row", None),
        P(),
        P(None, "col"),
        P(None, "col"),
        P(None, "col"),
        P(None, None, "col"),
        P(None, "col"),
        P(),
        P(),
        P(),
        P(),
        P(),
        P(None, None, None, ("col", "row")),
        P(None, ("col", "row")),
        P("col"),
        P(),
    )
    out_specs = P(("row", "col"), None)
    return jax.shard_map(local, mesh=mesh, in_specs=in_specs, out_specs=out_specs, check_vma=False)
```
